32 devices in a mesh: grp: 2 (over y), sp: 4 (over z), tp: 4 (over x, core).
Axes of the slice: x: 2, y: 2, z: 4, core: 2. Of those that a mesh axis runs over, the one named last changes fastest.
Arguments:
- mix_in: bfloat16 [2048, 1536], P(('grp', 'sp'), 'tp'), parts along dimension 0, may hold values from -6 to 6
- resid_in: bfloat16 [2048, 2048], P(('grp', 'sp', 'tp')), parts along dimension 0, may hold values from -6 to 6
- doc_ids: int32 [2048], P(('grp', 'sp')), parts along dimension 0, may hold values from 0 to 1, never falling along the last dimension, each value on 1 to 768 neighbouring positions
- group_weight: bfloat16 [4, 384, 384], P('tp'), may hold values from -0.3125 to 0.3125
- pool_scale: float32 [1536], P('tp'), may hold values from 0.1 to 1.9
- out_weight: bfloat16 [1536, 2048], P('tp'), may hold values from -0.15625 to 0.15625
- norm_gain: float32 [2048], replicated, may hold values from 0.1 to 1.9
- expert_ids: int32 [2048, 2], P(('grp', 'sp', 'tp')), parts along dimension 0, may hold values from 0 to 15, as said below
- route_weights: float32 [2048, 2], P(('grp', 'sp', 'tp')), parts along dimension 0, may hold values from 0.1 to 1
- w_gate: bfloat16 [16, 2048, 512], P(('sp', 'tp')), may hold values from -0.125 to 0.125
- w_up: bfloat16 [16, 2048, 512], P(('sp', 'tp')), may hold values from -0.125 to 0.125
- w_down: bfloat16 [16, 512, 2048], P(('sp', 'tp')), may hold values from -0.25 to 0.25
Outputs:
- layer_out: bfloat16 [2048, 2048], P(('grp', 'sp', 'tp')), parts along dimension 0
The draws below stay inside these ranges and needn't reach their ends.
There are 2 independent parts, one for each index of `grp`. The reference program is written for one: setup_inputs(seed, part) draws one part's arguments, and reference() takes and returns one part's arrays. A program takes and returns all parts, laid end to end along the dimension named above; an argument that names none is the same for every part. Nothing has to cross between parts.
Inputs may be any that keep to these rules, and one draw needn't show every extreme that they name: `doc_ids`: document numbers never fall along the positions. `expert_ids`: each row names two different experts of one group of 4 consecutive experts. Among the rows of one device (aligned blocks of 64 rows) no expert is named more than 16 times; in every draw the experts of some group are each named exactly 16 times in every block.
All inputs are finite; a program needn't handle non-finite values.
Results may differ from the reference program's by a relative error of at most 0.012.
Values may be sent and summed in bfloat16 or wider, within the bound.
A program may use at most 64 MiB of HBM per device.

```python
import math
import jax
import jax.numpy as jnp
import numpy as np
from jax import lax

D = 2048
GD = 384
FF = 512
POOL_GROUPS = 4
HALO = 16
EXPERT_GROUPS = 4
TOP_K = 2
MIX = 1536
SLICE = 64
TOKENS = 1024
EXPERTS = 16
EPG = 4
CAP = 16
DOCS = 2
SEG_MOST = 768


def block_order(subkey):
    return jax.random.permutation(subkey, SLICE)


def draw_expert_ids(key, part):
    blocks = TOKENS // SLICE
    busy_count = EPG * CAP // 2
    subkeys = jax.random.split(jax.random.fold_in(key, 11), 5)
    busy_group = jax.random.randint(subkeys[0], (), 0, EXPERT_GROUPS)
    spare_pick = jax.random.randint(subkeys[1], (blocks, SLICE), 0, EXPERT_GROUPS - 1)
    position = jnp.arange(SLICE, dtype=jnp.int32)[None, :]
    unshuffled = jnp.where(position < busy_count, busy_group, (busy_group + 1 + spare_pick) % EXPERT_GROUPS)
    row_order = jax.vmap(block_order)(jax.random.split(subkeys[2], blocks))
    row_group = jnp.take_along_axis(unshuffled, row_order, axis=1)
    onehot = (row_group[:, :, None] == jnp.arange(EXPERT_GROUPS, dtype=jnp.int32)[None, None, :]).astype(jnp.int32)
    row_rank = jnp.sum(onehot * (jnp.cumsum(onehot, axis=1) - 1), axis=2)
    first_shift = jax.random.randint(subkeys[3], (blocks, EXPERT_GROUPS), 0, EPG)
    second_shift = jax.random.randint(subkeys[4], (blocks, EXPERT_GROUPS), 0, EPG - 1)
    first_base = jnp.take_along_axis(first_shift, row_group, axis=1)
    second_extra = jnp.take_along_axis(second_shift, row_group, axis=1)
    first_pick = row_group * EPG + (row_rank + first_base) % EPG
    second_pick = row_group * EPG + (row_rank + first_base + 1 + second_extra) % EPG
    return jnp.stack([first_pick, second_pick], axis=-1).reshape(TOKENS, TOP_K).astype(jnp.int32)


def block_scale(stream_key, dims, shards, low, largest):
    level, own = 1.0, jax.random.fold_in(stream_key, 6)
    for dim, shards_of in shards:
        heights = jnp.exp(jax.random.uniform(jax.random.fold_in(own, dim), (shards_of,), jnp.float32, low / len(shards), largest / len(shards)))
        level = level * jnp.repeat(heights, dims[dim] // shards_of).reshape([-1 if axis == dim else 1 for axis in range(len(dims))])
    return level


def length_profile(number_of, total, most, skew):
    portions = [(1 << 20) // math.isqrt(rank ** skew) + 1 for rank in range(2, number_of + 1)]
    rest, holding = total - most - (number_of - 1), [1] * (number_of - 1)
    while rest > 0:
        candidates = [i for i in range(number_of - 1) if holding[i] < most]
        whole, budget = sum([portions[i] for i in candidates]), rest
        for i in candidates:
            extra = min(most - holding[i], max(1, budget * portions[i] // whole), rest)
            holding[i] = holding[i] + extra
            rest = rest - extra
    return np.array([most] + holding)


def ragged(own_key, amount, total, most, slope):
    if amount == 2:
        one = jax.random.randint(own_key, (), max(1, total - most), min(most, total - 1) + 1)
        return jnp.stack([one, total - one])
    tallies = jnp.asarray(length_profile(amount, total, most, slope), jnp.int32)
    pairs = (amount - 1) // 2
    source_of, sink = tallies[1:1 + 2 * pairs:2], tallies[2:2 + 2 * pairs:2]
    margin = jnp.minimum(source_of - 1, most - sink)
    moved = jax.random.randint(jax.random.fold_in(own_key, 1), (pairs,), 0, 1 << 20) % (margin + 1)
    tallies = tallies.at[1:1 + 2 * pairs:2].set(source_of - moved).at[2:2 + 2 * pairs:2].set(sink + moved)
    return tallies[jax.random.permutation(jax.random.fold_in(own_key, 2), amount)]


def scatter_about(stream_key, dims, deviation, most, cuts=(), kind=jnp.bfloat16):
    loudness = block_scale(stream_key, dims, cuts, -0.22, 0.18) if cuts else 1.0
    entries = jax.random.normal(stream_key, dims, jnp.float32) * deviation * loudness
    return jnp.minimum(jnp.maximum(entries, -most), most).astype(kind)


def setup_inputs(seed: int = 0, part: int = 0) -> dict:
    keys = jax.random.split(jax.random.key(seed), 13)
    part_splits = jax.random.split(jax.random.fold_in(keys[12], part), 13)
    return {
        "mix_in": scatter_about(part_splits[0], (TOKENS, MIX), 1.0, 6.0, ((0, 4), (1, 4))),
        "resid_in": scatter_about(part_splits[1], (TOKENS, D), 1.0, 6.0, ((0, 16),)),
        "doc_ids": jnp.searchsorted(jnp.cumsum(ragged(part_splits[2], DOCS, TOKENS, SEG_MOST, 2)), jnp.arange(TOKENS), side="right").astype(jnp.int32),
        "group_weight": scatter_about(keys[3], (POOL_GROUPS, GD, GD), GD ** -0.5, 0.3125, ((0, 4),)),
        "pool_scale": jnp.clip(1.0 + 0.18 * jax.random.normal(keys[4], (MIX,), jnp.float32), 0.1, 1.9),
        "out_weight": scatter_about(keys[5], (MIX, D), MIX ** -0.5, 0.15625, ((0, 4),)),
        "norm_gain": jnp.clip(1.0 + 0.18 * jax.random.normal(keys[6], (D,), jnp.float32), 0.1, 1.9),
        "expert_ids": draw_expert_ids(jax.random.fold_in(jax.random.fold_in(keys[12], part), 71), part),
        "route_weights": jnp.clip(jnp.exp(math.log(1.0) - 2.3025851 * jax.random.uniform(part_splits[8], (TOKENS, TOP_K), jnp.float32) ** block_scale(part_splits[8], (TOKENS, TOP_K), ((0, 16),), -0.2, 0.2)), 0.1, 1.0),
        "w_gate": scatter_about(keys[9], (EXPERTS, D, FF), D ** -0.5, 0.125, ((0, 16),)),
        "w_up": scatter_about(keys[10], (EXPERTS, D, FF), D ** -0.5, 0.125, ((0, 16),)),
        "w_down": scatter_about(keys[11], (EXPERTS, FF, D), FF ** -0.5, 0.25, ((0, 16),)),
    }


def expert_rows(flat_rows, gate_matrix, up_matrix, down_matrix):
    gate_part = jnp.dot(flat_rows, gate_matrix, preferred_element_type=jnp.float32)
    up_part = jnp.dot(flat_rows, up_matrix, preferred_element_type=jnp.float32)
    hidden = (jax.nn.silu(gate_part) * up_part).astype(jnp.bfloat16)
    return jnp.dot(hidden, down_matrix, preferred_element_type=jnp.float32).astype(jnp.bfloat16)

def reference(mix_in, resid_in, doc_ids, group_weight, pool_scale, out_weight, norm_gain, expert_ids, route_weights, w_gate, w_up, w_down):
    marked = doc_ids.astype(jnp.int32) + 1
    padded = jnp.concatenate([jnp.zeros((HALO, MIX), jnp.float32), mix_in.astype(jnp.float32)], axis=0)
    pad_marks = jnp.concatenate([jnp.zeros((HALO,), jnp.int32), marked])
    reach = jnp.left_shift(jnp.int32(2), jnp.arange(MIX, dtype=jnp.int32) // GD)
    running = jnp.zeros((TOKENS, MIX), jnp.float32)
    members = jnp.zeros((TOKENS, MIX), jnp.float32)
    for offset in range(HALO):
        rows_back = padded[HALO - offset:HALO - offset + TOKENS]
        same_doc = pad_marks[HALO - offset:HALO - offset + TOKENS] == marked
        keep = same_doc[:, None] & (offset < reach)[None, :]
        running = running + jnp.where(keep, rows_back, 0.0)
        members = members + keep.astype(jnp.float32)
    mixed = (running / members - mix_in.astype(jnp.float32)).astype(jnp.bfloat16)
    pieces = []
    for group_index in range(POOL_GROUPS):
        lower = group_index * GD
        product = jnp.dot(mixed[:, lower:lower + GD], group_weight[group_index], preferred_element_type=jnp.float32)
        pieces.append((product * pool_scale[lower:lower + GD]).astype(jnp.bfloat16))
    grouped = jnp.concatenate(pieces, axis=1)
    projected = jnp.dot(grouped, out_weight, preferred_element_type=jnp.float32)
    stream = (resid_in.astype(jnp.float32) + projected).astype(jnp.bfloat16)
    stream_f = stream.astype(jnp.float32)
    level = lax.optimization_barrier(jnp.mean(stream_f * stream_f, axis=1, keepdims=True))
    normed = (stream_f * lax.rsqrt(level + 1e-06) * norm_gain.astype(jnp.float32)).astype(jnp.bfloat16)
    route_total = TOKENS * TOP_K
    route_expert = expert_ids.reshape(-1).astype(jnp.int32)
    onehot = (route_expert[:, None] == jnp.arange(EXPERTS, dtype=jnp.int32)[None, :]).astype(jnp.int32)
    slot_index = lax.optimization_barrier(jnp.sum(onehot * (jnp.cumsum(onehot, axis=0) - 1), axis=1)).astype(jnp.int32)
    table = jnp.full((EXPERTS, EXPERTS * CAP), route_total, jnp.int32)
    table = table.at[route_expert, slot_index].set(jnp.arange(route_total, dtype=jnp.int32))
    normed_pad = jnp.concatenate([normed, jnp.zeros((1, D), jnp.bfloat16)], axis=0)

    def serve(answers, inputs):
        gate_matrix, up_matrix, down_matrix, routes = inputs
        rows_in = normed_pad[routes // TOP_K]
        served = expert_rows(rows_in, gate_matrix, up_matrix, down_matrix)
        return (answers.at[routes].set(served), None)
    answers, _ = lax.scan(serve, jnp.zeros((route_total + 1, D), jnp.bfloat16), (w_gate, w_up, w_down, table))
    weighted = answers[:route_total].astype(jnp.float32) * route_weights.reshape(-1)[:, None]
    paired = weighted.reshape(TOKENS, TOP_K, D)
    return (stream_f + paired[:, 0] + paired[:, 1]).astype(jnp.bfloat16)
```

```python
import functools

import jax
import jax.numpy as jnp
from jax import lax
from jax.experimental import pallas as pl
from jax.experimental.pallas import tpu as pltpu
from jax.sharding import PartitionSpec as P

HALO = 16
TOP_K = 2
EXPERT_GROUPS = 4
MESH = pl.DeviceIdType.MESH
F32 = jnp.float32
BF16 = jnp.bfloat16
I32 = jnp.int32


def iota(shape, dim):
    return lax.broadcasted_iota(I32, shape, dim)


def to_row(col):
    n = col.shape[0]
    eye = iota((n, n), 0) == iota((n, n), 1)
    return jnp.sum(jnp.where(eye, col, jnp.zeros_like(col)), axis=0, keepdims=True)


def to_col(row):
    n = row.shape[1]
    eye = iota((n, n), 0) == iota((n, n), 1)
    return jnp.sum(jnp.where(eye, row, jnp.zeros_like(row)), axis=1, keepdims=True)


def onehot(mask):
    return jnp.where(mask, 1.0, 0.0).astype(BF16)


class Plan:
    def __init__(self, sp_size, tp_size, token_rows):
        self.sp, self.tp, self.rows = sp_size, tp_size, token_rows
        self.experts = sp_size * tp_size
        self.groups = EXPERT_GROUPS
        self.span = sp_size // self.groups
        self.members = self.span * tp_size
        self.cap = max(TOP_K, 4 * token_rows // self.experts)
        self.block = min(token_rows, self.cap * self.members // TOP_K)
        if self.cap % 16 == 0:
            self.chunks, self.cap_pad = self.groups, self.cap
        else:
            self.chunks = 1
            whole = -(-self.cap * self.groups // 16) * 16
            self.cap_pad = whole // self.groups
        self.per_chunk = self.groups // self.chunks
        self.message = self.per_chunk * self.cap_pad
        self.served = self.members * self.message
        self.half = tp_size // 2
        self.parts = 2


def kernel(
    p,
    mix_hbm, resid_hbm, doc_ref, gw_hbm, scale_ref, ow_hbm, gain_ref, ids_ref, rw_ref, wg_hbm, wu_hbm, wd_hbm,
    out_ref,
    mix, resid, gw, ow, wg, wu, wd,
    halo, halo_doc, grp, keep, s1, r1, s2, r2, stream_f32, meta_out, meta_in, zb, zin, amat, chi, clo,
    xout, xin, ans, ret, zo, fin,
    load_sem, halo_send, halo_recv, m_send, m_recv, s1_send, s1_recv, s2_send, s2_recv,
    z_send, z_recv, x_send, x_recv, b_send, b_recv, f_send, f_recv,
):
    sp, tp = lax.axis_index("sp"), lax.axis_index("tp")
    local_rows, width = mix.shape
    d = resid.shape[1]
    rows, groups, half, parts = p.rows, p.groups, p.half, p.parts
    piece = d // parts
    loads = [
        pltpu.make_async_copy(src, dst, load_sem.at[i])
        for i, (src, dst) in enumerate(
            [
                (mix_hbm, mix), (gw_hbm.at[0], gw), (ow_hbm, ow), (resid_hbm, resid),
                (wg_hbm.at[0], wg), (wu_hbm.at[0], wu), (wd_hbm.at[0], wd),
            ]
        )
    ]
    for load in loads[:4]:
        load.start()

    my_group, lane_in_span = sp // p.span, sp % p.span
    me = lane_in_span * p.tp + tp
    flip = tp + 1 - 2 * (tp % 2)

    steps = [0] + sorted(range(1, groups), key=lambda step: min(step, groups - step))
    nearest = [(my_group + step) % groups for step in steps]

    def relay(group):
        return {"sp": group * p.span + lane_in_span, "tp": tp}

    def member(index):
        return {"sp": my_group * p.span + index // p.tp, "tp": index % p.tp}

    barrier = pltpu.get_barrier_semaphore()
    greeted = 0
    ahead, behind = (sp + 1) % p.sp, (sp + p.sp - 1) % p.sp
    targets = [{"sp": ahead, "tp": tp}, {"sp": behind, "tp": tp}]
    targets += [relay((my_group + off) % groups) for off in range(1, groups)]
    targets += [member((me + off) % p.members) for off in range(1, p.members)]
    for target in targets:
        pl.semaphore_signal(barrier, inc=1, device_id=target, device_id_type=MESH)
        greeted += 1

    def remote(src, dst, send, recv, device):
        return pltpu.make_async_remote_copy(
            src_ref=src, dst_ref=dst, send_sem=send, recv_sem=recv, device_id=device, device_id_type=MESH
        )

    ids = ids_ref[...]
    id0_row, id1_row = ids[0:1], ids[1:2]
    id0, id1 = to_col(id0_row), to_col(id1_row)
    earlier = iota((rows, rows), 0) < iota((rows, rows), 1)

    def rank_row(pick_row):
        hit = earlier & ((id0 == pick_row) | (id1 == pick_row))
        return jnp.sum(jnp.where(hit, 1, 0), axis=0, keepdims=True)

    group_row, group_col = id0_row // p.members, id0 // p.members
    place_row = group_row * p.block + jnp.sum(
        jnp.where(earlier & (group_col == group_row), 1, 0), axis=0, keepdims=True
    )
    offset = (my_group % p.per_chunk) * p.cap_pad

    def key_row(pick_row):
        return (pick_row % p.members) * p.message + offset + rank_row(pick_row)

    slots = groups * p.block
    chosen = iota((slots, rows), 0) == place_row
    chosen_b = onehot(chosen)
    place_col = to_col(place_row)
    spread_b = onehot(iota((rows, slots), 1) == place_col)

    def per_slot(row):
        return jnp.sum(jnp.where(chosen, row, jnp.zeros_like(row)), axis=1, keepdims=True)

    weights = rw_ref[...]
    columns = (
        (per_slot(key_row(id0_row) + 1) - 1).astype(F32),
        (per_slot(key_row(id1_row) + 1) - 1).astype(F32),
        per_slot(weights[0:1]),
        per_slot(weights[1:2]),
    )
    lane = iota((slots, 128), 1)
    meta = jnp.zeros((slots, 128), F32)
    for i, column in enumerate(columns):
        meta = jnp.where(lane == i, column, meta)
    for g in range(groups):
        meta_out[g] = meta[g * p.block : (g + 1) * p.block]

    pl.semaphore_wait(barrier, greeted)
    halo_copies = [
        remote(mix.at[pl.ds(local_rows - HALO, HALO)], halo, halo_send.at[0], halo_recv.at[0], {"sp": ahead, "tp": tp}),
        remote(doc_ref, halo_doc, halo_send.at[1], halo_recv.at[1], {"sp": ahead, "tp": tp}),
    ]
    loads[0].wait()

    @pl.when(sp < p.sp - 1)
    def _():
        for copy in halo_copies:
            copy.start()

    @pl.when(sp == 0)
    def _():
        halo[...] = jnp.zeros_like(halo)
        halo_doc[...] = jnp.zeros_like(halo_doc)


    doc_row = doc_ref[...]
    doc_col = to_col(doc_row)
    reach = jnp.left_shift(jnp.int32(2), tp)
    gap = iota((local_rows, local_rows), 0) - iota((local_rows, local_rows), 1)
    near = (doc_col == doc_row) & (gap >= 0) & (gap < reach)
    count = jnp.sum(jnp.where(near, 1.0, 0.0), axis=1, keepdims=True)
    mix_value = mix[...]
    running = jnp.dot(onehot(near), mix_value, preferred_element_type=F32)

    meta_copies = []
    for off in range(groups):
        g = nearest[off]
        if off == 0:
            copy = pltpu.make_async_copy(meta_out.at[g], meta_in.at[my_group], m_recv.at[my_group])
        else:
            copy = remote(meta_out.at[g], meta_in.at[my_group], m_send.at[g], m_recv.at[my_group], relay(g))
        copy.start()
        meta_copies.append(copy)

    @pl.when(sp > 0)
    def _():
        for copy in halo_copies:
            copy.wait_recv()

    back_gap = iota((HALO, HALO), 0) + HALO - iota((HALO, HALO), 1)
    first_reach = jnp.where(sp > 0, reach, 0)
    back = (doc_col[:HALO] == halo_doc[...][:, local_rows - HALO :]) & (back_gap < first_reach)
    head = running[:HALO] + jnp.dot(onehot(back), halo[...], preferred_element_type=F32)
    head_count = count[:HALO] + jnp.sum(jnp.where(back, 1.0, 0.0), axis=1, keepdims=True)
    running = jnp.concatenate([head, running[HALO:]], axis=0)
    count = jnp.concatenate([head_count, count[HALO:]], axis=0)
    mixed = (running / count - mix_value.astype(F32)).astype(BF16)
    loads[1].wait()
    grouped = (jnp.dot(mixed, gw[...], preferred_element_type=F32) * scale_ref[...].reshape(1, -1)).astype(BF16)
    for i in range(p.tp):
        grp[i] = grouped[i * rows : (i + 1) * rows]

    send_rows = jnp.concatenate([grp[(flip + 2 * j) % p.tp] for j in range(half)], axis=0)
    keep_rows = jnp.concatenate([grp[(tp + 2 * j) % p.tp] for j in range(half)], axis=0)
    loads[2].wait()
    first_hops = {}
    for h in range(parts):
        weight = ow[:, h * piece : (h + 1) * piece]
        product = jnp.dot(send_rows, weight, preferred_element_type=F32).astype(BF16)
        for j in reversed(range(half)):
            s1[j, h] = product[j * rows : (j + 1) * rows]
            copy = remote(s1.at[j, h], r1.at[j, h], s1_send.at[j, h], s1_recv.at[j, h], {"tp": flip})
            copy.start()
            first_hops[j, h] = copy
        kept = jnp.dot(keep_rows, weight, preferred_element_type=F32)
        for j in range(half):
            keep[j, h] = kept[j * rows : (j + 1) * rows]
    for load in loads[4:]:
        load.start()
    second_hops = {}
    for h in range(parts):
        for j in range(1, half):
            first_hops[j, h].wait_recv()
            s2[j, h] = (keep[j, h] + r1[j, h].astype(F32)).astype(BF16)
            copy = remote(
                s2.at[j, h], r2.at[j, h], s2_send.at[j, h], s2_recv.at[j, h], {"tp": (tp + 2 * j) % p.tp}
            )
            copy.start()
            second_hops[j, h] = copy

    for off in range(groups):
        b = nearest[off]
        if off == 0:
            meta_copies[0].wait()
        else:
            remote(meta_out.at[b], meta_in.at[b], m_send.at[b], m_recv.at[b], relay(b)).wait_recv()
    span_rows = p.per_chunk * p.block
    for k in range(p.chunks):
        info = jnp.concatenate([meta_in[k * p.per_chunk + i] for i in range(p.per_chunk)], axis=0)
        k0, k1 = info[:, 0:1], info[:, 1:2]
        k0_row, k1_row = to_row(k0).astype(I32), to_row(k1).astype(I32)
        target = iota((p.served, span_rows), 0)
        amat[k] = onehot((target == k0_row) | (target == k1_row))
        source = iota((span_rows, p.served), 1)
        combine = jnp.where(source == k0.astype(I32), info[:, 2:3], 0.0) + jnp.where(
            source == k1.astype(I32), info[:, 3:4], 0.0
        )
        high = combine.astype(BF16)
        chi[k] = high
        clo[k] = (combine - high.astype(F32)).astype(BF16)

    loads[3].wait()
    total = jnp.zeros((rows, 1), F32)
    for h in range(parts):
        cut = slice(h * piece, (h + 1) * piece)
        first_hops[0, h].wait_recv()
        summed = keep[0, h] + r1[0, h].astype(F32)
        for j in range(1, half):
            second_hops[j, h].wait_recv()
            summed = summed + r2[j, h].astype(F32)
        stream = (resid[:, cut].astype(F32) + summed).astype(BF16)
        stream_f = stream.astype(F32)
        stream_f32[:, cut] = stream_f
        total = total + jnp.sum(stream_f * stream_f, axis=1, keepdims=True)
    normed = (stream_f32[...] * lax.rsqrt(total / d + 1e-06) * gain_ref[...]).astype(BF16)

    gathered = jnp.dot(chosen_b, normed, preferred_element_type=F32).astype(BF16)
    for g in range(groups):
        zb[g] = gathered[g * p.block : (g + 1) * p.block]
    z_copies = []
    for off in range(groups):
        g = nearest[off]
        if off == 0:
            copy = pltpu.make_async_copy(zb.at[g], zin.at[my_group], z_recv.at[my_group])
        else:
            copy = remote(zb.at[g], zin.at[my_group], z_send.at[g], z_recv.at[my_group], relay(g))
        copy.start()
        z_copies.append(copy)

    if p.chunks == groups:
        order = [[off] for off in range(groups)]
    else:
        order = [list(range(groups))]

    x_copies, b_copies, f_copies = [], [], []

    def forward(offs):
        k = nearest[offs[0]] if p.chunks > 1 else 0
        for off in offs:
            b = nearest[off]
            if off == 0:
                z_copies[0].wait()
            else:
                remote(zb.at[b], zin.at[b], z_send.at[b], z_recv.at[b], relay(b)).wait_recv()
        if p.chunks > 1:
            source = zin[k]
        else:
            source = jnp.concatenate([zin[i] for i in range(groups)], axis=0)
        picked = jnp.dot(amat[k], source, preferred_element_type=F32).astype(BF16)
        for e in range(p.members):
            xout[k, e] = picked[e * p.message : (e + 1) * p.message]
        for step in range(p.members):
            e = (me + step) % p.members
            if step == 0:
                copy = pltpu.make_async_copy(xout.at[k, e], xin.at[k, me], x_recv.at[k, me])
            else:
                copy = remote(xout.at[k, e], xin.at[k, me], x_send.at[k, e], x_recv.at[k, me], member(e))
            copy.start()
            x_copies.append((step, copy))

    def serve(n, offs):
        k = nearest[offs[0]] if p.chunks > 1 else 0
        for step in range(p.members):
            e = (me + step) % p.members
            if step == 0:
                x_copies[n * p.members][1].wait()
            else:
                remote(xout.at[k, e], xin.at[k, e], x_send.at[k, e], x_recv.at[k, e], member(e)).wait_recv()
        if n == 0:
            for i in (4, 5, 6):
                loads[i].wait()
        flat = jnp.concatenate([xin[k, e] for e in range(p.members)], axis=0)
        gate_part = jnp.dot(flat, wg[...], preferred_element_type=F32)
        up_part = jnp.dot(flat, wu[...], preferred_element_type=F32)
        hidden = (gate_part * jax.nn.sigmoid(gate_part) * up_part).astype(BF16)
        answer = jnp.dot(hidden, wd[...], preferred_element_type=F32).astype(BF16)
        for e in range(p.members):
            ans[k, e] = answer[e * p.message : (e + 1) * p.message]
        for step in range(p.members):
            e = (me + step) % p.members
            if step == 0:
                copy = pltpu.make_async_copy(ans.at[k, e], ret.at[k, me], b_recv.at[k, me])
            else:
                copy = remote(ans.at[k, e], ret.at[k, me], b_send.at[k, e], b_recv.at[k, me], member(e))
            copy.start()
            b_copies.append((step, copy))

    def collect(n, offs):
        k = nearest[offs[0]] if p.chunks > 1 else 0
        for step in range(p.members):
            e = (me + step) % p.members
            if step == 0:
                b_copies[n * p.members][1].wait()
            else:
                remote(ans.at[k, e], ret.at[k, e], b_send.at[k, e], b_recv.at[k, e], member(e)).wait_recv()
        flat = jnp.concatenate([ret[k, e] for e in range(p.members)], axis=0)
        joined = jnp.dot(chi[k], flat, preferred_element_type=F32) + jnp.dot(clo[k], flat, preferred_element_type=F32)
        joined = joined.astype(BF16)
        if p.chunks > 1:
            zo[k] = joined
        else:
            for i in range(groups):
                zo[i] = joined[i * p.block : (i + 1) * p.block]
        for off in offs:
            b = nearest[off]
            if off == 0:
                copy = pltpu.make_async_copy(zo.at[b], fin.at[my_group], f_recv.at[my_group])
            else:
                copy = remote(zo.at[b], fin.at[my_group], f_send.at[b], f_recv.at[my_group], relay(b))
            copy.start()
            f_copies.append((off, copy))

    count_chunks = len(order)
    forward(order[0])
    for n in range(count_chunks):
        if n + 1 < count_chunks:
            forward(order[n + 1])
        serve(n, order[n])
        if n >= 1:
            collect(n - 1, order[n - 1])
    collect(count_chunks - 1, order[-1])

    for off in range(groups):
        g = nearest[off]
        if off == 0:
            [copy for o, copy in f_copies if o == 0][0].wait()
        else:
            remote(zo.at[g], fin.at[g], f_send.at[g], f_recv.at[g], relay(g)).wait_recv()
    flat = jnp.concatenate([fin[g] for g in range(groups)], axis=0)
    out_ref[...] = (stream_f32[...] + jnp.dot(spread_b, flat, preferred_element_type=F32)).astype(BF16)

    @pl.when(sp < p.sp - 1)
    def _():
        for copy in halo_copies:
            copy.wait_send()

    for copy in meta_copies[1:] + list(first_hops.values()) + list(second_hops.values()) + z_copies[1:]:
        copy.wait_send()
    for step, copy in x_copies + b_copies + f_copies:
        if step:
            copy.wait_send()


def ordered(position, table):
    n = len(table)
    return [
        sum((1 - ((position - z + n) % n + n - 1) // n) * table[z][i] for z in range(n)) for i in range(n)
    ]


def by_distance(n):
    return [sorted(range(n), key=lambda k: (abs(k - z), abs(2 * k - n + 1))) for z in range(n)]


def chunk_kernel(
    p,
    mix_hbm, resid_hbm, doc_ref, gw_hbm, scale_ref, ow_hbm, gain_ref, ids_ref, rw_ref, wg_hbm, wu_hbm, wd_hbm,
    out_ref,
    mix, resid, gw, ow, wg, wu, wd,
    halo, halo_doc, grp, keep, s1, r1, s2, r2, stream_f32, meta_out, meta_in, zb, zin, amat, chi, clo,
    xout, xin, ans, ret, zo, fin,
    load_sem, halo_send, halo_recv, m_send, m_recv, s1_send, s1_recv, s2_send, s2_recv,
    z_send, z_recv, x_send, x_recv, b_send, b_recv, f_send, f_recv,
):
    sp, tp = lax.axis_index("sp"), lax.axis_index("tp")
    local_rows, width = mix.shape
    d = resid.shape[1]
    rows, groups, half, members = p.rows, p.groups, p.half, p.members
    parts, x_parts, b_parts = zb.shape[1], xout.shape[1], ans.shape[1]
    piece, x_piece, b_piece = d // parts, d // x_parts, d // b_parts
    loads = [
        pltpu.make_async_copy(src, dst, load_sem.at[i])
        for i, (src, dst) in enumerate(
            [
                (mix_hbm, mix), (gw_hbm.at[0], gw), (ow_hbm, ow), (resid_hbm, resid),
                (wg_hbm.at[0], wg), (wu_hbm.at[0], wu), (wd_hbm.at[0], wd),
            ]
        )
    ]

    my_group, lane_in_span = sp // p.span, sp % p.span
    me = lane_in_span * p.tp + tp
    flip = tp + 1 - 2 * (tp % 2)
    order = ordered(my_group, by_distance(groups))
    others = order[1:]

    def relay(group):
        return {"sp": group * p.span + lane_in_span, "tp": tp}

    def member(index):
        return {"sp": my_group * p.span + index // p.tp, "tp": index % p.tp}

    barrier = pltpu.get_barrier_semaphore()
    greeted = 0
    ahead, behind = (sp + 1) % p.sp, (sp + p.sp - 1) % p.sp
    targets = [{"sp": ahead, "tp": tp}, {"sp": behind, "tp": tp}]
    targets += [relay((my_group + off) % groups) for off in range(1, groups)]
    targets += [member((me + off) % members) for off in range(1, members)]
    for target in targets:
        pl.semaphore_signal(barrier, inc=1, device_id=target, device_id_type=MESH)
        greeted += 1
    for load in loads:
        load.start()

    def remote(src, dst, send, recv, device):
        return pltpu.make_async_remote_copy(
            src_ref=src, dst_ref=dst, send_sem=send, recv_sem=recv, device_id=device, device_id_type=MESH
        )

    doc_row = doc_ref[...]
    doc_col = to_col(doc_row)
    reach = jnp.left_shift(jnp.int32(2), tp)
    gap = iota((local_rows, local_rows), 0) - iota((local_rows, local_rows), 1)
    near = (doc_col == doc_row) & (gap >= 0) & (gap < reach)
    count = jnp.sum(jnp.where(near, 1.0, 0.0), axis=1, keepdims=True)
    near_b = onehot(near)
    loads[0].wait()
    running = jnp.dot(near_b, mix[...], preferred_element_type=F32)
    mixed = (running / count - mix[...].astype(F32)).astype(BF16)
    loads[1].wait()
    scale = scale_ref[...].reshape(1, -1)
    grouped = (jnp.dot(mixed, gw[...], preferred_element_type=F32) * scale).astype(BF16)
    for i in range(p.tp):
        grp[i] = grouped[i * rows : (i + 1) * rows]

    send_rows = jnp.concatenate([grp[(flip + 2 * j) % p.tp] for j in range(half)], axis=0)
    keep_rows = jnp.concatenate([grp[(tp + 2 * j) % p.tp] for j in range(half)], axis=0)
    loads[2].wait()
    for h in range(parts):
        weight = ow[:, h * piece : (h + 1) * piece]
        product = jnp.dot(send_rows, weight, preferred_element_type=F32).astype(BF16)
        for j in range(half):
            s1[j, h] = product[j * rows : (j + 1) * rows]
        kept = jnp.dot(keep_rows, weight, preferred_element_type=F32)
        for j in range(half):
            keep[j, h] = kept[j * rows : (j + 1) * rows]

    with jax.named_scope("barrier"):
        pl.semaphore_wait(barrier, greeted)
    halo_copies = [
        remote(mix.at[pl.ds(local_rows - HALO, HALO)], halo, halo_send.at[0], halo_recv.at[0], {"sp": ahead, "tp": tp}),
        remote(doc_ref, halo_doc, halo_send.at[1], halo_recv.at[1], {"sp": ahead, "tp": tp}),
    ]

    @pl.when(sp < p.sp - 1)
    def _():
        for copy in halo_copies:
            copy.start()

    @pl.when(sp == 0)
    def _():
        halo[...] = jnp.zeros_like(halo)
        halo_doc[...] = jnp.zeros_like(halo_doc)

    first_hops = {
        (j, h): remote(s1.at[j, h], r1.at[j, h], s1_send.at[j, h], s1_recv.at[j, h], {"tp": flip})
        for j in range(half)
        for h in range(parts)
    }
    second_hops = {
        (j, h): remote(s2.at[j, h], r2.at[j, h], s2_send.at[j, h], s2_recv.at[j, h], {"tp": (tp + 2 * j) % p.tp})
        for j in range(1, half)
        for h in range(parts)
    }

    def send_first(late):
        for j in reversed(range(half)):
            block = (flip + 2 * j) % p.tp

            @pl.when((block == 0) if late else (block > 0))
            def _():
                for h in range(parts):
                    first_hops[j, h].start()

    def send_second(late):
        for j in range(1, half):
            block = (tp + 2 * j) % p.tp

            @pl.when((block == 0) if late else (block > 0))
            def _():
                for h in range(parts):
                    with jax.named_scope("fh_wait"):
                        first_hops[j, h].wait_recv()
                    s2[j, h] = (keep[j, h] + r1[j, h].astype(F32)).astype(BF16)
                    second_hops[j, h].start()

    send_first(False)

    ids = ids_ref[...]
    id0_row, id1_row = ids[0:1], ids[1:2]
    id0, id1 = to_col(id0_row), to_col(id1_row)
    earlier = iota((rows, rows), 0) < iota((rows, rows), 1)

    def rank_row(pick_row):
        hit = earlier & ((id0 == pick_row) | (id1 == pick_row))
        return jnp.sum(jnp.where(hit, 1, 0), axis=0, keepdims=True)

    group_row, group_col = id0_row // members, id0 // members
    place_row = group_row * p.block + jnp.sum(
        jnp.where(earlier & (group_col == group_row), 1, 0), axis=0, keepdims=True
    )

    def key_row(pick_row):
        return (pick_row % members) * p.message + rank_row(pick_row)

    slots = groups * p.block
    chosen = iota((slots, rows), 0) == place_row
    chosen_b = onehot(chosen)
    place_col = to_col(place_row)
    spread_b = onehot(iota((rows, slots), 1) == place_col)

    def per_slot(row):
        return jnp.sum(jnp.where(chosen, row, jnp.zeros_like(row)), axis=1, keepdims=True)

    weights = rw_ref[...]
    columns = (
        (per_slot(key_row(id0_row) + 1) - 1).astype(F32),
        (per_slot(key_row(id1_row) + 1) - 1).astype(F32),
        per_slot(weights[0:1]),
        per_slot(weights[1:2]),
    )
    lane = iota((slots, 128), 1)
    meta = jnp.zeros((slots, 128), F32)
    for i, column in enumerate(columns):
        meta = jnp.where(lane == i, column, meta)
    for g in range(groups):
        meta_out[g] = meta[g * p.block : (g + 1) * p.block]
    meta_copies = []
    for g in others:
        copy = remote(meta_out.at[g], meta_in.at[my_group], m_send.at[g], m_recv.at[my_group], relay(g))
        copy.start()
        meta_copies.append(copy)

    send_second(False)

    @pl.when(sp > 0)
    def _():
        for copy in halo_copies:
            with jax.named_scope("halo_wait"):
                copy.wait_recv()

    back_gap = iota((HALO, HALO), 0) + HALO - iota((HALO, HALO), 1)
    first_reach = jnp.where(sp > 0, reach, 0)
    back = (doc_col[:HALO] == halo_doc[...][:, local_rows - HALO :]) & (back_gap < first_reach)
    head = running[:HALO] + jnp.dot(onehot(back), halo[...], preferred_element_type=F32)
    head_count = count[:HALO] + jnp.sum(jnp.where(back, 1.0, 0.0), axis=1, keepdims=True)
    head_mixed = (head / head_count - mix[:HALO].astype(F32)).astype(BF16)
    head_grouped = (jnp.dot(head_mixed, gw[...], preferred_element_type=F32) * scale).astype(BF16)
    head_product = jnp.dot(head_grouped, ow[...], preferred_element_type=F32)
    keep_slot = ((p.tp - tp) % p.tp) // 2
    send_slot = ((p.tp - flip) % p.tp) // 2

    @pl.when(tp % 2 == 0)
    def _():
        for h in range(parts):
            keep[keep_slot, h, :HALO] = head_product[:, h * piece : (h + 1) * piece]

    @pl.when(tp % 2 == 1)
    def _():
        for h in range(parts):
            s1[send_slot, h, :HALO] = head_product[:, h * piece : (h + 1) * piece].astype(BF16)

    send_first(True)
    send_second(True)

    def tables(k, info):
        k0, k1 = info[:, 0:1], info[:, 1:2]
        k0_row, k1_row = to_row(k0).astype(I32), to_row(k1).astype(I32)
        target = iota((p.served, p.block), 0)
        amat[k] = onehot((target == k0_row) | (target == k1_row))
        source = iota((p.block, p.served), 1)
        combine = jnp.where(source == k0.astype(I32), info[:, 2:3], 0.0) + jnp.where(
            source == k1.astype(I32), info[:, 3:4], 0.0
        )
        high = combine.astype(BF16)
        chi[k] = high
        clo[k] = (combine - high.astype(F32)).astype(BF16)

    tables(my_group, meta_out[my_group])
    for g in others:
        with jax.named_scope("m_wait"):
            remote(meta_out.at[g], meta_in.at[g], m_send.at[g], m_recv.at[g], relay(g)).wait_recv()
        tables(g, meta_in[g])

    x_copies, b_copies, f_copies, z_copies = [], [], [], []
    ratio = parts // x_parts

    def forward_part(k, part, source):
        picked = jnp.dot(amat[k], source, preferred_element_type=F32).astype(BF16)
        for e in range(members):
            xout[k, part, e] = picked[e * p.message : (e + 1) * p.message]
        for step in list(range(2, members)) + [1]:
            e = (me + step) % members
            copy = remote(
                xout.at[k, part, e], xin.at[k, part, me], x_send.at[k, part, e], x_recv.at[k, part, me], member(e)
            )
            copy.start()
            x_copies.append(copy)
        xin[k, part, me] = xout[k, part, me]

    def send_z(g, h):
        copy = remote(zb.at[g, h], zin.at[my_group, h], z_send.at[g, h], z_recv.at[my_group, h], relay(g))
        copy.start()
        z_copies.append(copy)

    loads[3].wait()
    delayed = others[2:]
    for h in range(parts):
        cut = slice(h * piece, (h + 1) * piece)
        with jax.named_scope("fh0_wait"):
            first_hops[0, h].wait_recv()
        summed = keep[0, h] + r1[0, h].astype(F32)
        for j in range(1, half):
            with jax.named_scope("sh_wait"):
                second_hops[j, h].wait_recv()
            summed = summed + r2[j, h].astype(F32)
        stream = (resid[:, cut].astype(F32) + summed).astype(BF16)
        stream_f32[:, cut] = stream.astype(F32)
        gathered = jnp.dot(chosen_b, stream, preferred_element_type=F32).astype(BF16)
        for g in range(groups):
            zb[g, h] = gathered[g * p.block : (g + 1) * p.block]
        for g in others[:2]:
            send_z(g, h)
        if h % ratio == ratio - 1:
            first = h + 1 - ratio
            source = jnp.concatenate([zb[my_group, i] for i in range(first, h + 1)], axis=1)
            forward_part(my_group, h // ratio, source)
    for g in delayed:
        for h in range(parts):
            send_z(g, h)

    def forward(k):
        for part in range(x_parts):
            for h in range(part * ratio, (part + 1) * ratio):
                with jax.named_scope("z_wait"):
                    remote(zb.at[k, h], zin.at[k, h], z_send.at[k, h], z_recv.at[k, h], relay(k)).wait_recv()
            source = jnp.concatenate([zin[k, i] for i in range(part * ratio, (part + 1) * ratio)], axis=1)
            forward_part(k, part, source)

    waited = []

    def serve(k):
        for part in range(x_parts):
            for step in range(1, members):
                e = (me + step) % members
                with jax.named_scope("x_wait"):
                    remote(
                        xout.at[k, part, e], xin.at[k, part, e], x_send.at[k, part, e], x_recv.at[k, part, e], member(e)
                    ).wait_recv()
        if not waited:
            waited.append(True)
            for i in (4, 5, 6):
                loads[i].wait()
        with jax.named_scope("expert"):
            flat = jnp.concatenate(
                [jnp.concatenate([xin[k, part, e] for e in range(members)], axis=0) for part in range(x_parts)], axis=1
            ).astype(F32)
            level = jnp.sum(flat * flat, axis=1, keepdims=True) / d
            normed = (flat * lax.rsqrt(level + 1e-06) * gain_ref[...]).astype(BF16)
            gate_part = jnp.dot(normed, wg[...], preferred_element_type=F32)
            up_part = jnp.dot(normed, wu[...], preferred_element_type=F32)
            hidden = (gate_part * jax.nn.sigmoid(gate_part) * up_part).astype(BF16)
            for part in range(b_parts):
                weight = wd[:, part * b_piece : (part + 1) * b_piece]
                answer = jnp.dot(hidden, weight, preferred_element_type=F32).astype(BF16)
                for e in range(members):
                    ans[k, part, e] = answer[e * p.message : (e + 1) * p.message]
                for step in list(range(2, members)) + [1]:
                    e = (me + step) % members
                    copy = remote(
                        ans.at[k, part, e], ret.at[k, part, me], b_send.at[k, part, e], b_recv.at[k, part, me], member(e)
                    )
                    copy.start()
                    b_copies.append(copy)
                ret[k, part, me] = ans[k, part, me]

    def collect(k, own=False):
        for part in range(b_parts):
            for step in range(1, members):
                e = (me + step) % members
                with jax.named_scope("b_wait"):
                    remote(
                        ans.at[k, part, e], ret.at[k, part, e], b_send.at[k, part, e], b_recv.at[k, part, e], member(e)
                    ).wait_recv()
            flat = jnp.concatenate([ret[k, part, e] for e in range(members)], axis=0)
            joined = jnp.dot(chi[k], flat, preferred_element_type=F32) + jnp.dot(clo[k], flat, preferred_element_type=F32)
            if own:
                fin[k, part] = joined.astype(BF16)
            else:
                zo[k, part] = joined.astype(BF16)
                copy = remote(
                    zo.at[k, part], fin.at[my_group, part], f_send.at[k, part], f_recv.at[my_group, part], relay(k)
                )
                copy.start()
                f_copies.append(copy)

    forward(others[0])
    serve(my_group)
    forward(others[1])
    serve(others[0])
    collect(my_group, own=True)
    forward(others[2])
    serve(others[1])
    collect(others[0])
    serve(others[2])
    collect(others[1])
    collect(others[2])

    for part in range(b_parts):
        for g in others:
            with jax.named_scope("f_wait"):
                remote(zo.at[g, part], fin.at[g, part], f_send.at[g, part], f_recv.at[g, part], relay(g)).wait_recv()
        cut = slice(part * b_piece, (part + 1) * b_piece)
        flat = jnp.concatenate([fin[g, part] for g in range(groups)], axis=0)
        out_ref[:, cut] = (stream_f32[:, cut] + jnp.dot(spread_b, flat, preferred_element_type=F32)).astype(BF16)

    @pl.when(sp < p.sp - 1)
    def _():
        for copy in halo_copies:
            copy.wait_send()

    for copy in meta_copies + list(first_hops.values()) + list(second_hops.values()):
        copy.wait_send()
    for copy in z_copies + x_copies + b_copies + f_copies:
        copy.wait_send()


def shards(
    sp_size,
    tp_size,
    mix_in,
    resid_in,
    doc_ids,
    group_weight,
    pool_scale,
    out_weight,
    norm_gain,
    expert_ids,
    route_weights,
    w_gate,
    w_up,
    w_down,
):
    local_rows, width = mix_in.shape
    rows, d = resid_in.shape
    ff = w_gate.shape[2]
    p = Plan(sp_size, tp_size, rows)
    g, half, parts = p.groups, p.half, p.parts
    vmem = pl.BlockSpec(memory_space=pltpu.VMEM)
    hbm = pl.BlockSpec(memory_space=pl.ANY)
    dma = pltpu.SemaphoreType.DMA
    common = [
        pltpu.VMEM((local_rows, width), BF16),
        pltpu.VMEM((rows, d), BF16),
        pltpu.VMEM(group_weight.shape[1:], BF16),
        pltpu.VMEM(out_weight.shape, BF16),
        pltpu.VMEM(w_gate.shape[1:], BF16),
        pltpu.VMEM(w_up.shape[1:], BF16),
        pltpu.VMEM(w_down.shape[1:], BF16),
        pltpu.VMEM((HALO, width), BF16),
        pltpu.VMEM((1, local_rows), I32),
        pltpu.VMEM((tp_size, rows, width), BF16),
    ]
    stream_and_meta = [
        pltpu.VMEM((rows, d), F32),
        pltpu.VMEM((g, p.block, 128), F32),
        pltpu.VMEM((g, p.block, 128), F32),
    ]
    if p.chunks == g and p.groups == 4:
        body = chunk_kernel
        parts, x_parts, b_parts = 4, 2, 2
        exchange = (half, parts, rows, d // parts)
        slots = (g, parts, p.block, d // parts)
        sent = (g, x_parts, p.members, p.message, d // x_parts)
        answers = (g, b_parts, p.members, p.message, d // b_parts)
        final = (g, b_parts, p.block, d // b_parts)
        scratch = common + [
            pltpu.VMEM(exchange, F32),
            pltpu.VMEM(exchange, BF16),
            pltpu.VMEM(exchange, BF16),
            pltpu.VMEM(exchange, BF16),
            pltpu.VMEM(exchange, BF16),
        ] + stream_and_meta + [
            pltpu.VMEM(slots, BF16),
            pltpu.VMEM(slots, BF16),
            pltpu.VMEM((g, p.served, p.block), BF16),
            pltpu.VMEM((g, p.block, p.served), BF16),
            pltpu.VMEM((g, p.block, p.served), BF16),
            pltpu.VMEM(sent, BF16),
            pltpu.VMEM(sent, BF16),
            pltpu.VMEM(answers, BF16),
            pltpu.VMEM(answers, BF16),
            pltpu.VMEM(final, BF16),
            pltpu.VMEM(final, BF16),
            dma((7,)),
            dma((2,)), dma((2,)),
            dma((g,)), dma((g,)),
            dma((half, parts)), dma((half, parts)),
            dma((half, parts)), dma((half, parts)),
            dma((g, parts)), dma((g, parts)),
            dma((g, x_parts, p.members)), dma((g, x_parts, p.members)),
            dma((g, b_parts, p.members)), dma((g, b_parts, p.members)),
            dma((g, b_parts)), dma((g, b_parts)),
        ]
    else:
        body = kernel
        span_rows = p.per_chunk * p.block
        messages = (p.chunks, p.members, p.message, d)
        exchange = (half, parts, rows, d // parts)
        scratch = common + [
            pltpu.VMEM(exchange, F32),
            pltpu.VMEM(exchange, BF16),
            pltpu.VMEM(exchange, BF16),
            pltpu.VMEM(exchange, BF16),
            pltpu.VMEM(exchange, BF16),
        ] + stream_and_meta + [
            pltpu.VMEM((g, p.block, d), BF16),
            pltpu.VMEM((g, p.block, d), BF16),
            pltpu.VMEM((p.chunks, p.served, span_rows), BF16),
            pltpu.VMEM((p.chunks, span_rows, p.served), BF16),
            pltpu.VMEM((p.chunks, span_rows, p.served), BF16),
            pltpu.VMEM(messages, BF16),
            pltpu.VMEM(messages, BF16),
            pltpu.VMEM(messages, BF16),
            pltpu.VMEM(messages, BF16),
            pltpu.VMEM((g, p.block, d), BF16),
            pltpu.VMEM((g, p.block, d), BF16),
            dma((7,)),
            dma((2,)), dma((2,)),
            dma((g,)), dma((g,)),
            dma((half, parts)), dma((half, parts)),
            dma((half, parts)), dma((half, parts)),
            dma((g,)), dma((g,)),
            dma((p.chunks, p.members)), dma((p.chunks, p.members)),
            dma((p.chunks, p.members)), dma((p.chunks, p.members)),
            dma((g,)), dma((g,)),
        ]
    return pl.pallas_call(
        functools.partial(body, p),
        out_shape=jax.ShapeDtypeStruct((rows, d), BF16),
        in_specs=[hbm, hbm, vmem, hbm, vmem, hbm, vmem, vmem, vmem, hbm, hbm, hbm],
        out_specs=vmem,
        scratch_shapes=scratch,
        compiler_params=pltpu.CompilerParams(
            collective_id=0, has_side_effects=True, vmem_limit_bytes=56 * 1024 * 1024
        ),
    )(
        mix_in, resid_in, doc_ids.reshape(1, -1), group_weight, pool_scale, out_weight,
        norm_gain.reshape(1, -1), expert_ids.T, route_weights.T, w_gate, w_up, w_down,
    )


def solution(mesh):
    return jax.shard_map(
        functools.partial(shards, mesh.shape["sp"], mesh.shape["tp"]),
        mesh=mesh,
        in_specs=(
            P(("grp", "sp"), "tp"),
            P(("grp", "sp", "tp"), None),
            P(("grp", "sp")),
            P("tp", None, None),
            P("tp"),
            P("tp", None),
            P(),
            P(("grp", "sp", "tp"), None),
            P(("grp", "sp", "tp"), None),
            P(("sp", "tp"), None, None),
            P(("sp", "tp"), None, None),
            P(("sp", "tp"), None, None),
        ),
        out_specs=P(("grp", "sp", "tp"), None),
        check_vma=False,
    )
```

```python
import functools

import jax
import jax.numpy as jnp
from jax import lax
from jax.experimental import pallas as pl
from jax.experimental.pallas import tpu as pltpu
from jax.sharding import PartitionSpec as P

HALO = 16
TOP_K = 2
EXPERT_GROUPS = 4
PARTS = (4, 4, 2)
SEQUENCE = "Fn Fm Ff Sf Sm Cf Sn Cm So Cn Co"
Z_ORDER = ["00 10", "01 11", "02 12", "03 13 20 21 22 23"]
TABLE = [[0, 1, 2, 3], [1, 2, 0, 3], [2, 1, 3, 0], [3, 2, 1, 0]]
MESH = pl.DeviceIdType.MESH
F32 = jnp.float32
BF16 = jnp.bfloat16
I32 = jnp.int32


def iota(shape, dim):
    return lax.broadcasted_iota(I32, shape, dim)


def to_row(col):
    n = col.shape[0]
    eye = iota((n, n), 0) == iota((n, n), 1)
    return jnp.sum(jnp.where(eye, col, jnp.zeros_like(col)), axis=0, keepdims=True)


def to_col(row):
    n = row.shape[1]
    eye = iota((n, n), 0) == iota((n, n), 1)
    return jnp.sum(jnp.where(eye, row, jnp.zeros_like(row)), axis=1, keepdims=True)


def onehot(mask):
    return jnp.where(mask, 1.0, 0.0).astype(BF16)


class Plan:
    def __init__(self, sp_size, tp_size, token_rows):
        self.sp, self.tp, self.rows = sp_size, tp_size, token_rows
        self.experts = sp_size * tp_size
        self.groups = EXPERT_GROUPS
        self.span = sp_size // self.groups
        self.members = self.span * tp_size
        self.cap = max(TOP_K, 4 * token_rows // self.experts)
        self.block = min(token_rows, self.cap * self.members // TOP_K)
        if self.cap % 16 == 0:
            self.chunks, self.cap_pad = self.groups, self.cap
        else:
            self.chunks = 1
            whole = -(-self.cap * self.groups // 16) * 16
            self.cap_pad = whole // self.groups
        self.per_chunk = self.groups // self.chunks
        self.message = self.per_chunk * self.cap_pad
        self.served = self.members * self.message
        self.half = tp_size // 2
        self.parts = 2


def kernel(
    p,
    mix_hbm, resid_hbm, doc_ref, gw_hbm, scale_ref, ow_hbm, gain_ref, ids_ref, rw_ref, wg_hbm, wu_hbm, wd_hbm,
    out_ref,
    mix, resid, gw, ow, wg, wu, wd,
    halo, halo_doc, grp, keep, s1, r1, s2, r2, stream_f32, meta_out, meta_in, zb, zin, amat, chi, clo,
    xout, xin, ans, ret, zo, fin,
    load_sem, halo_send, halo_recv, m_send, m_recv, s1_send, s1_recv, s2_send, s2_recv,
    z_send, z_recv, x_send, x_recv, b_send, b_recv, f_send, f_recv,
):
    sp, tp = lax.axis_index("sp"), lax.axis_index("tp")
    local_rows, width = mix.shape
    d = resid.shape[1]
    rows, groups, half, parts = p.rows, p.groups, p.half, p.parts
    piece = d // parts
    loads = [
        pltpu.make_async_copy(src, dst, load_sem.at[i])
        for i, (src, dst) in enumerate(
            [
                (mix_hbm, mix), (gw_hbm.at[0], gw), (ow_hbm, ow), (resid_hbm, resid),
                (wg_hbm.at[0], wg), (wu_hbm.at[0], wu), (wd_hbm.at[0], wd),
            ]
        )
    ]
    for load in loads[:4]:
        load.start()

    my_group, lane_in_span = sp // p.span, sp % p.span
    me = lane_in_span * p.tp + tp
    flip = tp + 1 - 2 * (tp % 2)

    steps = [0] + sorted(range(1, groups), key=lambda step: min(step, groups - step))
    nearest = [(my_group + step) % groups for step in steps]

    def relay(group):
        return {"sp": group * p.span + lane_in_span, "tp": tp}

    def member(index):
        return {"sp": my_group * p.span + index // p.tp, "tp": index % p.tp}

    barrier = pltpu.get_barrier_semaphore()
    greeted = 0
    ahead, behind = (sp + 1) % p.sp, (sp + p.sp - 1) % p.sp
    targets = [{"sp": ahead, "tp": tp}, {"sp": behind, "tp": tp}]
    targets += [relay((my_group + off) % groups) for off in range(1, groups)]
    targets += [member((me + off) % p.members) for off in range(1, p.members)]
    for target in targets:
        pl.semaphore_signal(barrier, inc=1, device_id=target, device_id_type=MESH)
        greeted += 1

    def remote(src, dst, send, recv, device):
        return pltpu.make_async_remote_copy(
            src_ref=src, dst_ref=dst, send_sem=send, recv_sem=recv, device_id=device, device_id_type=MESH
        )

    ids = ids_ref[...]
    id0_row, id1_row = ids[0:1], ids[1:2]
    id0, id1 = to_col(id0_row), to_col(id1_row)
    earlier = iota((rows, rows), 0) < iota((rows, rows), 1)

    def rank_row(pick_row):
        hit = earlier & ((id0 == pick_row) | (id1 == pick_row))
        return jnp.sum(jnp.where(hit, 1, 0), axis=0, keepdims=True)

    group_row, group_col = id0_row // p.members, id0 // p.members
    place_row = group_row * p.block + jnp.sum(
        jnp.where(earlier & (group_col == group_row), 1, 0), axis=0, keepdims=True
    )
    offset = (my_group % p.per_chunk) * p.cap_pad

    def key_row(pick_row):
        return (pick_row % p.members) * p.message + offset + rank_row(pick_row)

    slots = groups * p.block
    chosen = iota((slots, rows), 0) == place_row
    chosen_b = onehot(chosen)
    place_col = to_col(place_row)
    spread_b = onehot(iota((rows, slots), 1) == place_col)

    def per_slot(row):
        return jnp.sum(jnp.where(chosen, row, jnp.zeros_like(row)), axis=1, keepdims=True)

    weights = rw_ref[...]
    columns = (
        (per_slot(key_row(id0_row) + 1) - 1).astype(F32),
        (per_slot(key_row(id1_row) + 1) - 1).astype(F32),
        per_slot(weights[0:1]),
        per_slot(weights[1:2]),
    )
    lane = iota((slots, 128), 1)
    meta = jnp.zeros((slots, 128), F32)
    for i, column in enumerate(columns):
        meta = jnp.where(lane == i, column, meta)
    for g in range(groups):
        meta_out[g] = meta[g * p.block : (g + 1) * p.block]

    pl.semaphore_wait(barrier, greeted)
    halo_copies = [
        remote(mix.at[pl.ds(local_rows - HALO, HALO)], halo, halo_send.at[0], halo_recv.at[0], {"sp": ahead, "tp": tp}),
        remote(doc_ref, halo_doc, halo_send.at[1], halo_recv.at[1], {"sp": ahead, "tp": tp}),
    ]
    loads[0].wait()

    @pl.when(sp < p.sp - 1)
    def _():
        for copy in halo_copies:
            copy.start()

    @pl.when(sp == 0)
    def _():
        halo[...] = jnp.zeros_like(halo)
        halo_doc[...] = jnp.zeros_like(halo_doc)


    doc_row = doc_ref[...]
    doc_col = to_col(doc_row)
    reach = jnp.left_shift(jnp.int32(2), tp)
    gap = iota((local_rows, local_rows), 0) - iota((local_rows, local_rows), 1)
    near = (doc_col == doc_row) & (gap >= 0) & (gap < reach)
    count = jnp.sum(jnp.where(near, 1.0, 0.0), axis=1, keepdims=True)
    mix_value = mix[...]
    running = jnp.dot(onehot(near), mix_value, preferred_element_type=F32)

    meta_copies = []
    for off in range(groups):
        g = nearest[off]
        if off == 0:
            copy = pltpu.make_async_copy(meta_out.at[g], meta_in.at[my_group], m_recv.at[my_group])
        else:
            copy = remote(meta_out.at[g], meta_in.at[my_group], m_send.at[g], m_recv.at[my_group], relay(g))
        copy.start()
        meta_copies.append(copy)

    @pl.when(sp > 0)
    def _():
        for copy in halo_copies:
            copy.wait_recv()

    back_gap = iota((HALO, HALO), 0) + HALO - iota((HALO, HALO), 1)
    first_reach = jnp.where(sp > 0, reach, 0)
    back = (doc_col[:HALO] == halo_doc[...][:, local_rows - HALO :]) & (back_gap < first_reach)
    head = running[:HALO] + jnp.dot(onehot(back), halo[...], preferred_element_type=F32)
    head_count = count[:HALO] + jnp.sum(jnp.where(back, 1.0, 0.0), axis=1, keepdims=True)
    running = jnp.concatenate([head, running[HALO:]], axis=0)
    count = jnp.concatenate([head_count, count[HALO:]], axis=0)
    mixed = (running / count - mix_value.astype(F32)).astype(BF16)
    loads[1].wait()
    grouped = (jnp.dot(mixed, gw[...], preferred_element_type=F32) * scale_ref[...].reshape(1, -1)).astype(BF16)
    for i in range(p.tp):
        grp[i] = grouped[i * rows : (i + 1) * rows]

    send_rows = jnp.concatenate([grp[(flip + 2 * j) % p.tp] for j in range(half)], axis=0)
    keep_rows = jnp.concatenate([grp[(tp + 2 * j) % p.tp] for j in range(half)], axis=0)
    loads[2].wait()
    first_hops = {}
    for h in range(parts):
        weight = ow[:, h * piece : (h + 1) * piece]
        product = jnp.dot(send_rows, weight, preferred_element_type=F32).astype(BF16)
        for j in reversed(range(half)):
            s1[j, h] = product[j * rows : (j + 1) * rows]
            copy = remote(s1.at[j, h], r1.at[j, h], s1_send.at[j, h], s1_recv.at[j, h], {"tp": flip})
            copy.start()
            first_hops[j, h] = copy
        kept = jnp.dot(keep_rows, weight, preferred_element_type=F32)
        for j in range(half):
            keep[j, h] = kept[j * rows : (j + 1) * rows]
    for load in loads[4:]:
        load.start()
    second_hops = {}
    for h in range(parts):
        for j in range(1, half):
            first_hops[j, h].wait_recv()
            s2[j, h] = (keep[j, h] + r1[j, h].astype(F32)).astype(BF16)
            copy = remote(
                s2.at[j, h], r2.at[j, h], s2_send.at[j, h], s2_recv.at[j, h], {"tp": (tp + 2 * j) % p.tp}
            )
            copy.start()
            second_hops[j, h] = copy

    for off in range(groups):
        b = nearest[off]
        if off == 0:
            meta_copies[0].wait()
        else:
            remote(meta_out.at[b], meta_in.at[b], m_send.at[b], m_recv.at[b], relay(b)).wait_recv()
    span_rows = p.per_chunk * p.block
    for k in range(p.chunks):
        info = jnp.concatenate([meta_in[k * p.per_chunk + i] for i in range(p.per_chunk)], axis=0)
        k0, k1 = info[:, 0:1], info[:, 1:2]
        k0_row, k1_row = to_row(k0).astype(I32), to_row(k1).astype(I32)
        target = iota((p.served, span_rows), 0)
        amat[k] = onehot((target == k0_row) | (target == k1_row))
        source = iota((span_rows, p.served), 1)
        combine = jnp.where(source == k0.astype(I32), info[:, 2:3], 0.0) + jnp.where(
            source == k1.astype(I32), info[:, 3:4], 0.0
        )
        high = combine.astype(BF16)
        chi[k] = high
        clo[k] = (combine - high.astype(F32)).astype(BF16)

    loads[3].wait()
    total = jnp.zeros((rows, 1), F32)
    for h in range(parts):
        cut = slice(h * piece, (h + 1) * piece)
        first_hops[0, h].wait_recv()
        summed = keep[0, h] + r1[0, h].astype(F32)
        for j in range(1, half):
            second_hops[j, h].wait_recv()
            summed = summed + r2[j, h].astype(F32)
        stream = (resid[:, cut].astype(F32) + summed).astype(BF16)
        stream_f = stream.astype(F32)
        stream_f32[:, cut] = stream_f
        total = total + jnp.sum(stream_f * stream_f, axis=1, keepdims=True)
    normed = (stream_f32[...] * lax.rsqrt(total / d + 1e-06) * gain_ref[...]).astype(BF16)

    gathered = jnp.dot(chosen_b, normed, preferred_element_type=F32).astype(BF16)
    for g in range(groups):
        zb[g] = gathered[g * p.block : (g + 1) * p.block]
    z_copies = []
    for off in range(groups):
        g = nearest[off]
        if off == 0:
            copy = pltpu.make_async_copy(zb.at[g], zin.at[my_group], z_recv.at[my_group])
        else:
            copy = remote(zb.at[g], zin.at[my_group], z_send.at[g], z_recv.at[my_group], relay(g))
        copy.start()
        z_copies.append(copy)

    if p.chunks == groups:
        order = [[off] for off in range(groups)]
    else:
        order = [list(range(groups))]

    x_copies, b_copies, f_copies = [], [], []

    def forward(offs):
        k = nearest[offs[0]] if p.chunks > 1 else 0
        for off in offs:
            b = nearest[off]
            if off == 0:
                z_copies[0].wait()
            else:
                remote(zb.at[b], zin.at[b], z_send.at[b], z_recv.at[b], relay(b)).wait_recv()
        if p.chunks > 1:
            source = zin[k]
        else:
            source = jnp.concatenate([zin[i] for i in range(groups)], axis=0)
        picked = jnp.dot(amat[k], source, preferred_element_type=F32).astype(BF16)
        for e in range(p.members):
            xout[k, e] = picked[e * p.message : (e + 1) * p.message]
        for step in range(p.members):
            e = (me + step) % p.members
            if step == 0:
                copy = pltpu.make_async_copy(xout.at[k, e], xin.at[k, me], x_recv.at[k, me])
            else:
                copy = remote(xout.at[k, e], xin.at[k, me], x_send.at[k, e], x_recv.at[k, me], member(e))
            copy.start()
            x_copies.append((step, copy))

    def serve(n, offs):
        k = nearest[offs[0]] if p.chunks > 1 else 0
        for step in range(p.members):
            e = (me + step) % p.members
            if step == 0:
                x_copies[n * p.members][1].wait()
            else:
                remote(xout.at[k, e], xin.at[k, e], x_send.at[k, e], x_recv.at[k, e], member(e)).wait_recv()
        if n == 0:
            for i in (4, 5, 6):
                loads[i].wait()
        flat = jnp.concatenate([xin[k, e] for e in range(p.members)], axis=0)
        gate_part = jnp.dot(flat, wg[...], preferred_element_type=F32)
        up_part = jnp.dot(flat, wu[...], preferred_element_type=F32)
        hidden = (gate_part * jax.nn.sigmoid(gate_part) * up_part).astype(BF16)
        answer = jnp.dot(hidden, wd[...], preferred_element_type=F32).astype(BF16)
        for e in range(p.members):
            ans[k, e] = answer[e * p.message : (e + 1) * p.message]
        for step in range(p.members):
            e = (me + step) % p.members
            if step == 0:
                copy = pltpu.make_async_copy(ans.at[k, e], ret.at[k, me], b_recv.at[k, me])
            else:
                copy = remote(ans.at[k, e], ret.at[k, me], b_send.at[k, e], b_recv.at[k, me], member(e))
            copy.start()
            b_copies.append((step, copy))

    def collect(n, offs):
        k = nearest[offs[0]] if p.chunks > 1 else 0
        for step in range(p.members):
            e = (me + step) % p.members
            if step == 0:
                b_copies[n * p.members][1].wait()
            else:
                remote(ans.at[k, e], ret.at[k, e], b_send.at[k, e], b_recv.at[k, e], member(e)).wait_recv()
        flat = jnp.concatenate([ret[k, e] for e in range(p.members)], axis=0)
        joined = jnp.dot(chi[k], flat, preferred_element_type=F32) + jnp.dot(clo[k], flat, preferred_element_type=F32)
        joined = joined.astype(BF16)
        if p.chunks > 1:
            zo[k] = joined
        else:
            for i in range(groups):
                zo[i] = joined[i * p.block : (i + 1) * p.block]
        for off in offs:
            b = nearest[off]
            if off == 0:
                copy = pltpu.make_async_copy(zo.at[b], fin.at[my_group], f_recv.at[my_group])
            else:
                copy = remote(zo.at[b], fin.at[my_group], f_send.at[b], f_recv.at[my_group], relay(b))
            copy.start()
            f_copies.append((off, copy))

    count_chunks = len(order)
    forward(order[0])
    for n in range(count_chunks):
        if n + 1 < count_chunks:
            forward(order[n + 1])
        serve(n, order[n])
        if n >= 1:
            collect(n - 1, order[n - 1])
    collect(count_chunks - 1, order[-1])

    for off in range(groups):
        g = nearest[off]
        if off == 0:
            [copy for o, copy in f_copies if o == 0][0].wait()
        else:
            remote(zo.at[g], fin.at[g], f_send.at[g], f_recv.at[g], relay(g)).wait_recv()
    flat = jnp.concatenate([fin[g] for g in range(groups)], axis=0)
    out_ref[...] = (stream_f32[...] + jnp.dot(spread_b, flat, preferred_element_type=F32)).astype(BF16)

    @pl.when(sp < p.sp - 1)
    def _():
        for copy in halo_copies:
            copy.wait_send()

    for copy in meta_copies[1:] + list(first_hops.values()) + list(second_hops.values()) + z_copies[1:]:
        copy.wait_send()
    for step, copy in x_copies + b_copies + f_copies:
        if step:
            copy.wait_send()


def ordered(position, table):
    n = len(table)
    return [
        sum((1 - ((position - z + n) % n + n - 1) // n) * table[z][i] for z in range(n)) for i in range(n)
    ]


def by_distance(n):
    return [sorted(range(n), key=lambda k: (abs(k - z), abs(2 * k - n + 1))) for z in range(n)]


def chunk_kernel(
    p,
    mix_hbm, resid_hbm, doc_ref, gw_hbm, scale_ref, ow_hbm, gain_ref, ids_ref, rw_ref, wg_hbm, wu_hbm, wd_hbm,
    out_ref,
    mix, resid, gw, ow, wg, wu, wd,
    halo, halo_doc, grp, keep, s1, r1, s2, r2, stream_f32, meta_out, meta_in, zb, zin, amat, chi, clo,
    xout, xin, ans, ret, zo, fin,
    load_sem, sent, halo_send, halo_recv, m_recv, s1_recv, s2_recv, z_recv, x_recv, b_recv, f_recv,
):
    sp, tp = lax.axis_index("sp"), lax.axis_index("tp")
    local_rows, width = mix.shape
    d = resid.shape[1]
    rows, groups, half, members = p.rows, p.groups, p.half, p.members
    parts, x_parts, b_parts = zb.shape[1], xout.shape[1], ans.shape[1]
    piece, x_piece, b_piece = d // parts, d // x_parts, d // b_parts
    loads = [
        pltpu.make_async_copy(src, dst, load_sem.at[i])
        for i, (src, dst) in enumerate(
            [
                (mix_hbm, mix), (gw_hbm.at[0], gw), (ow_hbm, ow), (resid_hbm, resid),
                (wg_hbm.at[0], wg), (wu_hbm.at[0], wu), (wd_hbm.at[0], wd),
            ]
        )
    ]

    my_group, lane_in_span = sp // p.span, sp % p.span
    me = lane_in_span * p.tp + tp
    flip = tp + 1 - 2 * (tp % 2)
    order = ordered(my_group, TABLE)
    others = order[1:]

    def relay(group):
        return {"sp": group * p.span + lane_in_span, "tp": tp}

    def member(index):
        return {"sp": my_group * p.span + index // p.tp, "tp": index % p.tp}

    barrier = pltpu.get_barrier_semaphore()
    greeted = 0
    ahead, behind = (sp + 1) % p.sp, (sp + p.sp - 1) % p.sp
    targets = [{"sp": ahead, "tp": tp}, {"sp": behind, "tp": tp}]
    targets += [relay((my_group + off) % groups) for off in range(1, groups)]
    targets += [member((me + off) % members) for off in range(1, members)]
    for target in targets:
        pl.semaphore_signal(barrier, inc=1, device_id=target, device_id_type=MESH)
        greeted += 1
    for load in loads:
        load.start()

    def remote(src, dst, send, recv, device):
        return pltpu.make_async_remote_copy(
            src_ref=src, dst_ref=dst, send_sem=send, recv_sem=recv, device_id=device, device_id_type=MESH
        )

    doc_row = doc_ref[...]
    doc_col = to_col(doc_row)
    reach = jnp.left_shift(jnp.int32(2), tp)
    gap = iota((local_rows, local_rows), 0) - iota((local_rows, local_rows), 1)
    near = (doc_col == doc_row) & (gap >= 0) & (gap < reach)
    count = jnp.sum(jnp.where(near, 1.0, 0.0), axis=1, keepdims=True)
    near_b = onehot(near)
    loads[0].wait()
    running = jnp.dot(near_b, mix[...], preferred_element_type=F32)
    mixed = (running / count - mix[...].astype(F32)).astype(BF16)
    loads[1].wait()
    scale = scale_ref[...].reshape(1, -1)
    grouped = (jnp.dot(mixed, gw[...], preferred_element_type=F32) * scale).astype(BF16)
    for i in range(p.tp):
        grp[i] = grouped[i * rows : (i + 1) * rows]

    send_rows = jnp.concatenate([grp[(flip + 2 * j) % p.tp] for j in range(half)], axis=0)
    keep_rows = jnp.concatenate([grp[(tp + 2 * j) % p.tp] for j in range(half)], axis=0)
    loads[2].wait()
    for h in range(parts):
        weight = ow[:, h * piece : (h + 1) * piece]
        product = jnp.dot(send_rows, weight, preferred_element_type=F32).astype(BF16)
        for j in range(half):
            s1[j, h] = product[j * rows : (j + 1) * rows]
        kept = jnp.dot(keep_rows, weight, preferred_element_type=F32)
        for j in range(half):
            keep[j, h] = kept[j * rows : (j + 1) * rows]

    with jax.named_scope("barrier"):
        pl.semaphore_wait(barrier, greeted)
    halo_copies = [
        remote(mix.at[pl.ds(local_rows - HALO, HALO)], halo, halo_send.at[0], halo_recv.at[0], {"sp": ahead, "tp": tp}),
        remote(doc_ref, halo_doc, halo_send.at[1], halo_recv.at[1], {"sp": ahead, "tp": tp}),
    ]

    def arrived(ref, semaphore):
        pltpu.make_async_copy(ref, ref, semaphore).wait()

    def place(source, target):
        return (target - source + groups) % groups - 1

    @pl.when(sp < p.sp - 1)
    def _():
        for copy in halo_copies:
            copy.start()

    @pl.when(sp == 0)
    def _():
        halo[...] = jnp.zeros_like(halo)
        halo_doc[...] = jnp.zeros_like(halo_doc)

    first_hops = {
        (j, h): remote(s1.at[j, h], r1.at[j, h], sent.at[0], s1_recv.at[j, h], {"tp": flip})
        for j in range(half)
        for h in range(parts)
    }
    second_hops = {
        (j, h): remote(
            s2.at[j - 1, h], r2.at[j - 1, h], sent.at[1], s2_recv.at[j - 1, h], {"tp": (tp + 2 * j) % p.tp}
        )
        for j in range(1, half)
        for h in range(parts)
    }

    def send_first(late):
        for j in reversed(range(half)):
            block = (flip + 2 * j) % p.tp

            @pl.when((block == 0) if late else (block > 0))
            def _():
                for h in range(parts):
                    first_hops[j, h].start()

    def send_second(late):
        for j in range(1, half):
            block = (tp + 2 * j) % p.tp

            @pl.when((block == 0) if late else (block > 0))
            def _():
                for h in range(parts):
                    with jax.named_scope("fh_wait"):
                        first_hops[j, h].wait_recv()
                    s2[j - 1, h] = (keep[j, h] + r1[j, h].astype(F32)).astype(BF16)
                    second_hops[j, h].start()

    send_first(False)

    ids = ids_ref[...]
    id0_row, id1_row = ids[0:1], ids[1:2]
    id0, id1 = to_col(id0_row), to_col(id1_row)
    earlier = iota((rows, rows), 0) < iota((rows, rows), 1)

    def rank_row(pick_row):
        hit = earlier & ((id0 == pick_row) | (id1 == pick_row))
        return jnp.sum(jnp.where(hit, 1, 0), axis=0, keepdims=True)

    group_row, group_col = id0_row // members, id0 // members
    place_row = group_row * p.block + jnp.sum(
        jnp.where(earlier & (group_col == group_row), 1, 0), axis=0, keepdims=True
    )

    def key_row(pick_row):
        return (pick_row % members) * p.message + rank_row(pick_row)

    slots = groups * p.block
    chosen = iota((slots, rows), 0) == place_row
    chosen_b = onehot(chosen)
    place_col = to_col(place_row)
    spread_order = jnp.concatenate([my_group * p.block + iota((1, p.block), 1)] + [g * p.block + iota((1, p.block), 1) for g in others], axis=1)
    spread_b = onehot(spread_order == place_col)

    def per_slot(row):
        return jnp.sum(jnp.where(chosen, row, jnp.zeros_like(row)), axis=1, keepdims=True)

    weights = rw_ref[...]
    columns = (
        (per_slot(key_row(id0_row) + 1) - 1).astype(F32),
        (per_slot(key_row(id1_row) + 1) - 1).astype(F32),
        per_slot(weights[0:1]),
        per_slot(weights[1:2]),
    )
    lane = iota((slots, 128), 1)
    meta = jnp.zeros((slots, 128), F32)
    for i, column in enumerate(columns):
        meta = jnp.where(lane == i, column, meta)
    for g in range(groups):
        meta_out[g] = meta[g * p.block : (g + 1) * p.block]
    for g in others:
        slot = place(my_group, g)
        remote(meta_out.at[g], meta_in.at[slot], sent.at[2], m_recv.at[slot], relay(g)).start()

    send_second(False)

    @pl.when(sp > 0)
    def _():
        for copy in halo_copies:
            with jax.named_scope("halo_wait"):
                copy.wait_recv()

    back_gap = iota((HALO, HALO), 0) + HALO - iota((HALO, HALO), 1)
    first_reach = jnp.where(sp > 0, reach, 0)
    back = (doc_col[:HALO] == halo_doc[...][:, local_rows - HALO :]) & (back_gap < first_reach)
    head = running[:HALO] + jnp.dot(onehot(back), halo[...], preferred_element_type=F32)
    head_count = count[:HALO] + jnp.sum(jnp.where(back, 1.0, 0.0), axis=1, keepdims=True)
    head_mixed = (head / head_count - mix[:HALO].astype(F32)).astype(BF16)
    head_grouped = (jnp.dot(head_mixed, gw[...], preferred_element_type=F32) * scale).astype(BF16)
    head_product = jnp.dot(head_grouped, ow[...], preferred_element_type=F32)
    keep_slot = ((p.tp - tp) % p.tp) // 2
    send_slot = ((p.tp - flip) % p.tp) // 2

    @pl.when(tp % 2 == 0)
    def _():
        for h in range(parts):
            keep[keep_slot, h, :HALO] = head_product[:, h * piece : (h + 1) * piece]

    @pl.when(tp % 2 == 1)
    def _():
        for h in range(parts):
            s1[send_slot, h, :HALO] = head_product[:, h * piece : (h + 1) * piece].astype(BF16)

    send_first(True)
    send_second(True)

    def tables(k, info):
        k0, k1 = info[:, 0:1], info[:, 1:2]
        k0_row, k1_row = to_row(k0).astype(I32), to_row(k1).astype(I32)
        target = iota((p.served, p.block), 0)
        amat[k] = onehot((target == k0_row) | (target == k1_row))
        source = iota((p.block, p.served), 1)
        combine = jnp.where(source == k0.astype(I32), info[:, 2:3], 0.0) + jnp.where(
            source == k1.astype(I32), info[:, 3:4], 0.0
        )
        high = combine.astype(BF16)
        chi[k] = high
        clo[k] = (combine - high.astype(F32)).astype(BF16)

    tables(my_group, meta_out[my_group])
    for g in others:
        with jax.named_scope("m_wait"):
            slot = place(g, my_group)
            arrived(meta_in.at[slot], m_recv.at[slot])
        tables(g, meta_in[slot])

    ratio = parts // x_parts

    def forward_part(k, part, source):
        picked = jnp.dot(amat[k], source, preferred_element_type=F32).astype(BF16)
        for e in range(members):
            xout[k, part, e] = picked[e * p.message : (e + 1) * p.message]
        for step in list(range(2, members)) + [1]:
            e = (me + step) % members
            remote(xout.at[k, part, e], xin.at[k, part, me], sent.at[4], x_recv.at[k, part], member(e)).start()
        xin[k, part, me] = xout[k, part, me]

    def send_z(g, h):
        slot = place(my_group, g)
        remote(zb.at[g, h], zin.at[slot, h], sent.at[3], z_recv.at[slot, h], relay(g)).start()

    loads[3].wait()
    for h in range(parts):
        cut = slice(h * piece, (h + 1) * piece)
        with jax.named_scope("fh0_wait"):
            first_hops[0, h].wait_recv()
        summed = keep[0, h] + r1[0, h].astype(F32)
        for j in range(1, half):
            with jax.named_scope("sh_wait"):
                second_hops[j, h].wait_recv()
            summed = summed + r2[j - 1, h].astype(F32)
        stream = (resid[:, cut].astype(F32) + summed).astype(BF16)
        stream_f32[:, cut] = stream.astype(F32)
        gathered = jnp.dot(chosen_b, stream, preferred_element_type=F32).astype(BF16)
        for g in range(groups):
            zb[g, h] = gathered[g * p.block : (g + 1) * p.block]
        for step in Z_ORDER[h].split():
            send_z(others[int(step[0])], int(step[1]))
        if h % ratio == ratio - 1:
            first = h + 1 - ratio
            source = jnp.concatenate([zb[my_group, i] for i in range(first, h + 1)], axis=1)
            forward_part(my_group, h // ratio, source)

    def forward(k, part):
        slot = place(k, my_group)
        for h in range(part * ratio, (part + 1) * ratio):
            with jax.named_scope("z_wait"):
                arrived(zin.at[slot, h], z_recv.at[slot, h])
        source = jnp.concatenate([zin[slot, i] for i in range(part * ratio, (part + 1) * ratio)], axis=1)
        forward_part(k, part, source)

    waited = []

    def serve(k):
        for part in range(x_parts):
            with jax.named_scope("x_wait"):
                arrived(xin.at[k, part, pl.ds(0, members - 1)], x_recv.at[k, part])
        if not waited:
            waited.append(True)
            for i in (4, 5, 6):
                loads[i].wait()
        with jax.named_scope("expert"):
            flat = jnp.concatenate(
                [jnp.concatenate([xin[k, part, e] for e in range(members)], axis=0) for part in range(x_parts)], axis=1
            ).astype(F32)
            level = jnp.sum(flat * flat, axis=1, keepdims=True) / d
            normed = (flat * lax.rsqrt(level + 1e-06) * gain_ref[...]).astype(BF16)
            gate_part = jnp.dot(normed, wg[...], preferred_element_type=F32)
            up_part = jnp.dot(normed, wu[...], preferred_element_type=F32)
            hidden = (gate_part * jax.nn.sigmoid(gate_part) * up_part).astype(BF16)
            for part in range(b_parts):
                weight = wd[:, part * b_piece : (part + 1) * b_piece]
                answer = jnp.dot(hidden, weight, preferred_element_type=F32).astype(BF16)
                for e in range(members):
                    ans[k, part, e] = answer[e * p.message : (e + 1) * p.message]
                for step in list(range(2, members)) + [1]:
                    e = (me + step) % members
                    remote(ans.at[k, part, e], ret.at[k, part, me], sent.at[5], b_recv.at[k, part], member(e)).start()
                ret[k, part, me] = ans[k, part, me]

    def collect(k, wanted, own=False):
        for part in wanted:
            with jax.named_scope("b_wait"):
                arrived(ret.at[k, part, pl.ds(0, members - 1)], b_recv.at[k, part])
            flat = jnp.concatenate([ret[k, part, e] for e in range(members)], axis=0)
            joined = jnp.dot(chi[k], flat, preferred_element_type=F32) + jnp.dot(clo[k], flat, preferred_element_type=F32)
            if own:
                fin[groups - 1, part] = joined.astype(BF16)
            else:
                slot = place(my_group, k)
                zo[k, part] = joined.astype(BF16)
                remote(zo.at[k, part], fin.at[slot, part], sent.at[6], f_recv.at[slot, part], relay(k)).start()

    chunks = {"o": my_group, "n": others[0], "m": others[1], "f": others[2]}
    for step in SEQUENCE.split():
        k = chunks[step[1]]
        if step[0] == "F":
            for part in [int(step[2])] if step[2:] else range(x_parts):
                forward(k, part)
        elif step[0] == "S":
            serve(k)
        else:
            collect(k, [int(step[2])] if step[2:] else range(b_parts), own=step[1] == "o")

    for part in range(b_parts):
        cut = slice(part * b_piece, (part + 1) * b_piece)
        total = stream_f32[:, cut]
        arrivals = [(groups - 1, my_group)] + [(place(g, my_group), g) for g in others]
        with jax.named_scope("f_wait"):
            for slot, _ in arrivals[1:]:
                arrived(fin.at[slot, part], f_recv.at[slot, part])
        flat = jnp.concatenate([fin[slot, part] for slot, _ in arrivals], axis=0)
        out_ref[:, cut] = (total + jnp.dot(spread_b, flat, preferred_element_type=F32)).astype(BF16)

    @pl.when(sp < p.sp - 1)
    def _():
        for copy in halo_copies:
            copy.wait_send()

    arrived(s1, sent.at[0])
    arrived(s2, sent.at[1])
    arrived(meta_out.at[pl.ds(0, groups - 1)], sent.at[2])
    arrived(zb.at[pl.ds(0, groups - 1)], sent.at[3])
    arrived(xout.at[:, :, pl.ds(0, members - 1)], sent.at[4])
    arrived(ans.at[:, :, pl.ds(0, members - 1)], sent.at[5])
    arrived(zo.at[pl.ds(0, groups - 1)], sent.at[6])


def shards(
    sp_size,
    tp_size,
    mix_in,
    resid_in,
    doc_ids,
    group_weight,
    pool_scale,
    out_weight,
    norm_gain,
    expert_ids,
    route_weights,
    w_gate,
    w_up,
    w_down,
):
    local_rows, width = mix_in.shape
    rows, d = resid_in.shape
    ff = w_gate.shape[2]
    p = Plan(sp_size, tp_size, rows)
    g, half, parts = p.groups, p.half, p.parts
    vmem = pl.BlockSpec(memory_space=pltpu.VMEM)
    hbm = pl.BlockSpec(memory_space=pl.ANY)
    dma = pltpu.SemaphoreType.DMA
    common = [
        pltpu.VMEM((local_rows, width), BF16),
        pltpu.VMEM((rows, d), BF16),
        pltpu.VMEM(group_weight.shape[1:], BF16),
        pltpu.VMEM(out_weight.shape, BF16),
        pltpu.VMEM(w_gate.shape[1:], BF16),
        pltpu.VMEM(w_up.shape[1:], BF16),
        pltpu.VMEM(w_down.shape[1:], BF16),
        pltpu.VMEM((HALO, width), BF16),
        pltpu.VMEM((1, local_rows), I32),
        pltpu.VMEM((tp_size, rows, width), BF16),
    ]
    stream_and_meta = [
        pltpu.VMEM((rows, d), F32),
        pltpu.VMEM((g, p.block, 128), F32),
        pltpu.VMEM((g, p.block, 128), F32),
    ]
    if p.chunks == g and p.groups == 4:
        body = chunk_kernel
        parts, x_parts, b_parts = PARTS
        exchange = (half, parts, rows, d // parts)
        remote_exchange = (half - 1, parts, rows, d // parts)
        slots = (g, parts, p.block, d // parts)
        scratch = common + [
            pltpu.VMEM(exchange, F32),
            pltpu.VMEM(exchange, BF16),
            pltpu.VMEM(exchange, BF16),
            pltpu.VMEM(remote_exchange, BF16),
            pltpu.VMEM(remote_exchange, BF16),
            pltpu.VMEM((rows, d), F32),
            pltpu.VMEM((g, p.block, 128), F32),
            pltpu.VMEM((g - 1, p.block, 128), F32),
            pltpu.VMEM(slots, BF16),
            pltpu.VMEM((g - 1, *slots[1:]), BF16),
            pltpu.VMEM((g, p.served, p.block), BF16),
            pltpu.VMEM((g, p.block, p.served), BF16),
            pltpu.VMEM((g, p.block, p.served), BF16),
            pltpu.VMEM((g, x_parts, p.members, p.message, d // x_parts), BF16),
            pltpu.VMEM((g, x_parts, p.members, p.message, d // x_parts), BF16),
            pltpu.VMEM((g, b_parts, p.members, p.message, d // b_parts), BF16),
            pltpu.VMEM((g, b_parts, p.members, p.message, d // b_parts), BF16),
            pltpu.VMEM((g, b_parts, p.block, d // b_parts), BF16),
            pltpu.VMEM((g, b_parts, p.block, d // b_parts), BF16),
            dma((7,)), dma((7,)),
            dma((2,)), dma((2,)),
            dma((g - 1,)),
            dma((half, parts)),
            dma((half - 1, parts)),
            dma((g - 1, parts)),
            dma((g, x_parts)),
            dma((g, b_parts)),
            dma((g - 1, b_parts)),
        ]
    else:
        body = kernel
        span_rows = p.per_chunk * p.block
        messages = (p.chunks, p.members, p.message, d)
        exchange = (half, parts, rows, d // parts)
        scratch = common + [
            pltpu.VMEM(exchange, F32),
            pltpu.VMEM(exchange, BF16),
            pltpu.VMEM(exchange, BF16),
            pltpu.VMEM(exchange, BF16),
            pltpu.VMEM(exchange, BF16),
        ] + stream_and_meta + [
            pltpu.VMEM((g, p.block, d), BF16),
            pltpu.VMEM((g, p.block, d), BF16),
            pltpu.VMEM((p.chunks, p.served, span_rows), BF16),
            pltpu.VMEM((p.chunks, span_rows, p.served), BF16),
            pltpu.VMEM((p.chunks, span_rows, p.served), BF16),
            pltpu.VMEM(messages, BF16),
            pltpu.VMEM(messages, BF16),
            pltpu.VMEM(messages, BF16),
            pltpu.VMEM(messages, BF16),
            pltpu.VMEM((g, p.block, d), BF16),
            pltpu.VMEM((g, p.block, d), BF16),
            dma((7,)),
            dma((2,)), dma((2,)),
            dma((g,)), dma((g,)),
            dma((half, parts)), dma((half, parts)),
            dma((half, parts)), dma((half, parts)),
            dma((g,)), dma((g,)),
            dma((p.chunks, p.members)), dma((p.chunks, p.members)),
            dma((p.chunks, p.members)), dma((p.chunks, p.members)),
            dma((g,)), dma((g,)),
        ]
    return pl.pallas_call(
        functools.partial(body, p),
        out_shape=pltpu.VMEM((rows, d), BF16),
        in_specs=[hbm, hbm, vmem, hbm, vmem, hbm, vmem, vmem, vmem, hbm, hbm, hbm],
        out_specs=vmem,
        scratch_shapes=scratch,
        compiler_params=pltpu.CompilerParams(
            collective_id=0, has_side_effects=True, vmem_limit_bytes=56 * 1024 * 1024
        ),
    )(
        mix_in, resid_in, doc_ids.reshape(1, -1), group_weight, pool_scale, out_weight,
        norm_gain.reshape(1, -1), expert_ids.T, route_weights.T, w_gate, w_up, w_down,
    )


def solution(mesh):
    return jax.shard_map(
        functools.partial(shards, mesh.shape["sp"], mesh.shape["tp"]),
        mesh=mesh,
        in_specs=(
            P(("grp", "sp"), "tp"),
            P(("grp", "sp", "tp"), None),
            P(("grp", "sp")),
            P("tp", None, None),
            P("tp"),
            P("tp", None),
            P(),
            P(("grp", "sp", "tp"), None),
            P(("grp", "sp", "tp"), None),
            P(("sp", "tp"), None, None),
            P(("sp", "tp"), None, None),
            P(("sp", "tp"), None, None),
        ),
        out_specs=P(("grp", "sp", "tp"), None),
        check_vma=False,
    )
```

```python
import functools

import jax
import jax.numpy as jnp
from jax import lax
from jax.experimental import pallas as pl
from jax.experimental.pallas import tpu as pltpu
from jax.sharding import PartitionSpec as P

HALO = 16
TOP_K = 2
EXPERT_GROUPS = 4
PARTS = (4, 4, 2)
SEQUENCE = ("Fn0 Fm0 Ff0", "Fn1 Fm1 Ff1", "Fn2 Fm2 Ff2", "Fn3 Fm3 Ff3", "Sf Sm Cf", "Sn Cm So", "Cn Co")
Z_ORDER = ["00 10 20", "01 11 21", "02 12 22", "03 13 23"]
SEND = [[1, 2, 3], [2, 0, 3], [1, 3, 0], [2, 1, 0]]
TABLE = [[0, 1, 2, 3], [1, 0, 2, 3], [2, 3, 1, 0], [3, 2, 1, 0]]
OWN_LATE = False
MESH = pl.DeviceIdType.MESH
F32 = jnp.float32
BF16 = jnp.bfloat16
I32 = jnp.int32


def iota(shape, dim):
    return lax.broadcasted_iota(I32, shape, dim)


def to_row(col):
    n = col.shape[0]
    eye = iota((n, n), 0) == iota((n, n), 1)
    return jnp.sum(jnp.where(eye, col, jnp.zeros_like(col)), axis=0, keepdims=True)


def to_col(row):
    n = row.shape[1]
    eye = iota((n, n), 0) == iota((n, n), 1)
    return jnp.sum(jnp.where(eye, row, jnp.zeros_like(row)), axis=1, keepdims=True)


def onehot(mask):
    return jnp.where(mask, 1.0, 0.0).astype(BF16)


class Plan:
    def __init__(self, sp_size, tp_size, token_rows):
        self.sp, self.tp, self.rows = sp_size, tp_size, token_rows
        self.experts = sp_size * tp_size
        self.groups = EXPERT_GROUPS
        self.span = sp_size // self.groups
        self.members = self.span * tp_size
        self.cap = max(TOP_K, 4 * token_rows // self.experts)
        self.block = min(token_rows, self.cap * self.members // TOP_K)
        if self.cap % 16 == 0:
            self.chunks, self.cap_pad = self.groups, self.cap
        else:
            self.chunks = 1
            whole = -(-self.cap * self.groups // 16) * 16
            self.cap_pad = whole // self.groups
        self.per_chunk = self.groups // self.chunks
        self.message = self.per_chunk * self.cap_pad
        self.served = self.members * self.message
        self.half = tp_size // 2
        self.parts = 2


def kernel(
    p,
    mix_hbm, resid_hbm, doc_ref, gw_hbm, scale_ref, ow_hbm, gain_ref, ids_ref, rw_ref, wg_hbm, wu_hbm, wd_hbm,
    out_ref,
    mix, resid, gw, ow, wg, wu, wd,
    halo, halo_doc, grp, keep, s1, r1, s2, r2, stream_f32, meta_out, meta_in, zb, zin, amat, chi, clo,
    xout, xin, ans, ret, zo, fin,
    load_sem, halo_send, halo_recv, m_send, m_recv, s1_send, s1_recv, s2_send, s2_recv,
    z_send, z_recv, x_send, x_recv, b_send, b_recv, f_send, f_recv,
):
    sp, tp = lax.axis_index("sp"), lax.axis_index("tp")
    local_rows, width = mix.shape
    d = resid.shape[1]
    rows, groups, half, parts = p.rows, p.groups, p.half, p.parts
    piece = d // parts
    loads = [
        pltpu.make_async_copy(src, dst, load_sem.at[i])
        for i, (src, dst) in enumerate(
            [
                (mix_hbm, mix), (gw_hbm.at[0], gw), (ow_hbm, ow), (resid_hbm, resid),
                (wg_hbm.at[0], wg), (wu_hbm.at[0], wu), (wd_hbm.at[0], wd),
            ]
        )
    ]
    for load in loads[:4]:
        load.start()

    my_group, lane_in_span = sp // p.span, sp % p.span
    me = lane_in_span * p.tp + tp
    flip = tp + 1 - 2 * (tp % 2)

    steps = [0] + sorted(range(1, groups), key=lambda step: min(step, groups - step))
    nearest = [(my_group + step) % groups for step in steps]

    def relay(group):
        return {"sp": group * p.span + lane_in_span, "tp": tp}

    def member(index):
        return {"sp": my_group * p.span + index // p.tp, "tp": index % p.tp}

    barrier = pltpu.get_barrier_semaphore()
    greeted = 0
    ahead, behind = (sp + 1) % p.sp, (sp + p.sp - 1) % p.sp
    targets = [{"sp": ahead, "tp": tp}, {"sp": behind, "tp": tp}]
    targets += [relay((my_group + off) % groups) for off in range(1, groups)]
    targets += [member((me + off) % p.members) for off in range(1, p.members)]
    for target in targets:
        pl.semaphore_signal(barrier, inc=1, device_id=target, device_id_type=MESH)
        greeted += 1

    def remote(src, dst, send, recv, device):
        return pltpu.make_async_remote_copy(
            src_ref=src, dst_ref=dst, send_sem=send, recv_sem=recv, device_id=device, device_id_type=MESH
        )

    ids = ids_ref[...]
    id0_row, id1_row = ids[0:1], ids[1:2]
    id0, id1 = to_col(id0_row), to_col(id1_row)
    earlier = iota((rows, rows), 0) < iota((rows, rows), 1)

    def rank_row(pick_row):
        hit = earlier & ((id0 == pick_row) | (id1 == pick_row))
        return jnp.sum(jnp.where(hit, 1, 0), axis=0, keepdims=True)

    group_row, group_col = id0_row // p.members, id0 // p.members
    place_row = group_row * p.block + jnp.sum(
        jnp.where(earlier & (group_col == group_row), 1, 0), axis=0, keepdims=True
    )
    offset = (my_group % p.per_chunk) * p.cap_pad

    def key_row(pick_row):
        return (pick_row % p.members) * p.message + offset + rank_row(pick_row)

    slots = groups * p.block
    chosen = iota((slots, rows), 0) == place_row
    chosen_b = onehot(chosen)
    place_col = to_col(place_row)
    spread_b = onehot(iota((rows, slots), 1) == place_col)

    def per_slot(row):
        return jnp.sum(jnp.where(chosen, row, jnp.zeros_like(row)), axis=1, keepdims=True)

    weights = rw_ref[...]
    columns = (
        (per_slot(key_row(id0_row) + 1) - 1).astype(F32),
        (per_slot(key_row(id1_row) + 1) - 1).astype(F32),
        per_slot(weights[0:1]),
        per_slot(weights[1:2]),
    )
    lane = iota((slots, 128), 1)
    meta = jnp.zeros((slots, 128), F32)
    for i, column in enumerate(columns):
        meta = jnp.where(lane == i, column, meta)
    for g in range(groups):
        meta_out[g] = meta[g * p.block : (g + 1) * p.block]

    pl.semaphore_wait(barrier, greeted)
    halo_copies = [
        remote(mix.at[pl.ds(local_rows - HALO, HALO)], halo, halo_send.at[0], halo_recv.at[0], {"sp": ahead, "tp": tp}),
        remote(doc_ref, halo_doc, halo_send.at[1], halo_recv.at[1], {"sp": ahead, "tp": tp}),
    ]
    loads[0].wait()

    @pl.when(sp < p.sp - 1)
    def _():
        for copy in halo_copies:
            copy.start()

    @pl.when(sp == 0)
    def _():
        halo[...] = jnp.zeros_like(halo)
        halo_doc[...] = jnp.zeros_like(halo_doc)


    doc_row = doc_ref[...]
    doc_col = to_col(doc_row)
    reach = jnp.left_shift(jnp.int32(2), tp)
    gap = iota((local_rows, local_rows), 0) - iota((local_rows, local_rows), 1)
    near = (doc_col == doc_row) & (gap >= 0) & (gap < reach)
    count = jnp.sum(jnp.where(near, 1.0, 0.0), axis=1, keepdims=True)
    mix_value = mix[...]
    running = jnp.dot(onehot(near), mix_value, preferred_element_type=F32)

    meta_copies = []
    for off in range(groups):
        g = nearest[off]
        if off == 0:
            copy = pltpu.make_async_copy(meta_out.at[g], meta_in.at[my_group], m_recv.at[my_group])
        else:
            copy = remote(meta_out.at[g], meta_in.at[my_group], m_send.at[g], m_recv.at[my_group], relay(g))
        copy.start()
        meta_copies.append(copy)

    @pl.when(sp > 0)
    def _():
        for copy in halo_copies:
            copy.wait_recv()

    back_gap = iota((HALO, HALO), 0) + HALO - iota((HALO, HALO), 1)
    first_reach = jnp.where(sp > 0, reach, 0)
    back = (doc_col[:HALO] == halo_doc[...][:, local_rows - HALO :]) & (back_gap < first_reach)
    head = running[:HALO] + jnp.dot(onehot(back), halo[...], preferred_element_type=F32)
    head_count = count[:HALO] + jnp.sum(jnp.where(back, 1.0, 0.0), axis=1, keepdims=True)
    running = jnp.concatenate([head, running[HALO:]], axis=0)
    count = jnp.concatenate([head_count, count[HALO:]], axis=0)
    mixed = (running / count - mix_value.astype(F32)).astype(BF16)
    loads[1].wait()
    grouped = (jnp.dot(mixed, gw[...], preferred_element_type=F32) * scale_ref[...].reshape(1, -1)).astype(BF16)
    for i in range(p.tp):
        grp[i] = grouped[i * rows : (i + 1) * rows]

    send_rows = jnp.concatenate([grp[(flip + 2 * j) % p.tp] for j in range(half)], axis=0)
    keep_rows = jnp.concatenate([grp[(tp + 2 * j) % p.tp] for j in range(half)], axis=0)
    loads[2].wait()
    first_hops = {}
    for h in range(parts):
        weight = ow[:, h * piece : (h + 1) * piece]
        product = jnp.dot(send_rows, weight, preferred_element_type=F32).astype(BF16)
        for j in reversed(range(half)):
            s1[j, h] = product[j * rows : (j + 1) * rows]
            copy = remote(s1.at[j, h], r1.at[j, h], s1_send.at[j, h], s1_recv.at[j, h], {"tp": flip})
            copy.start()
            first_hops[j, h] = copy
        kept = jnp.dot(keep_rows, weight, preferred_element_type=F32)
        for j in range(half):
            keep[j, h] = kept[j * rows : (j + 1) * rows]
    for load in loads[4:]:
        load.start()
    second_hops = {}
    for h in range(parts):
        for j in range(1, half):
            first_hops[j, h].wait_recv()
            s2[j, h] = (keep[j, h] + r1[j, h].astype(F32)).astype(BF16)
            copy = remote(
                s2.at[j, h], r2.at[j, h], s2_send.at[j, h], s2_recv.at[j, h], {"tp": (tp + 2 * j) % p.tp}
            )
            copy.start()
            second_hops[j, h] = copy

    for off in range(groups):
        b = nearest[off]
        if off == 0:
            meta_copies[0].wait()
        else:
            remote(meta_out.at[b], meta_in.at[b], m_send.at[b], m_recv.at[b], relay(b)).wait_recv()
    span_rows = p.per_chunk * p.block
    for k in range(p.chunks):
        info = jnp.concatenate([meta_in[k * p.per_chunk + i] for i in range(p.per_chunk)], axis=0)
        k0, k1 = info[:, 0:1], info[:, 1:2]
        k0_row, k1_row = to_row(k0).astype(I32), to_row(k1).astype(I32)
        target = iota((p.served, span_rows), 0)
        amat[k] = onehot((target == k0_row) | (target == k1_row))
        source = iota((span_rows, p.served), 1)
        combine = jnp.where(source == k0.astype(I32), info[:, 2:3], 0.0) + jnp.where(
            source == k1.astype(I32), info[:, 3:4], 0.0
        )
        high = combine.astype(BF16)
        chi[k] = high
        clo[k] = (combine - high.astype(F32)).astype(BF16)

    loads[3].wait()
    total = jnp.zeros((rows, 1), F32)
    for h in range(parts):
        cut = slice(h * piece, (h + 1) * piece)
        first_hops[0, h].wait_recv()
        summed = keep[0, h] + r1[0, h].astype(F32)
        for j in range(1, half):
            second_hops[j, h].wait_recv()
            summed = summed + r2[j, h].astype(F32)
        stream = (resid[:, cut].astype(F32) + summed).astype(BF16)
        stream_f = stream.astype(F32)
        stream_f32[:, cut] = stream_f
        total = total + jnp.sum(stream_f * stream_f, axis=1, keepdims=True)
    normed = (stream_f32[...] * lax.rsqrt(total / d + 1e-06) * gain_ref[...]).astype(BF16)

    gathered = jnp.dot(chosen_b, normed, preferred_element_type=F32).astype(BF16)
    for g in range(groups):
        zb[g] = gathered[g * p.block : (g + 1) * p.block]
    z_copies = []
    for off in range(groups):
        g = nearest[off]
        if off == 0:
            copy = pltpu.make_async_copy(zb.at[g], zin.at[my_group], z_recv.at[my_group])
        else:
            copy = remote(zb.at[g], zin.at[my_group], z_send.at[g], z_recv.at[my_group], relay(g))
        copy.start()
        z_copies.append(copy)

    if p.chunks == groups:
        order = [[off] for off in range(groups)]
    else:
        order = [list(range(groups))]

    x_copies, b_copies, f_copies = [], [], []

    def forward(offs):
        k = nearest[offs[0]] if p.chunks > 1 else 0
        for off in offs:
            b = nearest[off]
            if off == 0:
                z_copies[0].wait()
            else:
                remote(zb.at[b], zin.at[b], z_send.at[b], z_recv.at[b], relay(b)).wait_recv()
        if p.chunks > 1:
            source = zin[k]
        else:
            source = jnp.concatenate([zin[i] for i in range(groups)], axis=0)
        picked = jnp.dot(amat[k], source, preferred_element_type=F32).astype(BF16)
        for e in range(p.members):
            xout[k, e] = picked[e * p.message : (e + 1) * p.message]
        for step in range(p.members):
            e = (me + step) % p.members
            if step == 0:
                copy = pltpu.make_async_copy(xout.at[k, e], xin.at[k, me], x_recv.at[k, me])
            else:
                copy = remote(xout.at[k, e], xin.at[k, me], x_send.at[k, e], x_recv.at[k, me], member(e))
            copy.start()
            x_copies.append((step, copy))

    def serve(n, offs):
        k = nearest[offs[0]] if p.chunks > 1 else 0
        for step in range(p.members):
            e = (me + step) % p.members
            if step == 0:
                x_copies[n * p.members][1].wait()
            else:
                remote(xout.at[k, e], xin.at[k, e], x_send.at[k, e], x_recv.at[k, e], member(e)).wait_recv()
        if n == 0:
            for i in (4, 5, 6):
                loads[i].wait()
        flat = jnp.concatenate([xin[k, e] for e in range(p.members)], axis=0)
        gate_part = jnp.dot(flat, wg[...], preferred_element_type=F32)
        up_part = jnp.dot(flat, wu[...], preferred_element_type=F32)
        hidden = (gate_part * jax.nn.sigmoid(gate_part) * up_part).astype(BF16)
        answer = jnp.dot(hidden, wd[...], preferred_element_type=F32).astype(BF16)
        for e in range(p.members):
            ans[k, e] = answer[e * p.message : (e + 1) * p.message]
        for step in range(p.members):
            e = (me + step) % p.members
            if step == 0:
                copy = pltpu.make_async_copy(ans.at[k, e], ret.at[k, me], b_recv.at[k, me])
            else:
                copy = remote(ans.at[k, e], ret.at[k, me], b_send.at[k, e], b_recv.at[k, me], member(e))
            copy.start()
            b_copies.append((step, copy))

    def collect(n, offs):
        k = nearest[offs[0]] if p.chunks > 1 else 0
        for step in range(p.members):
            e = (me + step) % p.members
            if step == 0:
                b_copies[n * p.members][1].wait()
            else:
                remote(ans.at[k, e], ret.at[k, e], b_send.at[k, e], b_recv.at[k, e], member(e)).wait_recv()
        flat = jnp.concatenate([ret[k, e] for e in range(p.members)], axis=0)
        joined = jnp.dot(chi[k], flat, preferred_element_type=F32) + jnp.dot(clo[k], flat, preferred_element_type=F32)
        joined = joined.astype(BF16)
        if p.chunks > 1:
            zo[k] = joined
        else:
            for i in range(groups):
                zo[i] = joined[i * p.block : (i + 1) * p.block]
        for off in offs:
            b = nearest[off]
            if off == 0:
                copy = pltpu.make_async_copy(zo.at[b], fin.at[my_group], f_recv.at[my_group])
            else:
                copy = remote(zo.at[b], fin.at[my_group], f_send.at[b], f_recv.at[my_group], relay(b))
            copy.start()
            f_copies.append((off, copy))

    count_chunks = len(order)
    forward(order[0])
    for n in range(count_chunks):
        if n + 1 < count_chunks:
            forward(order[n + 1])
        serve(n, order[n])
        if n >= 1:
            collect(n - 1, order[n - 1])
    collect(count_chunks - 1, order[-1])

    for off in range(groups):
        g = nearest[off]
        if off == 0:
            [copy for o, copy in f_copies if o == 0][0].wait()
        else:
            remote(zo.at[g], fin.at[g], f_send.at[g], f_recv.at[g], relay(g)).wait_recv()
    flat = jnp.concatenate([fin[g] for g in range(groups)], axis=0)
    out_ref[...] = (stream_f32[...] + jnp.dot(spread_b, flat, preferred_element_type=F32)).astype(BF16)

    @pl.when(sp < p.sp - 1)
    def _():
        for copy in halo_copies:
            copy.wait_send()

    for copy in meta_copies[1:] + list(first_hops.values()) + list(second_hops.values()) + z_copies[1:]:
        copy.wait_send()
    for step, copy in x_copies + b_copies + f_copies:
        if step:
            copy.wait_send()


def ordered(position, table):
    n = len(table)
    return [
        sum((1 - ((position - z + n) % n + n - 1) // n) * table[z][i] for z in range(n)) for i in range(len(table[0]))
    ]


def chunk_kernel(
    p,
    mix_hbm, resid_hbm, doc_ref, gw_hbm, scale_ref, ow_hbm, gain_ref, ids_ref, rw_ref, wg_hbm, wu_hbm, wd_hbm,
    out_ref,
    mix, resid, gw, ow, wg, wu, wd,
    halo, halo_doc, grp, keep, s1, r1, s2, r2, stream_f32, meta_out, meta_in, zb, zin, amat, chi, clo,
    xout, xin, ans, ret, zo, fin,
    load_sem, sent, halo_send, halo_recv, m_recv, s1_recv, s2_recv, z_recv, x_recv, b_recv, f_recv,
):
    sp, tp = lax.axis_index("sp"), lax.axis_index("tp")
    local_rows, width = mix.shape
    d = resid.shape[1]
    rows, groups, half, members = p.rows, p.groups, p.half, p.members
    parts, x_parts, b_parts = zb.shape[1], xout.shape[1], ans.shape[1]
    piece, x_piece, b_piece = d // parts, d // x_parts, d // b_parts
    loads = [
        pltpu.make_async_copy(src, dst, load_sem.at[i])
        for i, (src, dst) in enumerate(
            [
                (mix_hbm, mix), (gw_hbm.at[0], gw), (ow_hbm, ow), (resid_hbm, resid),
                (wg_hbm.at[0], wg), (wu_hbm.at[0], wu), (wd_hbm.at[0], wd),
            ]
        )
    ]

    my_group, lane_in_span = sp // p.span, sp % p.span
    me = lane_in_span * p.tp + tp
    flip = tp + 1 - 2 * (tp % 2)
    order = ordered(my_group, TABLE)
    others = order[1:]
    receivers = ordered(my_group, SEND)

    def relay(group):
        return {"sp": group * p.span + lane_in_span, "tp": tp}

    def member(index):
        return {"sp": my_group * p.span + index // p.tp, "tp": index % p.tp}

    barrier = pltpu.get_barrier_semaphore()
    greeted = 0
    ahead, behind = (sp + 1) % p.sp, (sp + p.sp - 1) % p.sp
    targets = [{"sp": ahead, "tp": tp}, {"sp": behind, "tp": tp}]
    targets += [relay((my_group + off) % groups) for off in range(1, groups)]
    targets += [member((me + off) % members) for off in range(1, members)]
    for target in targets:
        pl.semaphore_signal(barrier, inc=1, device_id=target, device_id_type=MESH)
        greeted += 1
    for load in loads:
        load.start()

    def remote(src, dst, send, recv, device):
        return pltpu.make_async_remote_copy(
            src_ref=src, dst_ref=dst, send_sem=send, recv_sem=recv, device_id=device, device_id_type=MESH
        )

    doc_row = doc_ref[...]
    doc_col = to_col(doc_row)
    reach = jnp.left_shift(jnp.int32(2), tp)
    gap = iota((local_rows, local_rows), 0) - iota((local_rows, local_rows), 1)
    near = (doc_col == doc_row) & (gap >= 0) & (gap < reach)
    count = jnp.sum(jnp.where(near, 1.0, 0.0), axis=1, keepdims=True)
    near_b = onehot(near)
    loads[0].wait()
    running = jnp.dot(near_b, mix[...], preferred_element_type=F32)
    mixed = (running / count - mix[...].astype(F32)).astype(BF16)
    loads[1].wait()
    scale = scale_ref[...].reshape(1, -1)
    grouped = (jnp.dot(mixed, gw[...], preferred_element_type=F32) * scale).astype(BF16)
    for i in range(p.tp):
        grp[i] = grouped[i * rows : (i + 1) * rows]

    send_rows = jnp.concatenate([grp[(flip + 2 * j) % p.tp] for j in range(half)], axis=0)
    keep_rows = jnp.concatenate([grp[(tp + 2 * j) % p.tp] for j in range(half)], axis=0)
    loads[2].wait()
    for h in range(parts):
        weight = ow[:, h * piece : (h + 1) * piece]
        product = jnp.dot(send_rows, weight, preferred_element_type=F32).astype(BF16)
        for j in range(half):
            s1[j, h] = product[j * rows : (j + 1) * rows]
        kept = jnp.dot(keep_rows, weight, preferred_element_type=F32)
        for j in range(half):
            keep[j, h] = kept[j * rows : (j + 1) * rows]

    with jax.named_scope("barrier"):
        pl.semaphore_wait(barrier, greeted)
    halo_copies = [
        remote(mix.at[pl.ds(local_rows - HALO, HALO)], halo, halo_send.at[0], halo_recv.at[0], {"sp": ahead, "tp": tp}),
        remote(doc_ref, halo_doc, halo_send.at[1], halo_recv.at[1], {"sp": ahead, "tp": tp}),
    ]

    def arrived(ref, semaphore):
        pltpu.make_async_copy(ref, ref, semaphore).wait()

    def place(source, target):
        return (target - source + groups) % groups - 1

    @pl.when(sp < p.sp - 1)
    def _():
        for copy in halo_copies:
            copy.start()

    @pl.when(sp == 0)
    def _():
        halo[...] = jnp.zeros_like(halo)
        halo_doc[...] = jnp.zeros_like(halo_doc)

    first_hops = {
        (j, h): remote(s1.at[j, h], r1.at[j, h], sent.at[0], s1_recv.at[j, h], {"tp": flip})
        for j in range(half)
        for h in range(parts)
    }
    second_hops = {
        (j, h): remote(
            s2.at[j - 1, h], r2.at[j - 1, h], sent.at[1], s2_recv.at[j - 1, h], {"tp": (tp + 2 * j) % p.tp}
        )
        for j in range(1, half)
        for h in range(parts)
    }

    def send_first(late):
        for j in reversed(range(half)):
            block = (flip + 2 * j) % p.tp

            @pl.when((block == 0) if late else (block > 0))
            def _():
                for h in range(parts):
                    first_hops[j, h].start()

    def send_second(late):
        for j in range(1, half):
            block = (tp + 2 * j) % p.tp

            @pl.when((block == 0) if late else (block > 0))
            def _():
                for h in range(parts):
                    with jax.named_scope("fh_wait"):
                        first_hops[j, h].wait_recv()
                    s2[j - 1, h] = (keep[j, h] + r1[j, h].astype(F32)).astype(BF16)
                    second_hops[j, h].start()

    send_first(False)

    ids = ids_ref[...]
    id0_row, id1_row = ids[0:1], ids[1:2]
    id0, id1 = to_col(id0_row), to_col(id1_row)
    earlier = iota((rows, rows), 0) < iota((rows, rows), 1)

    def rank_row(pick_row):
        hit = earlier & ((id0 == pick_row) | (id1 == pick_row))
        return jnp.sum(jnp.where(hit, 1, 0), axis=0, keepdims=True)

    group_row, group_col = id0_row // members, id0 // members
    place_row = group_row * p.block + jnp.sum(
        jnp.where(earlier & (group_col == group_row), 1, 0), axis=0, keepdims=True
    )

    def key_row(pick_row):
        return (pick_row % members) * p.message + rank_row(pick_row)

    slots = groups * p.block
    chosen = iota((slots, rows), 0) == place_row
    chosen_b = onehot(chosen)
    place_col = to_col(place_row)
    spread_order = jnp.concatenate([my_group * p.block + iota((1, p.block), 1)] + [g * p.block + iota((1, p.block), 1) for g in others], axis=1)
    spread_b = onehot(spread_order == place_col)

    def per_slot(row):
        return jnp.sum(jnp.where(chosen, row, jnp.zeros_like(row)), axis=1, keepdims=True)

    weights = rw_ref[...]
    columns = (
        (per_slot(key_row(id0_row) + 1) - 1).astype(F32),
        (per_slot(key_row(id1_row) + 1) - 1).astype(F32),
        per_slot(weights[0:1]),
        per_slot(weights[1:2]),
    )
    lane = iota((slots, 128), 1)
    meta = jnp.zeros((slots, 128), F32)
    for i, column in enumerate(columns):
        meta = jnp.where(lane == i, column, meta)
    for g in range(groups):
        meta_out[g] = meta[g * p.block : (g + 1) * p.block]
    for g in others:
        slot = place(my_group, g)
        remote(meta_out.at[g], meta_in.at[slot], sent.at[2], m_recv.at[slot], relay(g)).start()

    send_second(False)

    @pl.when(sp > 0)
    def _():
        for copy in halo_copies:
            with jax.named_scope("halo_wait"):
                copy.wait_recv()

    back_gap = iota((HALO, HALO), 0) + HALO - iota((HALO, HALO), 1)
    first_reach = jnp.where(sp > 0, reach, 0)
    back = (doc_col[:HALO] == halo_doc[...][:, local_rows - HALO :]) & (back_gap < first_reach)
    head = running[:HALO] + jnp.dot(onehot(back), halo[...], preferred_element_type=F32)
    head_count = count[:HALO] + jnp.sum(jnp.where(back, 1.0, 0.0), axis=1, keepdims=True)
    head_mixed = (head / head_count - mix[:HALO].astype(F32)).astype(BF16)
    head_grouped = (jnp.dot(head_mixed, gw[...], preferred_element_type=F32) * scale).astype(BF16)
    head_product = jnp.dot(head_grouped, ow[...], preferred_element_type=F32)
    keep_slot = ((p.tp - tp) % p.tp) // 2
    send_slot = ((p.tp - flip) % p.tp) // 2

    @pl.when(tp % 2 == 0)
    def _():
        for h in range(parts):
            keep[keep_slot, h, :HALO] = head_product[:, h * piece : (h + 1) * piece]

    @pl.when(tp % 2 == 1)
    def _():
        for h in range(parts):
            s1[send_slot, h, :HALO] = head_product[:, h * piece : (h + 1) * piece].astype(BF16)

    send_first(True)
    send_second(True)

    def tables(k, info):
        k0, k1 = info[:, 0:1], info[:, 1:2]
        k0_row, k1_row = to_row(k0).astype(I32), to_row(k1).astype(I32)
        target = iota((p.served, p.block), 0)
        amat[k] = onehot((target == k0_row) | (target == k1_row))
        source = iota((p.block, p.served), 1)
        combine = jnp.where(source == k0.astype(I32), info[:, 2:3], 0.0) + jnp.where(
            source == k1.astype(I32), info[:, 3:4], 0.0
        )
        high = combine.astype(BF16)
        chi[k] = high
        clo[k] = (combine - high.astype(F32)).astype(BF16)

    tables(my_group, meta_out[my_group])
    for g in others:
        with jax.named_scope("m_wait"):
            slot = place(g, my_group)
            arrived(meta_in.at[slot], m_recv.at[slot])
        tables(g, meta_in[slot])

    ratio = parts // x_parts

    def forward_part(k, part, source):
        picked = jnp.dot(amat[k], source, preferred_element_type=F32).astype(BF16)
        for e in range(members):
            xout[k, part, e] = picked[e * p.message : (e + 1) * p.message]
        for step in list(range(2, members)) + [1]:
            e = (me + step) % members
            remote(xout.at[k, part, e], xin.at[k, part, me], sent.at[4], x_recv.at[k, part], member(e)).start()
        xin[k, part, me] = xout[k, part, me]

    def send_z(g, h):
        slot = place(my_group, g)
        remote(zb.at[g, h], zin.at[slot, h], sent.at[3], z_recv.at[slot, h], relay(g)).start()

    def forward_own(part):
        source = jnp.concatenate([zb[my_group, i] for i in range(part * ratio, (part + 1) * ratio)], axis=1)
        forward_part(my_group, part, source)

    loads[3].wait()
    for h in range(parts):
        cut = slice(h * piece, (h + 1) * piece)
        with jax.named_scope("fh0_wait"):
            first_hops[0, h].wait_recv()
        summed = keep[0, h] + r1[0, h].astype(F32)
        for j in range(1, half):
            with jax.named_scope("sh_wait"):
                second_hops[j, h].wait_recv()
            summed = summed + r2[j - 1, h].astype(F32)
        stream = (resid[:, cut].astype(F32) + summed).astype(BF16)
        stream_f32[:, cut] = stream.astype(F32)
        gathered = jnp.dot(chosen_b, stream, preferred_element_type=F32).astype(BF16)
        for g in range(groups):
            zb[g, h] = gathered[g * p.block : (g + 1) * p.block]
        for step in Z_ORDER[h].split():
            send_z(receivers[int(step[0])], int(step[1]))
        if h % ratio == ratio - 1 and not OWN_LATE:
            forward_own(h // ratio)

    def forward(k, part):
        slot = place(k, my_group)
        for h in range(part * ratio, (part + 1) * ratio):
            with jax.named_scope("z_wait"):
                arrived(zin.at[slot, h], z_recv.at[slot, h])
        source = jnp.concatenate([zin[slot, i] for i in range(part * ratio, (part + 1) * ratio)], axis=1)
        forward_part(k, part, source)

    waited = []

    def serve(k):
        for part in range(x_parts):
            with jax.named_scope("x_wait"):
                arrived(xin.at[k, part, pl.ds(0, members - 1)], x_recv.at[k, part])
        if not waited:
            waited.append(True)
            for i in (4, 5, 6):
                loads[i].wait()
        with jax.named_scope("expert"):
            flat = jnp.concatenate(
                [jnp.concatenate([xin[k, part, e] for e in range(members)], axis=0) for part in range(x_parts)], axis=1
            ).astype(F32)
            level = jnp.sum(flat * flat, axis=1, keepdims=True) / d
            normed = (flat * lax.rsqrt(level + 1e-06) * gain_ref[...]).astype(BF16)
            gate_part = jnp.dot(normed, wg[...], preferred_element_type=F32)
            up_part = jnp.dot(normed, wu[...], preferred_element_type=F32)
            hidden = (gate_part * jax.nn.sigmoid(gate_part) * up_part).astype(BF16)
            for part in range(b_parts):
                weight = wd[:, part * b_piece : (part + 1) * b_piece]
                answer = jnp.dot(hidden, weight, preferred_element_type=F32).astype(BF16)
                for e in range(members):
                    ans[k, part, e] = answer[e * p.message : (e + 1) * p.message]
                for step in list(range(2, members)) + [1]:
                    e = (me + step) % members
                    remote(ans.at[k, part, e], ret.at[k, part, me], sent.at[5], b_recv.at[k, part], member(e)).start()
                ret[k, part, me] = ans[k, part, me]

    def collect(k, wanted, own=False):
        for part in wanted:
            with jax.named_scope("b_wait"):
                arrived(ret.at[k, part, pl.ds(0, members - 1)], b_recv.at[k, part])
            flat = jnp.concatenate([ret[k, part, e] for e in range(members)], axis=0)
            joined = jnp.dot(chi[k], flat, preferred_element_type=F32) + jnp.dot(clo[k], flat, preferred_element_type=F32)
            if own:
                fin[groups - 1, part] = joined.astype(BF16)
            else:
                slot = place(my_group, k)
                zo[k, part] = joined.astype(BF16)
                remote(zo.at[k, part], fin.at[slot, part], sent.at[6], f_recv.at[slot, part], relay(k)).start()

    chunks = {"o": my_group, "n": others[0], "m": others[1], "f": others[2]}
    for step in " ".join(SEQUENCE).split():
        k = chunks[step[1]]
        if step[:2] == "Fo":
            for part in [int(step[2])] if step[2:] else range(x_parts):
                forward_own(part)
        elif step[0] == "F":
            for part in [int(step[2])] if step[2:] else range(x_parts):
                forward(k, part)
        elif step[0] == "S":
            serve(k)
        else:
            collect(k, [int(step[2])] if step[2:] else range(b_parts), own=step[1] == "o")

    for part in range(b_parts):
        cut = slice(part * b_piece, (part + 1) * b_piece)
        total = stream_f32[:, cut]
        arrivals = [(groups - 1, my_group)] + [(place(g, my_group), g) for g in others]
        with jax.named_scope("f_wait"):
            for slot, _ in arrivals[1:]:
                arrived(fin.at[slot, part], f_recv.at[slot, part])
        flat = jnp.concatenate([fin[slot, part] for slot, _ in arrivals], axis=0)
        out_ref[:, cut] = (total + jnp.dot(spread_b, flat, preferred_element_type=F32)).astype(BF16)

    @pl.when(sp < p.sp - 1)
    def _():
        for copy in halo_copies:
            copy.wait_send()

    arrived(s1, sent.at[0])
    arrived(s2, sent.at[1])
    arrived(meta_out.at[pl.ds(0, groups - 1)], sent.at[2])
    arrived(zb.at[pl.ds(0, groups - 1)], sent.at[3])
    arrived(xout.at[:, :, pl.ds(0, members - 1)], sent.at[4])
    arrived(ans.at[:, :, pl.ds(0, members - 1)], sent.at[5])
    arrived(zo.at[pl.ds(0, groups - 1)], sent.at[6])


def shards(
    sp_size,
    tp_size,
    mix_in,
    resid_in,
    doc_ids,
    group_weight,
    pool_scale,
    out_weight,
    norm_gain,
    expert_ids,
    route_weights,
    w_gate,
    w_up,
    w_down,
):
    local_rows, width = mix_in.shape
    rows, d = resid_in.shape
    ff = w_gate.shape[2]
    p = Plan(sp_size, tp_size, rows)
    g, half, parts = p.groups, p.half, p.parts
    vmem = pl.BlockSpec(memory_space=pltpu.VMEM)
    hbm = pl.BlockSpec(memory_space=pl.ANY)
    dma = pltpu.SemaphoreType.DMA
    common = [
        pltpu.VMEM((local_rows, width), BF16),
        pltpu.VMEM((rows, d), BF16),
        pltpu.VMEM(group_weight.shape[1:], BF16),
        pltpu.VMEM(out_weight.shape, BF16),
        pltpu.VMEM(w_gate.shape[1:], BF16),
        pltpu.VMEM(w_up.shape[1:], BF16),
        pltpu.VMEM(w_down.shape[1:], BF16),
        pltpu.VMEM((HALO, width), BF16),
        pltpu.VMEM((1, local_rows), I32),
        pltpu.VMEM((tp_size, rows, width), BF16),
    ]
    stream_and_meta = [
        pltpu.VMEM((rows, d), F32),
        pltpu.VMEM((g, p.block, 128), F32),
        pltpu.VMEM((g, p.block, 128), F32),
    ]
    if p.chunks == g and p.groups == 4:
        body = chunk_kernel
        parts, x_parts, b_parts = PARTS
        exchange = (half, parts, rows, d // parts)
        remote_exchange = (half - 1, parts, rows, d // parts)
        slots = (g, parts, p.block, d // parts)
        scratch = common + [
            pltpu.VMEM(exchange, F32),
            pltpu.VMEM(exchange, BF16),
            pltpu.VMEM(exchange, BF16),
            pltpu.VMEM(remote_exchange, BF16),
            pltpu.VMEM(remote_exchange, BF16),
            pltpu.VMEM((rows, d), F32),
            pltpu.VMEM((g, p.block, 128), F32),
            pltpu.VMEM((g - 1, p.block, 128), F32),
            pltpu.VMEM(slots, BF16),
            pltpu.VMEM((g - 1, *slots[1:]), BF16),
            pltpu.VMEM((g, p.served, p.block), BF16),
            pltpu.VMEM((g, p.block, p.served), BF16),
            pltpu.VMEM((g, p.block, p.served), BF16),
            pltpu.VMEM((g, x_parts, p.members, p.message, d // x_parts), BF16),
            pltpu.VMEM((g, x_parts, p.members, p.message, d // x_parts), BF16),
            pltpu.VMEM((g, b_parts, p.members, p.message, d // b_parts), BF16),
            pltpu.VMEM((g, b_parts, p.members, p.message, d // b_parts), BF16),
            pltpu.VMEM((g, b_parts, p.block, d // b_parts), BF16),
            pltpu.VMEM((g, b_parts, p.block, d // b_parts), BF16),
            dma((7,)), dma((7,)),
            dma((2,)), dma((2,)),
            dma((g - 1,)),
            dma((half, parts)),
            dma((half - 1, parts)),
            dma((g - 1, parts)),
            dma((g, x_parts)),
            dma((g, b_parts)),
            dma((g - 1, b_parts)),
        ]
    else:
        body = kernel
        span_rows = p.per_chunk * p.block
        messages = (p.chunks, p.members, p.message, d)
        exchange = (half, parts, rows, d // parts)
        scratch = common + [
            pltpu.VMEM(exchange, F32),
            pltpu.VMEM(exchange, BF16),
            pltpu.VMEM(exchange, BF16),
            pltpu.VMEM(exchange, BF16),
            pltpu.VMEM(exchange, BF16),
        ] + stream_and_meta + [
            pltpu.VMEM((g, p.block, d), BF16),
            pltpu.VMEM((g, p.block, d), BF16),
            pltpu.VMEM((p.chunks, p.served, span_rows), BF16),
            pltpu.VMEM((p.chunks, span_rows, p.served), BF16),
            pltpu.VMEM((p.chunks, span_rows, p.served), BF16),
            pltpu.VMEM(messages, BF16),
            pltpu.VMEM(messages, BF16),
            pltpu.VMEM(messages, BF16),
            pltpu.VMEM(messages, BF16),
            pltpu.VMEM((g, p.block, d), BF16),
            pltpu.VMEM((g, p.block, d), BF16),
            dma((7,)),
            dma((2,)), dma((2,)),
            dma((g,)), dma((g,)),
            dma((half, parts)), dma((half, parts)),
            dma((half, parts)), dma((half, parts)),
            dma((g,)), dma((g,)),
            dma((p.chunks, p.members)), dma((p.chunks, p.members)),
            dma((p.chunks, p.members)), dma((p.chunks, p.members)),
            dma((g,)), dma((g,)),
        ]
    return pl.pallas_call(
        functools.partial(body, p),
        out_shape=pltpu.VMEM((rows, d), BF16),
        in_specs=[hbm, hbm, vmem, hbm, vmem, hbm, vmem, vmem, vmem, hbm, hbm, hbm],
        out_specs=vmem,
        scratch_shapes=scratch,
        compiler_params=pltpu.CompilerParams(
            collective_id=0, has_side_effects=True, vmem_limit_bytes=56 * 1024 * 1024
        ),
    )(
        mix_in, resid_in, doc_ids.reshape(1, -1), group_weight, pool_scale, out_weight,
        norm_gain.reshape(1, -1), expert_ids.T, route_weights.T, w_gate, w_up, w_down,
    )


def solution(mesh):
    return jax.shard_map(
        functools.partial(shards, mesh.shape["sp"], mesh.shape["tp"]),
        mesh=mesh,
        in_specs=(
            P(("grp", "sp"), "tp"),
            P(("grp", "sp", "tp"), None),
            P(("grp", "sp")),
            P("tp", None, None),
            P("tp"),
            P("tp", None),
            P(),
            P(("grp", "sp", "tp"), None),
            P(("grp", "sp", "tp"), None),
            P(("sp", "tp"), None, None),
            P(("sp", "tp"), None, None),
            P(("sp", "tp"), None, None),
        ),
        out_specs=P(("grp", "sp", "tp"), None),
        check_vma=False,
    )
```

```python
import functools

import jax
import jax.numpy as jnp
from jax import lax
from jax.experimental import pallas as pl
from jax.experimental.pallas import tpu as pltpu
from jax.sharding import PartitionSpec as P

HALO = 16
TOP_K = 2
EXPERT_GROUPS = 4
PARTS = (4, 4, 2)
SEQUENCE = ("Fm Fn Ff", "Sm Sf Cm Sn", "Cf So Bo", "Cn Co")
Z_ORDER = (((1, 0), (0, 0)), ((1, 1), (0, 1)), ((1, 2), (0, 2)), ((1, 3), (0, 3), (2, 0), (2, 1), (2, 2), (2, 3)))
SEND = [[1, 2, 3], [0, 3, 2], [3, 0, 1], [2, 1, 0]]
TABLE = [[0, 1, 2, 3], [1, 3, 0, 2], [2, 3, 0, 1], [3, 2, 0, 1]]
OWN_LATE = False
W_AT = (1, 3, 3, 3)
MESH = pl.DeviceIdType.MESH
F32 = jnp.float32
BF16 = jnp.bfloat16
I32 = jnp.int32


def iota(shape, dim):
    return lax.broadcasted_iota(I32, shape, dim)


def to_row(col):
    n = col.shape[0]
    eye = iota((n, n), 0) == iota((n, n), 1)
    return jnp.sum(jnp.where(eye, col, jnp.zeros_like(col)), axis=0, keepdims=True)


def to_col(row):
    n = row.shape[1]
    eye = iota((n, n), 0) == iota((n, n), 1)
    return jnp.sum(jnp.where(eye, row, jnp.zeros_like(row)), axis=1, keepdims=True)


def onehot(mask):
    return jnp.where(mask, 1.0, 0.0).astype(BF16)


class Plan:
    def __init__(self, sp_size, tp_size, token_rows):
        self.sp, self.tp, self.rows = sp_size, tp_size, token_rows
        self.experts = sp_size * tp_size
        self.groups = EXPERT_GROUPS
        self.span = sp_size // self.groups
        self.members = self.span * tp_size
        self.cap = max(TOP_K, 4 * token_rows // self.experts)
        self.block = min(token_rows, self.cap * self.members // TOP_K)
        if self.cap % 16 == 0:
            self.chunks, self.cap_pad = self.groups, self.cap
        else:
            self.chunks = 1
            whole = -(-self.cap * self.groups // 16) * 16
            self.cap_pad = whole // self.groups
        self.per_chunk = self.groups // self.chunks
        self.message = self.per_chunk * self.cap_pad
        self.served = self.members * self.message
        self.half = tp_size // 2
        self.parts = 2


def kernel(
    p,
    mix_hbm, resid_hbm, doc_ref, gw_hbm, scale_ref, ow_hbm, gain_ref, ids_ref, rw_ref, wg_hbm, wu_hbm, wd_hbm,
    out_ref,
    mix, resid, gw, ow, wg, wu, wd,
    halo, halo_doc, grp, keep, s1, r1, s2, r2, stream_f32, meta_out, meta_in, zb, zin, amat, chi, clo,
    xout, xin, ans, ret, zo, fin,
    load_sem, halo_send, halo_recv, m_send, m_recv, s1_send, s1_recv, s2_send, s2_recv,
    z_send, z_recv, x_send, x_recv, b_send, b_recv, f_send, f_recv,
):
    sp, tp = lax.axis_index("sp"), lax.axis_index("tp")
    local_rows, width = mix.shape
    d = resid.shape[1]
    rows, groups, half, parts = p.rows, p.groups, p.half, p.parts
    piece = d // parts
    loads = [
        pltpu.make_async_copy(src, dst, load_sem.at[i])
        for i, (src, dst) in enumerate(
            [
                (mix_hbm, mix), (gw_hbm.at[0], gw), (ow_hbm, ow), (resid_hbm, resid),
                (wg_hbm.at[0], wg), (wu_hbm.at[0], wu), (wd_hbm.at[0], wd),
            ]
        )
    ]
    for load in loads[:4]:
        load.start()

    my_group, lane_in_span = sp // p.span, sp % p.span
    me = lane_in_span * p.tp + tp
    flip = tp + 1 - 2 * (tp % 2)

    steps = [0] + sorted(range(1, groups), key=lambda step: min(step, groups - step))
    nearest = [(my_group + step) % groups for step in steps]

    def relay(group):
        return {"sp": group * p.span + lane_in_span, "tp": tp}

    def member(index):
        return {"sp": my_group * p.span + index // p.tp, "tp": index % p.tp}

    barrier = pltpu.get_barrier_semaphore()
    greeted = 0
    ahead, behind = (sp + 1) % p.sp, (sp + p.sp - 1) % p.sp
    targets = [{"sp": ahead, "tp": tp}, {"sp": behind, "tp": tp}]
    targets += [relay((my_group + off) % groups) for off in range(1, groups)]
    targets += [member((me + off) % p.members) for off in range(1, p.members)]
    for target in targets:
        pl.semaphore_signal(barrier, inc=1, device_id=target, device_id_type=MESH)
        greeted += 1

    def remote(src, dst, send, recv, device):
        return pltpu.make_async_remote_copy(
            src_ref=src, dst_ref=dst, send_sem=send, recv_sem=recv, device_id=device, device_id_type=MESH
        )

    ids = ids_ref[...]
    id0_row, id1_row = ids[0:1], ids[1:2]
    id0, id1 = to_col(id0_row), to_col(id1_row)
    earlier = iota((rows, rows), 0) < iota((rows, rows), 1)

    def rank_row(pick_row):
        hit = earlier & ((id0 == pick_row) | (id1 == pick_row))
        return jnp.sum(jnp.where(hit, 1, 0), axis=0, keepdims=True)

    group_row, group_col = id0_row // p.members, id0 // p.members
    place_row = group_row * p.block + jnp.sum(
        jnp.where(earlier & (group_col == group_row), 1, 0), axis=0, keepdims=True
    )
    offset = (my_group % p.per_chunk) * p.cap_pad

    def key_row(pick_row):
        return (pick_row % p.members) * p.message + offset + rank_row(pick_row)

    slots = groups * p.block
    chosen = iota((slots, rows), 0) == place_row
    chosen_b = onehot(chosen)
    place_col = to_col(place_row)
    spread_b = onehot(iota((rows, slots), 1) == place_col)

    def per_slot(row):
        return jnp.sum(jnp.where(chosen, row, jnp.zeros_like(row)), axis=1, keepdims=True)

    weights = rw_ref[...]
    columns = (
        (per_slot(key_row(id0_row) + 1) - 1).astype(F32),
        (per_slot(key_row(id1_row) + 1) - 1).astype(F32),
        per_slot(weights[0:1]),
        per_slot(weights[1:2]),
    )
    lane = iota((slots, 128), 1)
    meta = jnp.zeros((slots, 128), F32)
    for i, column in enumerate(columns):
        meta = jnp.where(lane == i, column, meta)
    for g in range(groups):
        meta_out[g] = meta[g * p.block : (g + 1) * p.block]

    pl.semaphore_wait(barrier, greeted)
    halo_copies = [
        remote(mix.at[pl.ds(local_rows - HALO, HALO)], halo, halo_send.at[0], halo_recv.at[0], {"sp": ahead, "tp": tp}),
        remote(doc_ref, halo_doc, halo_send.at[1], halo_recv.at[1], {"sp": ahead, "tp": tp}),
    ]
    loads[0].wait()

    @pl.when(sp < p.sp - 1)
    def _():
        for copy in halo_copies:
            copy.start()

    @pl.when(sp == 0)
    def _():
        halo[...] = jnp.zeros_like(halo)
        halo_doc[...] = jnp.zeros_like(halo_doc)


    doc_row = doc_ref[...]
    doc_col = to_col(doc_row)
    reach = jnp.left_shift(jnp.int32(2), tp)
    gap = iota((local_rows, local_rows), 0) - iota((local_rows, local_rows), 1)
    near = (doc_col == doc_row) & (gap >= 0) & (gap < reach)
    count = jnp.sum(jnp.where(near, 1.0, 0.0), axis=1, keepdims=True)
    mix_value = mix[...]
    running = jnp.dot(onehot(near), mix_value, preferred_element_type=F32)

    meta_copies = []
    for off in range(groups):
        g = nearest[off]
        if off == 0:
            copy = pltpu.make_async_copy(meta_out.at[g], meta_in.at[my_group], m_recv.at[my_group])
        else:
            copy = remote(meta_out.at[g], meta_in.at[my_group], m_send.at[g], m_recv.at[my_group], relay(g))
        copy.start()
        meta_copies.append(copy)

    @pl.when(sp > 0)
    def _():
        for copy in halo_copies:
            copy.wait_recv()

    back_gap = iota((HALO, HALO), 0) + HALO - iota((HALO, HALO), 1)
    first_reach = jnp.where(sp > 0, reach, 0)
    back = (doc_col[:HALO] == halo_doc[...][:, local_rows - HALO :]) & (back_gap < first_reach)
    head = running[:HALO] + jnp.dot(onehot(back), halo[...], preferred_element_type=F32)
    head_count = count[:HALO] + jnp.sum(jnp.where(back, 1.0, 0.0), axis=1, keepdims=True)
    running = jnp.concatenate([head, running[HALO:]], axis=0)
    count = jnp.concatenate([head_count, count[HALO:]], axis=0)
    mixed = (running / count - mix_value.astype(F32)).astype(BF16)
    loads[1].wait()
    grouped = (jnp.dot(mixed, gw[...], preferred_element_type=F32) * scale_ref[...].reshape(1, -1)).astype(BF16)
    for i in range(p.tp):
        grp[i] = grouped[i * rows : (i + 1) * rows]

    send_rows = jnp.concatenate([grp[(flip + 2 * j) % p.tp] for j in range(half)], axis=0)
    keep_rows = jnp.concatenate([grp[(tp + 2 * j) % p.tp] for j in range(half)], axis=0)
    loads[2].wait()
    first_hops = {}
    for h in range(parts):
        weight = ow[:, h * piece : (h + 1) * piece]
        product = jnp.dot(send_rows, weight, preferred_element_type=F32).astype(BF16)
        for j in reversed(range(half)):
            s1[j, h] = product[j * rows : (j + 1) * rows]
            copy = remote(s1.at[j, h], r1.at[j, h], s1_send.at[j, h], s1_recv.at[j, h], {"tp": flip})
            copy.start()
            first_hops[j, h] = copy
        kept = jnp.dot(keep_rows, weight, preferred_element_type=F32)
        for j in range(half):
            keep[j, h] = kept[j * rows : (j + 1) * rows]
    for load in loads[4:]:
        load.start()
    second_hops = {}
    for h in range(parts):
        for j in range(1, half):
            first_hops[j, h].wait_recv()
            s2[j, h] = (keep[j, h] + r1[j, h].astype(F32)).astype(BF16)
            copy = remote(
                s2.at[j, h], r2.at[j, h], s2_send.at[j, h], s2_recv.at[j, h], {"tp": (tp + 2 * j) % p.tp}
            )
            copy.start()
            second_hops[j, h] = copy

    for off in range(groups):
        b = nearest[off]
        if off == 0:
            meta_copies[0].wait()
        else:
            remote(meta_out.at[b], meta_in.at[b], m_send.at[b], m_recv.at[b], relay(b)).wait_recv()
    span_rows = p.per_chunk * p.block
    for k in range(p.chunks):
        info = jnp.concatenate([meta_in[k * p.per_chunk + i] for i in range(p.per_chunk)], axis=0)
        k0, k1 = info[:, 0:1], info[:, 1:2]
        k0_row, k1_row = to_row(k0).astype(I32), to_row(k1).astype(I32)
        target = iota((p.served, span_rows), 0)
        amat[k] = onehot((target == k0_row) | (target == k1_row))
        source = iota((span_rows, p.served), 1)
        combine = jnp.where(source == k0.astype(I32), info[:, 2:3], 0.0) + jnp.where(
            source == k1.astype(I32), info[:, 3:4], 0.0
        )
        high = combine.astype(BF16)
        chi[k] = high
        clo[k] = (combine - high.astype(F32)).astype(BF16)

    loads[3].wait()
    total = jnp.zeros((rows, 1), F32)
    for h in range(parts):
        cut = slice(h * piece, (h + 1) * piece)
        first_hops[0, h].wait_recv()
        summed = keep[0, h] + r1[0, h].astype(F32)
        for j in range(1, half):
            second_hops[j, h].wait_recv()
            summed = summed + r2[j, h].astype(F32)
        stream = (resid[:, cut].astype(F32) + summed).astype(BF16)
        stream_f = stream.astype(F32)
        stream_f32[:, cut] = stream_f
        total = total + jnp.sum(stream_f * stream_f, axis=1, keepdims=True)
    normed = (stream_f32[...] * lax.rsqrt(total / d + 1e-06) * gain_ref[...]).astype(BF16)

    gathered = jnp.dot(chosen_b, normed, preferred_element_type=F32).astype(BF16)
    for g in range(groups):
        zb[g] = gathered[g * p.block : (g + 1) * p.block]
    z_copies = []
    for off in range(groups):
        g = nearest[off]
        if off == 0:
            copy = pltpu.make_async_copy(zb.at[g], zin.at[my_group], z_recv.at[my_group])
        else:
            copy = remote(zb.at[g], zin.at[my_group], z_send.at[g], z_recv.at[my_group], relay(g))
        copy.start()
        z_copies.append(copy)

    if p.chunks == groups:
        order = [[off] for off in range(groups)]
    else:
        order = [list(range(groups))]

    x_copies, b_copies, f_copies = [], [], []

    def forward(offs):
        k = nearest[offs[0]] if p.chunks > 1 else 0
        for off in offs:
            b = nearest[off]
            if off == 0:
                z_copies[0].wait()
            else:
                remote(zb.at[b], zin.at[b], z_send.at[b], z_recv.at[b], relay(b)).wait_recv()
        if p.chunks > 1:
            source = zin[k]
        else:
            source = jnp.concatenate([zin[i] for i in range(groups)], axis=0)
        picked = jnp.dot(amat[k], source, preferred_element_type=F32).astype(BF16)
        for e in range(p.members):
            xout[k, e] = picked[e * p.message : (e + 1) * p.message]
        for step in range(p.members):
            e = (me + step) % p.members
            if step == 0:
                copy = pltpu.make_async_copy(xout.at[k, e], xin.at[k, me], x_recv.at[k, me])
            else:
                copy = remote(xout.at[k, e], xin.at[k, me], x_send.at[k, e], x_recv.at[k, me], member(e))
            copy.start()
            x_copies.append((step, copy))

    def serve(n, offs):
        k = nearest[offs[0]] if p.chunks > 1 else 0
        for step in range(p.members):
            e = (me + step) % p.members
            if step == 0:
                x_copies[n * p.members][1].wait()
            else:
                remote(xout.at[k, e], xin.at[k, e], x_send.at[k, e], x_recv.at[k, e], member(e)).wait_recv()
        if n == 0:
            for i in (4, 5, 6):
                loads[i].wait()
        flat = jnp.concatenate([xin[k, e] for e in range(p.members)], axis=0)
        gate_part = jnp.dot(flat, wg[...], preferred_element_type=F32)
        up_part = jnp.dot(flat, wu[...], preferred_element_type=F32)
        hidden = (gate_part * jax.nn.sigmoid(gate_part) * up_part).astype(BF16)
        answer = jnp.dot(hidden, wd[...], preferred_element_type=F32).astype(BF16)
        for e in range(p.members):
            ans[k, e] = answer[e * p.message : (e + 1) * p.message]
        for step in range(p.members):
            e = (me + step) % p.members
            if step == 0:
                copy = pltpu.make_async_copy(ans.at[k, e], ret.at[k, me], b_recv.at[k, me])
            else:
                copy = remote(ans.at[k, e], ret.at[k, me], b_send.at[k, e], b_recv.at[k, me], member(e))
            copy.start()
            b_copies.append((step, copy))

    def collect(n, offs):
        k = nearest[offs[0]] if p.chunks > 1 else 0
        for step in range(p.members):
            e = (me + step) % p.members
            if step == 0:
                b_copies[n * p.members][1].wait()
            else:
                remote(ans.at[k, e], ret.at[k, e], b_send.at[k, e], b_recv.at[k, e], member(e)).wait_recv()
        flat = jnp.concatenate([ret[k, e] for e in range(p.members)], axis=0)
        joined = jnp.dot(chi[k], flat, preferred_element_type=F32) + jnp.dot(clo[k], flat, preferred_element_type=F32)
        joined = joined.astype(BF16)
        if p.chunks > 1:
            zo[k] = joined
        else:
            for i in range(groups):
                zo[i] = joined[i * p.block : (i + 1) * p.block]
        for off in offs:
            b = nearest[off]
            if off == 0:
                copy = pltpu.make_async_copy(zo.at[b], fin.at[my_group], f_recv.at[my_group])
            else:
                copy = remote(zo.at[b], fin.at[my_group], f_send.at[b], f_recv.at[my_group], relay(b))
            copy.start()
            f_copies.append((off, copy))

    count_chunks = len(order)
    forward(order[0])
    for n in range(count_chunks):
        if n + 1 < count_chunks:
            forward(order[n + 1])
        serve(n, order[n])
        if n >= 1:
            collect(n - 1, order[n - 1])
    collect(count_chunks - 1, order[-1])

    for off in range(groups):
        g = nearest[off]
        if off == 0:
            [copy for o, copy in f_copies if o == 0][0].wait()
        else:
            remote(zo.at[g], fin.at[g], f_send.at[g], f_recv.at[g], relay(g)).wait_recv()
    flat = jnp.concatenate([fin[g] for g in range(groups)], axis=0)
    out_ref[...] = (stream_f32[...] + jnp.dot(spread_b, flat, preferred_element_type=F32)).astype(BF16)

    @pl.when(sp < p.sp - 1)
    def _():
        for copy in halo_copies:
            copy.wait_send()

    for copy in meta_copies[1:] + list(first_hops.values()) + list(second_hops.values()) + z_copies[1:]:
        copy.wait_send()
    for step, copy in x_copies + b_copies + f_copies:
        if step:
            copy.wait_send()


def ordered(position, table):
    n = len(table)
    return [
        sum((1 - ((position - z + n) % n + n - 1) // n) * table[z][i] for z in range(n)) for i in range(len(table[0]))
    ]


def chunk_kernel(
    p,
    mix_hbm, resid_hbm, doc_ref, gw_hbm, scale_ref, ow_hbm, gain_ref, ids_ref, rw_ref, wg_hbm, wu_hbm, wd_hbm,
    out_ref,
    mix, resid, gw, ow, wg, wu, wd,
    halo, halo_doc, grp, keep, s1, r1, s2, r2, stream_f32, meta_out, meta_in, zb, zin, amat, chi, clo,
    xout, xin, gates, ups, levels, ans, ret, zo, fin,
    load_sem, sent, halo_send, halo_recv, m_recv, s1_recv, s2_recv, z_recv, x_recv, b_recv, f_recv, far,
):
    sp, tp = lax.axis_index("sp"), lax.axis_index("tp")
    local_rows, width = mix.shape
    d = resid.shape[1]
    rows, groups, half, members = p.rows, p.groups, p.half, p.members
    parts, x_parts, b_parts = zb.shape[1], xout.shape[1], ans.shape[1]
    piece, x_piece, b_piece = d // parts, d // x_parts, d // b_parts
    loads = [
        pltpu.make_async_copy(src, dst, load_sem.at[i])
        for i, (src, dst) in enumerate(
            [
                (mix_hbm, mix), (gw_hbm.at[0], gw), (ow_hbm, ow), (resid_hbm, resid),
                (wg_hbm.at[0], wg), (wu_hbm.at[0], wu), (wd_hbm.at[0], wd),
            ]
        )
    ]

    my_group, lane_in_span = sp // p.span, sp % p.span
    me = lane_in_span * p.tp + tp
    flip = tp + 1 - 2 * (tp % 2)
    order = ordered(my_group, TABLE)
    others = order[1:]
    receivers = ordered(my_group, SEND)

    def relay(group):
        return {"sp": group * p.span + lane_in_span, "tp": tp}

    def member(index):
        return {"sp": my_group * p.span + index // p.tp, "tp": index % p.tp}

    barrier = pltpu.get_barrier_semaphore()
    has_ahead, has_behind = (2 * p.sp - 2 - sp) // p.sp, (sp + p.sp - 1) // p.sp
    ahead = (sp + 1) % p.sp

    def greet(semaphore):
        @pl.when(sp < p.sp - 1)
        def _():
            pl.semaphore_signal(semaphore, inc=1, device_id={"sp": sp + 1, "tp": tp}, device_id_type=MESH)

        @pl.when(sp > 0)
        def _():
            pl.semaphore_signal(semaphore, inc=1, device_id={"sp": sp - 1, "tp": tp}, device_id_type=MESH)

    greet(barrier)
    for off in range(1, members):
        pl.semaphore_signal(barrier, inc=1, device_id=member((me + off) % members), device_id_type=MESH)
    def weights_now(stage):
        for load, when in zip(loads[3:], W_AT):
            if when == stage:
                load.start()

    for load in loads[:3]:
        load.start()
    weights_now(0)

    def remote(src, dst, send, recv, device):
        return pltpu.make_async_remote_copy(
            src_ref=src, dst_ref=dst, send_sem=send, recv_sem=recv, device_id=device, device_id_type=MESH
        )

    doc_row = doc_ref[...]
    doc_col = to_col(doc_row)
    reach = jnp.left_shift(jnp.int32(2), tp)
    gap = iota((local_rows, local_rows), 0) - iota((local_rows, local_rows), 1)
    near = (doc_col == doc_row) & (gap >= 0) & (gap < reach)
    count = jnp.sum(jnp.where(near, 1.0, 0.0), axis=1, keepdims=True)
    near_b = onehot(near)
    loads[0].wait()
    running = jnp.dot(near_b, mix[...], preferred_element_type=F32)
    mixed = (running / count - mix[...].astype(F32)).astype(BF16)
    loads[1].wait()
    scale = scale_ref[...].reshape(1, -1)
    grouped = (jnp.dot(mixed, gw[...], preferred_element_type=F32) * scale).astype(BF16)
    for i in range(p.tp):
        grp[i] = grouped[i * rows : (i + 1) * rows]

    with jax.named_scope("barrier"):
        pl.semaphore_wait(barrier, members - 1 + has_ahead + has_behind)
    halo_copies = [
        remote(mix.at[pl.ds(local_rows - HALO, HALO)], halo, halo_send.at[0], halo_recv.at[0], {"sp": ahead, "tp": tp}),
        remote(doc_ref, halo_doc, halo_send.at[1], halo_recv.at[1], {"sp": ahead, "tp": tp}),
    ]

    @pl.when(sp < p.sp - 1)
    def _():
        for copy in halo_copies:
            copy.start()

    @pl.when(sp == 0)
    def _():
        halo[...] = jnp.zeros_like(halo)
        halo_doc[...] = jnp.zeros_like(halo_doc)

    greet(far.at[0])


    send_rows = jnp.concatenate([grp[(flip + 2 * j) % p.tp] for j in range(half)], axis=0)
    keep_rows = jnp.concatenate([grp[(tp + 2 * j) % p.tp] for j in range(half)], axis=0)
    loads[2].wait()
    for h in range(parts):
        weight = ow[:, h * piece : (h + 1) * piece]
        product = jnp.dot(send_rows, weight, preferred_element_type=F32).astype(BF16)
        for j in range(half):
            s1[j, h] = product[j * rows : (j + 1) * rows]
        kept = jnp.dot(keep_rows, weight, preferred_element_type=F32)
        for j in range(half):
            keep[j, h] = kept[j * rows : (j + 1) * rows]

    def arrived(ref, semaphore):
        pltpu.make_async_copy(ref, ref, semaphore).wait()

    def place(source, target):
        return (target - source + groups) % groups - 1


    first_hops = {
        (j, h): remote(s1.at[j, h], r1.at[j, h], sent.at[0], s1_recv.at[j, h], {"tp": flip})
        for j in range(half)
        for h in range(parts)
    }
    second_hops = {
        (j, h): remote(
            s2.at[j - 1, h], r2.at[j - 1, h], sent.at[1], s2_recv.at[j - 1, h], {"tp": (tp + 2 * j) % p.tp}
        )
        for j in range(1, half)
        for h in range(parts)
    }

    def send_first():
        for j in reversed(range(half)):

            @pl.when((flip + 2 * j) % p.tp > 0)
            def _():
                for h in range(parts):
                    first_hops[j, h].start()

    def send_second(late):
        for j in range(1, half):
            block = (tp + 2 * j) % p.tp

            @pl.when((block == 0) if late else (block > 0))
            def _():
                for h in range(parts):
                    with jax.named_scope("fh_wait"):
                        first_hops[j, h].wait_recv()
                    s2[j - 1, h] = (keep[j, h] + r1[j, h].astype(F32)).astype(BF16)
                    second_hops[j, h].start()

    send_first()
    for turn in range(1, p.sp - 2):
        pl.semaphore_wait(far.at[turn - 1], has_ahead + has_behind)
        greet(far.at[turn])
    weights_now(1)

    ids = ids_ref[...]
    id0_row, id1_row = ids[0:1], ids[1:2]
    id0, id1 = to_col(id0_row), to_col(id1_row)
    earlier = iota((rows, rows), 0) < iota((rows, rows), 1)

    def rank_row(pick_row):
        hit = earlier & ((id0 == pick_row) | (id1 == pick_row))
        return jnp.sum(jnp.where(hit, 1, 0), axis=0, keepdims=True)

    group_row, group_col = id0_row // members, id0 // members
    place_row = group_row * p.block + jnp.sum(
        jnp.where(earlier & (group_col == group_row), 1, 0), axis=0, keepdims=True
    )

    def key_row(pick_row):
        return (pick_row % members) * p.message + rank_row(pick_row)

    slots = groups * p.block
    chosen = iota((slots, rows), 0) == place_row
    chosen_b = onehot(chosen)
    place_col = to_col(place_row)
    spread_order = jnp.concatenate([my_group * p.block + iota((1, p.block), 1)] + [g * p.block + iota((1, p.block), 1) for g in others], axis=1)
    spread_b = onehot(spread_order == place_col)

    def per_slot(row):
        return jnp.sum(jnp.where(chosen, row, jnp.zeros_like(row)), axis=1, keepdims=True)

    weights = rw_ref[...]
    columns = (
        (per_slot(key_row(id0_row) + 1) - 1).astype(F32),
        (per_slot(key_row(id1_row) + 1) - 1).astype(F32),
        per_slot(weights[0:1]),
        per_slot(weights[1:2]),
    )
    lane = iota((slots, 128), 1)
    meta = jnp.zeros((slots, 128), F32)
    for i, column in enumerate(columns):
        meta = jnp.where(lane == i, column, meta)
    for g in range(groups):
        meta_out[g] = meta[g * p.block : (g + 1) * p.block]
    send_second(False)
    weights_now(2)

    @pl.when(sp > 0)
    def _():
        for copy in halo_copies:
            with jax.named_scope("halo_wait"):
                copy.wait_recv()

    back_gap = iota((HALO, HALO), 0) + HALO - iota((HALO, HALO), 1)
    first_reach = jnp.where(sp > 0, reach, 0)
    back = (doc_col[:HALO] == halo_doc[...][:, local_rows - HALO :]) & (back_gap < first_reach)
    head = running[:HALO] + jnp.dot(onehot(back), halo[...], preferred_element_type=F32)
    head_count = count[:HALO] + jnp.sum(jnp.where(back, 1.0, 0.0), axis=1, keepdims=True)
    head_mixed = (head / head_count - mix[:HALO].astype(F32)).astype(BF16)
    head_grouped = (jnp.dot(head_mixed, gw[...], preferred_element_type=F32) * scale).astype(BF16)
    keep_slot = ((p.tp - tp) % p.tp) // 2
    send_slot = ((p.tp - flip) % p.tp) // 2
    for h in range(parts):
        weight = ow[:, h * piece : (h + 1) * piece]
        head_product = jnp.dot(head_grouped, weight, preferred_element_type=F32)

        @pl.when(tp % 2 == 0)
        def _():
            keep[keep_slot, h, :HALO] = head_product

        @pl.when(tp % 2 == 1)
        def _():
            s1[send_slot, h, :HALO] = head_product.astype(BF16)
            remote(
                s1.at[send_slot, h], r1.at[send_slot, h], sent.at[0], s1_recv.at[send_slot, h], {"tp": flip}
            ).start()

    with jax.named_scope("far"):
        pl.semaphore_wait(far.at[p.sp - 3], has_ahead + has_behind)
    for g in others:
        slot = place(my_group, g)
        remote(meta_out.at[g], meta_in.at[slot], sent.at[2], m_recv.at[slot], relay(g)).start()

    send_second(True)
    weights_now(3)

    def tables(k, info):
        k0, k1 = info[:, 0:1], info[:, 1:2]
        k0_row, k1_row = to_row(k0).astype(I32), to_row(k1).astype(I32)
        target = iota((p.served, p.block), 0)
        amat[k] = onehot((target == k0_row) | (target == k1_row))
        source = iota((p.block, p.served), 1)
        combine = jnp.where(source == k0.astype(I32), info[:, 2:3], 0.0) + jnp.where(
            source == k1.astype(I32), info[:, 3:4], 0.0
        )
        high = combine.astype(BF16)
        chi[k] = high
        clo[k] = (combine - high.astype(F32)).astype(BF16)

    tables(my_group, meta_out[my_group])
    ratio = parts // x_parts

    def forward_part(k, part, source):
        picked = jnp.dot(amat[k], source, preferred_element_type=F32).astype(BF16)
        for e in range(members):
            xout[k, part, e] = picked[e * p.message : (e + 1) * p.message]
        for step in list(range(2, members)) + [1]:
            e = (me + step) % members
            remote(xout.at[k, part, e], xin.at[k, part, me], sent.at[4], x_recv.at[k, part], member(e)).start()
        xin[k, part, me] = xout[k, part, me]

    def send_z(g, h):
        slot = place(my_group, g)
        remote(zb.at[g, h], zin.at[slot, h], sent.at[3], z_recv.at[slot, h], relay(g)).start()

    def forward_own(part):
        source = jnp.concatenate([zb[my_group, i] for i in range(part * ratio, (part + 1) * ratio)], axis=1)
        forward_part(my_group, part, source)

    loads[3].wait()
    for h in range(parts):
        weights_now(4 + h)
        cut = slice(h * piece, (h + 1) * piece)
        with jax.named_scope("fh0_wait"):
            first_hops[0, h].wait_recv()
        summed = keep[0, h] + r1[0, h].astype(F32)
        for j in range(1, half):
            with jax.named_scope("sh_wait"):
                second_hops[j, h].wait_recv()
            summed = summed + r2[j - 1, h].astype(F32)
        stream = (resid[:, cut].astype(F32) + summed).astype(BF16)
        stream_f32[:, cut] = stream.astype(F32)
        gathered = jnp.dot(chosen_b, stream, preferred_element_type=F32).astype(BF16)
        for g in range(groups):
            zb[g, h] = gathered[g * p.block : (g + 1) * p.block]
        for position, part in Z_ORDER[h]:
            send_z(receivers[position], part)
        if h % ratio == ratio - 1 and not OWN_LATE:
            forward_own(h // ratio)

    for g in others:
        with jax.named_scope("m_wait"):
            slot = place(g, my_group)
            arrived(meta_in.at[slot], m_recv.at[slot])
        tables(g, meta_in[slot])

    def forward(k, part):
        slot = place(k, my_group)
        for h in range(part * ratio, (part + 1) * ratio):
            with jax.named_scope("z_wait"):
                arrived(zin.at[slot, h], z_recv.at[slot, h])
        source = jnp.concatenate([zin[slot, i] for i in range(part * ratio, (part + 1) * ratio)], axis=1)
        forward_part(k, part, source)

    waited, absorbed = [], set()

    def absorb(k, name, part):
        with jax.named_scope("x_wait"):
            arrived(xin.at[k, part, pl.ds(0, members - 1)], x_recv.at[k, part])
        if not waited:
            waited.append(True)
            for i in (4, 5, 6):
                loads[i].wait()
        cut = slice(part * x_piece, (part + 1) * x_piece)
        flat = jnp.concatenate([xin[k, part, e] for e in range(members)], axis=0).astype(F32)
        level = jnp.broadcast_to(jnp.sum(flat * flat, axis=1, keepdims=True), (p.served, 128))
        scaled = (flat * gain_ref[:, cut]).astype(BF16)
        gate_part = jnp.dot(scaled, wg[cut], preferred_element_type=F32)
        up_part = jnp.dot(scaled, wu[cut], preferred_element_type=F32)
        if part == 0:
            levels[k], gates[k], ups[k] = level, gate_part, up_part
        else:
            levels[k] += level
            gates[k] += gate_part
            ups[k] += up_part
        absorbed.add((name, part))

    def answer_back(k, part):
        for step in list(range(2, members)) + [1]:
            e = (me + step) % members
            remote(ans.at[k, part, e], ret.at[k, part, me], sent.at[5], b_recv.at[k, part], member(e)).start()

    def serve(k, name):
        for part in range(x_parts):
            if (name, part) not in absorbed:
                absorb(k, name, part)
        with jax.named_scope("expert"):
            factor = lax.rsqrt(levels[k][:, :1] / d + 1e-06)
            gate_part = gates[k] * factor
            hidden = (gate_part * jax.nn.sigmoid(gate_part) * (ups[k] * factor)).astype(BF16)
            for part in range(b_parts):
                weight = wd[:, part * b_piece : (part + 1) * b_piece]
                answer = jnp.dot(hidden, weight, preferred_element_type=F32).astype(BF16)
                for e in range(members):
                    ans[k, part, e] = answer[e * p.message : (e + 1) * p.message]
                if name != "o":
                    answer_back(k, part)
                ret[k, part, me] = ans[k, part, me]

    def collect(k, wanted, own=False):
        for part in wanted:
            with jax.named_scope("b_wait"):
                arrived(ret.at[k, part, pl.ds(0, members - 1)], b_recv.at[k, part])
            flat = jnp.concatenate([ret[k, part, e] for e in range(members)], axis=0)
            joined = jnp.dot(chi[k], flat, preferred_element_type=F32) + jnp.dot(clo[k], flat, preferred_element_type=F32)
            if own:
                fin[groups - 1, part] = joined.astype(BF16)
            else:
                slot = place(my_group, k)
                zo[k, part] = joined.astype(BF16)
                remote(zo.at[k, part], fin.at[slot, part], sent.at[6], f_recv.at[slot, part], relay(k)).start()

    weights_now(4 + parts)
    chunks = {"o": my_group, "n": others[0], "m": others[1], "f": others[2]}
    for step in " ".join(SEQUENCE).split():
        k = chunks[step[1]]
        if step[:2] == "Fo":
            for part in [int(step[2])] if step[2:] else range(x_parts):
                forward_own(part)
        elif step[0] == "F":
            for part in [int(step[2])] if step[2:] else range(x_parts):
                forward(k, part)
        elif step[0] == "E":
            for part in [int(step[2])] if step[2:] else range(x_parts):
                absorb(k, step[1], part)
        elif step[0] == "B":
            for part in [int(step[2])] if step[2:] else range(b_parts):
                answer_back(k, part)
        elif step[0] == "S":
            serve(k, step[1])
        else:
            collect(k, [int(step[2])] if step[2:] else range(b_parts), own=step[1] == "o")

    for part in range(b_parts):
        cut = slice(part * b_piece, (part + 1) * b_piece)
        total = stream_f32[:, cut]
        arrivals = [(groups - 1, my_group)] + [(place(g, my_group), g) for g in others]
        with jax.named_scope("f_wait"):
            for slot, _ in arrivals[1:]:
                arrived(fin.at[slot, part], f_recv.at[slot, part])
        flat = jnp.concatenate([fin[slot, part] for slot, _ in arrivals], axis=0)
        out_ref[:, cut] = (total + jnp.dot(spread_b, flat, preferred_element_type=F32)).astype(BF16)

    @pl.when(sp < p.sp - 1)
    def _():
        for copy in halo_copies:
            copy.wait_send()

    arrived(s1, sent.at[0])
    arrived(s2, sent.at[1])
    arrived(meta_out.at[pl.ds(0, groups - 1)], sent.at[2])
    arrived(zb.at[pl.ds(0, groups - 1)], sent.at[3])
    arrived(xout.at[:, :, pl.ds(0, members - 1)], sent.at[4])
    arrived(ans.at[:, :, pl.ds(0, members - 1)], sent.at[5])
    arrived(zo.at[pl.ds(0, groups - 1)], sent.at[6])


def shards(
    sp_size,
    tp_size,
    mix_in,
    resid_in,
    doc_ids,
    group_weight,
    pool_scale,
    out_weight,
    norm_gain,
    expert_ids,
    route_weights,
    w_gate,
    w_up,
    w_down,
):
    local_rows, width = mix_in.shape
    rows, d = resid_in.shape
    ff = w_gate.shape[2]
    p = Plan(sp_size, tp_size, rows)
    g, half, parts = p.groups, p.half, p.parts
    vmem = pl.BlockSpec(memory_space=pltpu.VMEM)
    hbm = pl.BlockSpec(memory_space=pl.ANY)
    dma = pltpu.SemaphoreType.DMA
    common = [
        pltpu.VMEM((local_rows, width), BF16),
        pltpu.VMEM((rows, d), BF16),
        pltpu.VMEM(group_weight.shape[1:], BF16),
        pltpu.VMEM(out_weight.shape, BF16),
        pltpu.VMEM(w_gate.shape[1:], BF16),
        pltpu.VMEM(w_up.shape[1:], BF16),
        pltpu.VMEM(w_down.shape[1:], BF16),
        pltpu.VMEM((HALO, width), BF16),
        pltpu.VMEM((1, local_rows), I32),
        pltpu.VMEM((tp_size, rows, width), BF16),
    ]
    stream_and_meta = [
        pltpu.VMEM((rows, d), F32),
        pltpu.VMEM((g, p.block, 128), F32),
        pltpu.VMEM((g, p.block, 128), F32),
    ]
    if p.chunks == g and sp_size == g == 4:
        body = chunk_kernel
        parts, x_parts, b_parts = PARTS
        exchange = (half, parts, rows, d // parts)
        remote_exchange = (half - 1, parts, rows, d // parts)
        slots = (g, parts, p.block, d // parts)
        scratch = common + [
            pltpu.VMEM(exchange, F32),
            pltpu.VMEM(exchange, BF16),
            pltpu.VMEM(exchange, BF16),
            pltpu.VMEM(remote_exchange, BF16),
            pltpu.VMEM(remote_exchange, BF16),
            pltpu.VMEM((rows, d), F32),
            pltpu.VMEM((g, p.block, 128), F32),
            pltpu.VMEM((g - 1, p.block, 128), F32),
            pltpu.VMEM(slots, BF16),
            pltpu.VMEM((g - 1, *slots[1:]), BF16),
            pltpu.VMEM((g, p.served, p.block), BF16),
            pltpu.VMEM((g, p.block, p.served), BF16),
            pltpu.VMEM((g, p.block, p.served), BF16),
            pltpu.VMEM((g, x_parts, p.members, p.message, d // x_parts), BF16),
            pltpu.VMEM((g, x_parts, p.members, p.message, d // x_parts), BF16),
            pltpu.VMEM((g, p.served, w_gate.shape[2]), F32),
            pltpu.VMEM((g, p.served, w_gate.shape[2]), F32),
            pltpu.VMEM((g, p.served, 128), F32),
            pltpu.VMEM((g, b_parts, p.members, p.message, d // b_parts), BF16),
            pltpu.VMEM((g, b_parts, p.members, p.message, d // b_parts), BF16),
            pltpu.VMEM((g, b_parts, p.block, d // b_parts), BF16),
            pltpu.VMEM((g, b_parts, p.block, d // b_parts), BF16),
            dma((7,)), dma((7,)),
            dma((2,)), dma((2,)),
            dma((g - 1,)),
            dma((half, parts)),
            dma((half - 1, parts)),
            dma((g - 1, parts)),
            dma((g, x_parts)),
            dma((g, b_parts)),
            dma((g - 1, b_parts)),
            pltpu.SemaphoreType.REGULAR((sp_size - 2,)),
        ]
    else:
        body = kernel
        span_rows = p.per_chunk * p.block
        messages = (p.chunks, p.members, p.message, d)
        exchange = (half, parts, rows, d // parts)
        scratch = common + [
            pltpu.VMEM(exchange, F32),
            pltpu.VMEM(exchange, BF16),
            pltpu.VMEM(exchange, BF16),
            pltpu.VMEM(exchange, BF16),
            pltpu.VMEM(exchange, BF16),
        ] + stream_and_meta + [
            pltpu.VMEM((g, p.block, d), BF16),
            pltpu.VMEM((g, p.block, d), BF16),
            pltpu.VMEM((p.chunks, p.served, span_rows), BF16),
            pltpu.VMEM((p.chunks, span_rows, p.served), BF16),
            pltpu.VMEM((p.chunks, span_rows, p.served), BF16),
            pltpu.VMEM(messages, BF16),
            pltpu.VMEM(messages, BF16),
            pltpu.VMEM(messages, BF16),
            pltpu.VMEM(messages, BF16),
            pltpu.VMEM((g, p.block, d), BF16),
            pltpu.VMEM((g, p.block, d), BF16),
            dma((7,)),
            dma((2,)), dma((2,)),
            dma((g,)), dma((g,)),
            dma((half, parts)), dma((half, parts)),
            dma((half, parts)), dma((half, parts)),
            dma((g,)), dma((g,)),
            dma((p.chunks, p.members)), dma((p.chunks, p.members)),
            dma((p.chunks, p.members)), dma((p.chunks, p.members)),
            dma((g,)), dma((g,)),
        ]
    return pl.pallas_call(
        functools.partial(body, p),
        out_shape=pltpu.VMEM((rows, d), BF16),
        in_specs=[hbm, hbm, vmem, hbm, vmem, hbm, vmem, vmem, vmem, hbm, hbm, hbm],
        out_specs=vmem,
        scratch_shapes=scratch,
        compiler_params=pltpu.CompilerParams(
            collective_id=0, has_side_effects=True, vmem_limit_bytes=56 * 1024 * 1024
        ),
    )(
        mix_in, resid_in, doc_ids.reshape(1, -1), group_weight, pool_scale, out_weight,
        norm_gain.reshape(1, -1), expert_ids.T, route_weights.T, w_gate, w_up, w_down,
    )


def solution(mesh):
    return jax.shard_map(
        functools.partial(shards, mesh.shape["sp"], mesh.shape["tp"]),
        mesh=mesh,
        in_specs=(
            P(("grp", "sp"), "tp"),
            P(("grp", "sp", "tp"), None),
            P(("grp", "sp")),
            P("tp", None, None),
            P("tp"),
            P("tp", None),
            P(),
            P(("grp", "sp", "tp"), None),
            P(("grp", "sp", "tp"), None),
            P(("sp", "tp"), None, None),
            P(("sp", "tp"), None, None),
            P(("sp", "tp"), None, None),
        ),
        out_specs=P(("grp", "sp", "tp"), None),
        check_vma=False,
    )
```

```python
import functools

import jax
import jax.numpy as jnp
from jax import lax
from jax.experimental import pallas as pl
from jax.experimental.pallas import tpu as pltpu
from jax.sharding import PartitionSpec as P

HALO = 16
TOP_K = 2
EXPERT_GROUPS = 4
PARTS = (4, 4, 2)
SEQUENCE = ("Fm Fn Ff", "Sm Sf En Eo", "Cm Sn Cf", "So Bo", "Cn Co")
Z_ORDER = (((1, 0), (0, 0)), ((1, 1), (0, 1)), ((1, 2), (0, 2)), ((1, 3), (0, 3), (2, 0), (2, 1), (2, 2), (2, 3)))
SEND = [[1, 2, 3], [0, 3, 2], [3, 0, 1], [2, 0, 1]]
TABLE = [[0, 1, 3, 2], [1, 3, 0, 2], [2, 3, 0, 1], [3, 2, 0, 1]]
OWN_LATE = False
W_AT = (1, 3, 3, 3)
MESH = pl.DeviceIdType.MESH
F32 = jnp.float32
BF16 = jnp.bfloat16
I32 = jnp.int32


def iota(shape, dim):
    return lax.broadcasted_iota(I32, shape, dim)


def to_row(col):
    n = col.shape[0]
    eye = iota((n, n), 0) == iota((n, n), 1)
    return jnp.sum(jnp.where(eye, col, jnp.zeros_like(col)), axis=0, keepdims=True)


def to_col(row):
    n = row.shape[1]
    eye = iota((n, n), 0) == iota((n, n), 1)
    return jnp.sum(jnp.where(eye, row, jnp.zeros_like(row)), axis=1, keepdims=True)


def onehot(mask):
    return jnp.where(mask, 1.0, 0.0).astype(BF16)


class Plan:
    def __init__(self, sp_size, tp_size, token_rows):
        self.sp, self.tp, self.rows = sp_size, tp_size, token_rows
        self.experts = sp_size * tp_size
        self.groups = EXPERT_GROUPS
        self.span = sp_size // self.groups
        self.members = self.span * tp_size
        self.cap = max(TOP_K, 4 * token_rows // self.experts)
        self.block = min(token_rows, self.cap * self.members // TOP_K)
        if self.cap % 16 == 0:
            self.chunks, self.cap_pad = self.groups, self.cap
        else:
            self.chunks = 1
            whole = -(-self.cap * self.groups // 16) * 16
            self.cap_pad = whole // self.groups
        self.per_chunk = self.groups // self.chunks
        self.message = self.per_chunk * self.cap_pad
        self.served = self.members * self.message
        self.half = tp_size // 2
        self.parts = 2


def kernel(
    p,
    mix_hbm, resid_hbm, doc_ref, gw_hbm, scale_ref, ow_hbm, gain_ref, ids_ref, rw_ref, wg_hbm, wu_hbm, wd_hbm,
    out_ref,
    mix, resid, gw, ow, wg, wu, wd,
    halo, halo_doc, grp, keep, s1, r1, s2, r2, stream_f32, meta_out, meta_in, zb, zin, amat, chi, clo,
    xout, xin, ans, ret, zo, fin,
    load_sem, halo_send, halo_recv, m_send, m_recv, s1_send, s1_recv, s2_send, s2_recv,
    z_send, z_recv, x_send, x_recv, b_send, b_recv, f_send, f_recv,
):
    sp, tp = lax.axis_index("sp"), lax.axis_index("tp")
    local_rows, width = mix.shape
    d = resid.shape[1]
    rows, groups, half, parts = p.rows, p.groups, p.half, p.parts
    piece = d // parts
    loads = [
        pltpu.make_async_copy(src, dst, load_sem.at[i])
        for i, (src, dst) in enumerate(
            [
                (mix_hbm, mix), (gw_hbm.at[0], gw), (ow_hbm, ow), (resid_hbm, resid),
                (wg_hbm.at[0], wg), (wu_hbm.at[0], wu), (wd_hbm.at[0], wd),
            ]
        )
    ]
    for load in loads[:4]:
        load.start()

    my_group, lane_in_span = sp // p.span, sp % p.span
    me = lane_in_span * p.tp + tp
    flip = tp + 1 - 2 * (tp % 2)

    steps = [0] + sorted(range(1, groups), key=lambda step: min(step, groups - step))
    nearest = [(my_group + step) % groups for step in steps]

    def relay(group):
        return {"sp": group * p.span + lane_in_span, "tp": tp}

    def member(index):
        return {"sp": my_group * p.span + index // p.tp, "tp": index % p.tp}

    barrier = pltpu.get_barrier_semaphore()
    greeted = 0
    ahead, behind = (sp + 1) % p.sp, (sp + p.sp - 1) % p.sp
    targets = [{"sp": ahead, "tp": tp}, {"sp": behind, "tp": tp}]
    targets += [relay((my_group + off) % groups) for off in range(1, groups)]
    targets += [member((me + off) % p.members) for off in range(1, p.members)]
    for target in targets:
        pl.semaphore_signal(barrier, inc=1, device_id=target, device_id_type=MESH)
        greeted += 1

    def remote(src, dst, send, recv, device):
        return pltpu.make_async_remote_copy(
            src_ref=src, dst_ref=dst, send_sem=send, recv_sem=recv, device_id=device, device_id_type=MESH
        )

    ids = ids_ref[...]
    id0_row, id1_row = ids[0:1], ids[1:2]
    id0, id1 = to_col(id0_row), to_col(id1_row)
    earlier = iota((rows, rows), 0) < iota((rows, rows), 1)

    def rank_row(pick_row):
        hit = earlier & ((id0 == pick_row) | (id1 == pick_row))
        return jnp.sum(jnp.where(hit, 1, 0), axis=0, keepdims=True)

    group_row, group_col = id0_row // p.members, id0 // p.members
    place_row = group_row * p.block + jnp.sum(
        jnp.where(earlier & (group_col == group_row), 1, 0), axis=0, keepdims=True
    )
    offset = (my_group % p.per_chunk) * p.cap_pad

    def key_row(pick_row):
        return (pick_row % p.members) * p.message + offset + rank_row(pick_row)

    slots = groups * p.block
    chosen = iota((slots, rows), 0) == place_row
    chosen_b = onehot(chosen)
    place_col = to_col(place_row)
    spread_b = onehot(iota((rows, slots), 1) == place_col)

    def per_slot(row):
        return jnp.sum(jnp.where(chosen, row, jnp.zeros_like(row)), axis=1, keepdims=True)

    weights = rw_ref[...]
    columns = (
        (per_slot(key_row(id0_row) + 1) - 1).astype(F32),
        (per_slot(key_row(id1_row) + 1) - 1).astype(F32),
        per_slot(weights[0:1]),
        per_slot(weights[1:2]),
    )
    lane = iota((slots, 128), 1)
    meta = jnp.zeros((slots, 128), F32)
    for i, column in enumerate(columns):
        meta = jnp.where(lane == i, column, meta)
    for g in range(groups):
        meta_out[g] = meta[g * p.block : (g + 1) * p.block]

    pl.semaphore_wait(barrier, greeted)
    halo_copies = [
        remote(mix.at[pl.ds(local_rows - HALO, HALO)], halo, halo_send.at[0], halo_recv.at[0], {"sp": ahead, "tp": tp}),
        remote(doc_ref, halo_doc, halo_send.at[1], halo_recv.at[1], {"sp": ahead, "tp": tp}),
    ]
    loads[0].wait()

    @pl.when(sp < p.sp - 1)
    def _():
        for copy in halo_copies:
            copy.start()

    @pl.when(sp == 0)
    def _():
        halo[...] = jnp.zeros_like(halo)
        halo_doc[...] = jnp.zeros_like(halo_doc)


    doc_row = doc_ref[...]
    doc_col = to_col(doc_row)
    reach = jnp.left_shift(jnp.int32(2), tp)
    gap = iota((local_rows, local_rows), 0) - iota((local_rows, local_rows), 1)
    near = (doc_col == doc_row) & (gap >= 0) & (gap < reach)
    count = jnp.sum(jnp.where(near, 1.0, 0.0), axis=1, keepdims=True)
    mix_value = mix[...]
    running = jnp.dot(onehot(near), mix_value, preferred_element_type=F32)

    meta_copies = []
    for off in range(groups):
        g = nearest[off]
        if off == 0:
            copy = pltpu.make_async_copy(meta_out.at[g], meta_in.at[my_group], m_recv.at[my_group])
        else:
            copy = remote(meta_out.at[g], meta_in.at[my_group], m_send.at[g], m_recv.at[my_group], relay(g))
        copy.start()
        meta_copies.append(copy)

    @pl.when(sp > 0)
    def _():
        for copy in halo_copies:
            copy.wait_recv()

    back_gap = iota((HALO, HALO), 0) + HALO - iota((HALO, HALO), 1)
    first_reach = jnp.where(sp > 0, reach, 0)
    back = (doc_col[:HALO] == halo_doc[...][:, local_rows - HALO :]) & (back_gap < first_reach)
    head = running[:HALO] + jnp.dot(onehot(back), halo[...], preferred_element_type=F32)
    head_count = count[:HALO] + jnp.sum(jnp.where(back, 1.0, 0.0), axis=1, keepdims=True)
    running = jnp.concatenate([head, running[HALO:]], axis=0)
    count = jnp.concatenate([head_count, count[HALO:]], axis=0)
    mixed = (running / count - mix_value.astype(F32)).astype(BF16)
    loads[1].wait()
    grouped = (jnp.dot(mixed, gw[...], preferred_element_type=F32) * scale_ref[...].reshape(1, -1)).astype(BF16)
    for i in range(p.tp):
        grp[i] = grouped[i * rows : (i + 1) * rows]

    send_rows = jnp.concatenate([grp[(flip + 2 * j) % p.tp] for j in range(half)], axis=0)
    keep_rows = jnp.concatenate([grp[(tp + 2 * j) % p.tp] for j in range(half)], axis=0)
    loads[2].wait()
    first_hops = {}
    for h in range(parts):
        weight = ow[:, h * piece : (h + 1) * piece]
        product = jnp.dot(send_rows, weight, preferred_element_type=F32).astype(BF16)
        for j in reversed(range(half)):
            s1[j, h] = product[j * rows : (j + 1) * rows]
            copy = remote(s1.at[j, h], r1.at[j, h], s1_send.at[j, h], s1_recv.at[j, h], {"tp": flip})
            copy.start()
            first_hops[j, h] = copy
        kept = jnp.dot(keep_rows, weight, preferred_element_type=F32)
        for j in range(half):
            keep[j, h] = kept[j * rows : (j + 1) * rows]
    for load in loads[4:]:
        load.start()
    second_hops = {}
    for h in range(parts):
        for j in range(1, half):
            first_hops[j, h].wait_recv()
            s2[j, h] = (keep[j, h] + r1[j, h].astype(F32)).astype(BF16)
            copy = remote(
                s2.at[j, h], r2.at[j, h], s2_send.at[j, h], s2_recv.at[j, h], {"tp": (tp + 2 * j) % p.tp}
            )
            copy.start()
            second_hops[j, h] = copy

    for off in range(groups):
        b = nearest[off]
        if off == 0:
            meta_copies[0].wait()
        else:
            remote(meta_out.at[b], meta_in.at[b], m_send.at[b], m_recv.at[b], relay(b)).wait_recv()
    span_rows = p.per_chunk * p.block
    for k in range(p.chunks):
        info = jnp.concatenate([meta_in[k * p.per_chunk + i] for i in range(p.per_chunk)], axis=0)
        k0, k1 = info[:, 0:1], info[:, 1:2]
        k0_row, k1_row = to_row(k0).astype(I32), to_row(k1).astype(I32)
        target = iota((p.served, span_rows), 0)
        amat[k] = onehot((target == k0_row) | (target == k1_row))
        source = iota((span_rows, p.served), 1)
        combine = jnp.where(source == k0.astype(I32), info[:, 2:3], 0.0) + jnp.where(
            source == k1.astype(I32), info[:, 3:4], 0.0
        )
        high = combine.astype(BF16)
        chi[k] = high
        clo[k] = (combine - high.astype(F32)).astype(BF16)

    loads[3].wait()
    total = jnp.zeros((rows, 1), F32)
    for h in range(parts):
        cut = slice(h * piece, (h + 1) * piece)
        first_hops[0, h].wait_recv()
        summed = keep[0, h] + r1[0, h].astype(F32)
        for j in range(1, half):
            second_hops[j, h].wait_recv()
            summed = summed + r2[j, h].astype(F32)
        stream = (resid[:, cut].astype(F32) + summed).astype(BF16)
        stream_f = stream.astype(F32)
        stream_f32[:, cut] = stream_f
        total = total + jnp.sum(stream_f * stream_f, axis=1, keepdims=True)
    normed = (stream_f32[...] * lax.rsqrt(total / d + 1e-06) * gain_ref[...]).astype(BF16)

    gathered = jnp.dot(chosen_b, normed, preferred_element_type=F32).astype(BF16)
    for g in range(groups):
        zb[g] = gathered[g * p.block : (g + 1) * p.block]
    z_copies = []
    for off in range(groups):
        g = nearest[off]
        if off == 0:
            copy = pltpu.make_async_copy(zb.at[g], zin.at[my_group], z_recv.at[my_group])
        else:
            copy = remote(zb.at[g], zin.at[my_group], z_send.at[g], z_recv.at[my_group], relay(g))
        copy.start()
        z_copies.append(copy)

    if p.chunks == groups:
        order = [[off] for off in range(groups)]
    else:
        order = [list(range(groups))]

    x_copies, b_copies, f_copies = [], [], []

    def forward(offs):
        k = nearest[offs[0]] if p.chunks > 1 else 0
        for off in offs:
            b = nearest[off]
            if off == 0:
                z_copies[0].wait()
            else:
                remote(zb.at[b], zin.at[b], z_send.at[b], z_recv.at[b], relay(b)).wait_recv()
        if p.chunks > 1:
            source = zin[k]
        else:
            source = jnp.concatenate([zin[i] for i in range(groups)], axis=0)
        picked = jnp.dot(amat[k], source, preferred_element_type=F32).astype(BF16)
        for e in range(p.members):
            xout[k, e] = picked[e * p.message : (e + 1) * p.message]
        for step in range(p.members):
            e = (me + step) % p.members
            if step == 0:
                copy = pltpu.make_async_copy(xout.at[k, e], xin.at[k, me], x_recv.at[k, me])
            else:
                copy = remote(xout.at[k, e], xin.at[k, me], x_send.at[k, e], x_recv.at[k, me], member(e))
            copy.start()
            x_copies.append((step, copy))

    def serve(n, offs):
        k = nearest[offs[0]] if p.chunks > 1 else 0
        for step in range(p.members):
            e = (me + step) % p.members
            if step == 0:
                x_copies[n * p.members][1].wait()
            else:
                remote(xout.at[k, e], xin.at[k, e], x_send.at[k, e], x_recv.at[k, e], member(e)).wait_recv()
        if n == 0:
            for i in (4, 5, 6):
                loads[i].wait()
        flat = jnp.concatenate([xin[k, e] for e in range(p.members)], axis=0)
        gate_part = jnp.dot(flat, wg[...], preferred_element_type=F32)
        up_part = jnp.dot(flat, wu[...], preferred_element_type=F32)
        hidden = (gate_part * jax.nn.sigmoid(gate_part) * up_part).astype(BF16)
        answer = jnp.dot(hidden, wd[...], preferred_element_type=F32).astype(BF16)
        for e in range(p.members):
            ans[k, e] = answer[e * p.message : (e + 1) * p.message]
        for step in range(p.members):
            e = (me + step) % p.members
            if step == 0:
                copy = pltpu.make_async_copy(ans.at[k, e], ret.at[k, me], b_recv.at[k, me])
            else:
                copy = remote(ans.at[k, e], ret.at[k, me], b_send.at[k, e], b_recv.at[k, me], member(e))
            copy.start()
            b_copies.append((step, copy))

    def collect(n, offs):
        k = nearest[offs[0]] if p.chunks > 1 else 0
        for step in range(p.members):
            e = (me + step) % p.members
            if step == 0:
                b_copies[n * p.members][1].wait()
            else:
                remote(ans.at[k, e], ret.at[k, e], b_send.at[k, e], b_recv.at[k, e], member(e)).wait_recv()
        flat = jnp.concatenate([ret[k, e] for e in range(p.members)], axis=0)
        joined = jnp.dot(chi[k], flat, preferred_element_type=F32) + jnp.dot(clo[k], flat, preferred_element_type=F32)
        joined = joined.astype(BF16)
        if p.chunks > 1:
            zo[k] = joined
        else:
            for i in range(groups):
                zo[i] = joined[i * p.block : (i + 1) * p.block]
        for off in offs:
            b = nearest[off]
            if off == 0:
                copy = pltpu.make_async_copy(zo.at[b], fin.at[my_group], f_recv.at[my_group])
            else:
                copy = remote(zo.at[b], fin.at[my_group], f_send.at[b], f_recv.at[my_group], relay(b))
            copy.start()
            f_copies.append((off, copy))

    count_chunks = len(order)
    forward(order[0])
    for n in range(count_chunks):
        if n + 1 < count_chunks:
            forward(order[n + 1])
        serve(n, order[n])
        if n >= 1:
            collect(n - 1, order[n - 1])
    collect(count_chunks - 1, order[-1])

    for off in range(groups):
        g = nearest[off]
        if off == 0:
            [copy for o, copy in f_copies if o == 0][0].wait()
        else:
            remote(zo.at[g], fin.at[g], f_send.at[g], f_recv.at[g], relay(g)).wait_recv()
    flat = jnp.concatenate([fin[g] for g in range(groups)], axis=0)
    out_ref[...] = (stream_f32[...] + jnp.dot(spread_b, flat, preferred_element_type=F32)).astype(BF16)

    @pl.when(sp < p.sp - 1)
    def _():
        for copy in halo_copies:
            copy.wait_send()

    for copy in meta_copies[1:] + list(first_hops.values()) + list(second_hops.values()) + z_copies[1:]:
        copy.wait_send()
    for step, copy in x_copies + b_copies + f_copies:
        if step:
            copy.wait_send()


def ordered(position, table):
    n = len(table)
    return [
        sum((1 - ((position - z + n) % n + n - 1) // n) * table[z][i] for z in range(n)) for i in range(len(table[0]))
    ]


def chunk_kernel(
    p,
    mix_hbm, resid_hbm, doc_ref, gw_hbm, scale_ref, ow_hbm, gain_ref, ids_ref, rw_ref, wg_hbm, wu_hbm, wd_hbm,
    out_ref,
    mix, resid, gw, ow, wg, wu, wd,
    halo, halo_doc, grp, keep, s1, r1, s2, r2, stream_f32, meta_out, meta_in, zb, zin, amat, chi, clo,
    xout, xin, gates, ups, levels, ans, ret, zo, fin,
    load_sem, sent, halo_send, halo_recv, m_recv, s1_recv, s2_recv, z_recv, x_recv, b_recv, f_recv, far,
):
    sp, tp = lax.axis_index("sp"), lax.axis_index("tp")
    local_rows, width = mix.shape
    d = resid.shape[1]
    rows, groups, half, members = p.rows, p.groups, p.half, p.members
    parts, x_parts, b_parts = zb.shape[1], xout.shape[1], ans.shape[1]
    piece, x_piece, b_piece = d // parts, d // x_parts, d // b_parts
    loads = [
        pltpu.make_async_copy(src, dst, load_sem.at[i])
        for i, (src, dst) in enumerate(
            [
                (mix_hbm, mix), (gw_hbm.at[0], gw), (ow_hbm, ow), (resid_hbm, resid),
                (wg_hbm.at[0], wg), (wu_hbm.at[0], wu), (wd_hbm.at[0], wd),
            ]
        )
    ]

    my_group, lane_in_span = sp // p.span, sp % p.span
    me = lane_in_span * p.tp + tp
    flip = tp + 1 - 2 * (tp % 2)
    order = ordered(my_group, TABLE)
    others = order[1:]
    receivers = ordered(my_group, SEND)

    def relay(group):
        return {"sp": group * p.span + lane_in_span, "tp": tp}

    def member(index):
        return {"sp": my_group * p.span + index // p.tp, "tp": index % p.tp}

    barrier = pltpu.get_barrier_semaphore()
    has_ahead, has_behind = (2 * p.sp - 2 - sp) // p.sp, (sp + p.sp - 1) // p.sp
    ahead = (sp + 1) % p.sp

    def greet(semaphore):
        @pl.when(sp < p.sp - 1)
        def _():
            pl.semaphore_signal(semaphore, inc=1, device_id={"sp": sp + 1, "tp": tp}, device_id_type=MESH)

        @pl.when(sp > 0)
        def _():
            pl.semaphore_signal(semaphore, inc=1, device_id={"sp": sp - 1, "tp": tp}, device_id_type=MESH)

    greet(barrier)
    for off in range(1, members):
        pl.semaphore_signal(barrier, inc=1, device_id=member((me + off) % members), device_id_type=MESH)
    def weights_now(stage):
        for load, when in zip(loads[3:], W_AT):
            if when == stage:
                load.start()

    for load in loads[:3]:
        load.start()
    weights_now(0)

    def remote(src, dst, send, recv, device):
        return pltpu.make_async_remote_copy(
            src_ref=src, dst_ref=dst, send_sem=send, recv_sem=recv, device_id=device, device_id_type=MESH
        )

    doc_row = doc_ref[...]
    doc_col = to_col(doc_row)
    reach = jnp.left_shift(jnp.int32(2), tp)
    gap = iota((local_rows, local_rows), 0) - iota((local_rows, local_rows), 1)
    near = (doc_col == doc_row) & (gap >= 0) & (gap < reach)
    count = jnp.sum(jnp.where(near, 1.0, 0.0), axis=1, keepdims=True)
    near_b = onehot(near)
    loads[0].wait()
    running = jnp.dot(near_b, mix[...], preferred_element_type=F32)
    mixed = (running / count - mix[...].astype(F32)).astype(BF16)
    loads[1].wait()
    scale = scale_ref[...].reshape(1, -1)
    grouped = (jnp.dot(mixed, gw[...], preferred_element_type=F32) * scale).astype(BF16)
    for i in range(p.tp):
        grp[i] = grouped[i * rows : (i + 1) * rows]

    with jax.named_scope("barrier"):
        pl.semaphore_wait(barrier, members - 1 + has_ahead + has_behind)
    halo_copies = [
        remote(mix.at[pl.ds(local_rows - HALO, HALO)], halo, halo_send.at[0], halo_recv.at[0], {"sp": ahead, "tp": tp}),
        remote(doc_ref, halo_doc, halo_send.at[1], halo_recv.at[1], {"sp": ahead, "tp": tp}),
    ]

    @pl.when(sp < p.sp - 1)
    def _():
        for copy in halo_copies:
            copy.start()

    @pl.when(sp == 0)
    def _():
        halo[...] = jnp.zeros_like(halo)
        halo_doc[...] = jnp.zeros_like(halo_doc)

    greet(far.at[0])


    send_rows = jnp.concatenate([grp[(flip + 2 * j) % p.tp] for j in range(half)], axis=0)
    keep_rows = jnp.concatenate([grp[(tp + 2 * j) % p.tp] for j in range(half)], axis=0)
    loads[2].wait()
    for h in range(parts):
        weight = ow[:, h * piece : (h + 1) * piece]
        product = jnp.dot(send_rows, weight, preferred_element_type=F32).astype(BF16)
        for j in range(half):
            s1[j, h] = product[j * rows : (j + 1) * rows]
        kept = jnp.dot(keep_rows, weight, preferred_element_type=F32)
        for j in range(half):
            keep[j, h] = kept[j * rows : (j + 1) * rows]

    def arrived(ref, semaphore):
        pltpu.make_async_copy(ref, ref, semaphore).wait()

    def place(source, target):
        return (target - source + groups) % groups - 1


    first_hops = {
        (j, h): remote(s1.at[j, h], r1.at[j, h], sent.at[0], s1_recv.at[j, h], {"tp": flip})
        for j in range(half)
        for h in range(parts)
    }
    second_hops = {
        (j, h): remote(
            s2.at[j - 1, h], r2.at[j - 1, h], sent.at[1], s2_recv.at[j - 1, h], {"tp": (tp + 2 * j) % p.tp}
        )
        for j in range(1, half)
        for h in range(parts)
    }

    def send_first():
        for j in reversed(range(half)):

            @pl.when((flip + 2 * j) % p.tp > 0)
            def _():
                for h in range(parts):
                    first_hops[j, h].start()

    def send_second(late):
        for j in range(1, half):
            block = (tp + 2 * j) % p.tp

            @pl.when((block == 0) if late else (block > 0))
            def _():
                for h in range(parts):
                    with jax.named_scope("fh_wait"):
                        first_hops[j, h].wait_recv()
                    s2[j - 1, h] = (keep[j, h] + r1[j, h].astype(F32)).astype(BF16)
                    second_hops[j, h].start()

    send_first()
    for turn in range(1, p.sp - 2):
        pl.semaphore_wait(far.at[turn - 1], has_ahead + has_behind)
        greet(far.at[turn])
    weights_now(1)

    ids = ids_ref[...]
    id0_row, id1_row = ids[0:1], ids[1:2]
    id0, id1 = to_col(id0_row), to_col(id1_row)
    earlier = iota((rows, rows), 0) < iota((rows, rows), 1)

    def rank_row(pick_row):
        hit = earlier & ((id0 == pick_row) | (id1 == pick_row))
        return jnp.sum(jnp.where(hit, 1, 0), axis=0, keepdims=True)

    group_row, group_col = id0_row // members, id0 // members
    place_row = group_row * p.block + jnp.sum(
        jnp.where(earlier & (group_col == group_row), 1, 0), axis=0, keepdims=True
    )

    def key_row(pick_row):
        return (pick_row % members) * p.message + rank_row(pick_row)

    slots = groups * p.block
    chosen = iota((slots, rows), 0) == place_row
    chosen_b = onehot(chosen)
    place_col = to_col(place_row)
    spread_order = jnp.concatenate([my_group * p.block + iota((1, p.block), 1)] + [g * p.block + iota((1, p.block), 1) for g in others], axis=1)
    spread_b = onehot(spread_order == place_col)

    def per_slot(row):
        return jnp.sum(jnp.where(chosen, row, jnp.zeros_like(row)), axis=1, keepdims=True)

    weights = rw_ref[...]
    columns = (
        (per_slot(key_row(id0_row) + 1) - 1).astype(F32),
        (per_slot(key_row(id1_row) + 1) - 1).astype(F32),
        per_slot(weights[0:1]),
        per_slot(weights[1:2]),
    )
    lane = iota((slots, 128), 1)
    meta = jnp.zeros((slots, 128), F32)
    for i, column in enumerate(columns):
        meta = jnp.where(lane == i, column, meta)
    for g in range(groups):
        meta_out[g] = meta[g * p.block : (g + 1) * p.block]
    send_second(False)
    weights_now(2)

    @pl.when(sp > 0)
    def _():
        for copy in halo_copies:
            with jax.named_scope("halo_wait"):
                copy.wait_recv()

    back_gap = iota((HALO, HALO), 0) + HALO - iota((HALO, HALO), 1)
    first_reach = jnp.where(sp > 0, reach, 0)
    back = (doc_col[:HALO] == halo_doc[...][:, local_rows - HALO :]) & (back_gap < first_reach)
    head = running[:HALO] + jnp.dot(onehot(back), halo[...], preferred_element_type=F32)
    head_count = count[:HALO] + jnp.sum(jnp.where(back, 1.0, 0.0), axis=1, keepdims=True)
    head_mixed = (head / head_count - mix[:HALO].astype(F32)).astype(BF16)
    head_grouped = (jnp.dot(head_mixed, gw[...], preferred_element_type=F32) * scale).astype(BF16)
    keep_slot = ((p.tp - tp) % p.tp) // 2
    send_slot = ((p.tp - flip) % p.tp) // 2
    for h in range(parts):
        weight = ow[:, h * piece : (h + 1) * piece]
        head_product = jnp.dot(head_grouped, weight, preferred_element_type=F32)

        @pl.when(tp % 2 == 0)
        def _():
            keep[keep_slot, h, :HALO] = head_product

        @pl.when(tp % 2 == 1)
        def _():
            s1[send_slot, h, :HALO] = head_product.astype(BF16)
            remote(
                s1.at[send_slot, h], r1.at[send_slot, h], sent.at[0], s1_recv.at[send_slot, h], {"tp": flip}
            ).start()

    with jax.named_scope("far"):
        pl.semaphore_wait(far.at[p.sp - 3], has_ahead + has_behind)
    for g in others:
        slot = place(my_group, g)
        remote(meta_out.at[g], meta_in.at[slot], sent.at[2], m_recv.at[slot], relay(g)).start()

    send_second(True)
    weights_now(3)

    def tables(k, info):
        k0, k1 = info[:, 0:1], info[:, 1:2]
        k0_row, k1_row = to_row(k0).astype(I32), to_row(k1).astype(I32)
        target = iota((p.served, p.block), 0)
        amat[k] = onehot((target == k0_row) | (target == k1_row))
        source = iota((p.block, p.served), 1)
        combine = jnp.where(source == k0.astype(I32), info[:, 2:3], 0.0) + jnp.where(
            source == k1.astype(I32), info[:, 3:4], 0.0
        )
        high = combine.astype(BF16)
        chi[k] = high
        clo[k] = (combine - high.astype(F32)).astype(BF16)

    tables(my_group, meta_out[my_group])
    ratio = parts // x_parts

    def forward_part(k, part, source):
        picked = jnp.dot(amat[k], source, preferred_element_type=F32).astype(BF16)
        for e in range(members):
            xout[k, part, e] = picked[e * p.message : (e + 1) * p.message]
        for step in list(range(2, members)) + [1]:
            e = (me + step) % members
            remote(xout.at[k, part, e], xin.at[k, part, me], sent.at[4], x_recv.at[k, part], member(e)).start()
        xin[k, part, me] = xout[k, part, me]

    def send_z(g, h):
        slot = place(my_group, g)
        remote(zb.at[g, h], zin.at[slot, h], sent.at[3], z_recv.at[slot, h], relay(g)).start()

    def forward_own(part):
        source = jnp.concatenate([zb[my_group, i] for i in range(part * ratio, (part + 1) * ratio)], axis=1)
        forward_part(my_group, part, source)

    loads[3].wait()
    for h in range(parts):
        weights_now(4 + h)
        cut = slice(h * piece, (h + 1) * piece)
        with jax.named_scope("fh0_wait"):
            first_hops[0, h].wait_recv()
        summed = keep[0, h] + r1[0, h].astype(F32)
        for j in range(1, half):
            with jax.named_scope("sh_wait"):
                second_hops[j, h].wait_recv()
            summed = summed + r2[j - 1, h].astype(F32)
        stream = (resid[:, cut].astype(F32) + summed).astype(BF16)
        stream_f32[:, cut] = stream.astype(F32)
        gathered = jnp.dot(chosen_b, stream, preferred_element_type=F32).astype(BF16)
        for g in range(groups):
            zb[g, h] = gathered[g * p.block : (g + 1) * p.block]
        for position, part in Z_ORDER[h]:
            send_z(receivers[position], part)
        if h % ratio == ratio - 1 and not OWN_LATE:
            forward_own(h // ratio)

    for g in others:
        with jax.named_scope("m_wait"):
            slot = place(g, my_group)
            arrived(meta_in.at[slot], m_recv.at[slot])
        tables(g, meta_in[slot])

    def forward(k, part):
        slot = place(k, my_group)
        for h in range(part * ratio, (part + 1) * ratio):
            with jax.named_scope("z_wait"):
                arrived(zin.at[slot, h], z_recv.at[slot, h])
        source = jnp.concatenate([zin[slot, i] for i in range(part * ratio, (part + 1) * ratio)], axis=1)
        forward_part(k, part, source)

    waited, absorbed = [], set()

    def absorb(k, name, part):
        with jax.named_scope("x_wait"):
            arrived(xin.at[k, part, pl.ds(0, members - 1)], x_recv.at[k, part])
        if not waited:
            waited.append(True)
            for i in (4, 5, 6):
                loads[i].wait()
        cut = slice(part * x_piece, (part + 1) * x_piece)
        flat = jnp.concatenate([xin[k, part, e] for e in range(members)], axis=0).astype(F32)
        level = jnp.broadcast_to(jnp.sum(flat * flat, axis=1, keepdims=True), (p.served, 128))
        scaled = (flat * gain_ref[:, cut]).astype(BF16)
        gate_part = jnp.dot(scaled, wg[cut], preferred_element_type=F32)
        up_part = jnp.dot(scaled, wu[cut], preferred_element_type=F32)
        if part == 0:
            levels[k], gates[k], ups[k] = level, gate_part, up_part
        else:
            levels[k] += level
            gates[k] += gate_part
            ups[k] += up_part
        absorbed.add((name, part))

    def answer_back(k, part):
        for step in list(range(2, members)) + [1]:
            e = (me + step) % members
            remote(ans.at[k, part, e], ret.at[k, part, me], sent.at[5], b_recv.at[k, part], member(e)).start()

    def serve(k, name):
        for part in range(x_parts):
            if (name, part) not in absorbed:
                absorb(k, name, part)
        with jax.named_scope("expert"):
            factor = lax.rsqrt(levels[k][:, :1] / d + 1e-06)
            gate_part = gates[k] * factor
            hidden = (gate_part * jax.nn.sigmoid(gate_part) * (ups[k] * factor)).astype(BF16)
            for part in range(b_parts):
                weight = wd[:, part * b_piece : (part + 1) * b_piece]
                answer = jnp.dot(hidden, weight, preferred_element_type=F32).astype(BF16)
                for e in range(members):
                    ans[k, part, e] = answer[e * p.message : (e + 1) * p.message]
                if name != "o":
                    answer_back(k, part)
                ret[k, part, me] = ans[k, part, me]

    def collect(k, wanted, own=False):
        for part in wanted:
            with jax.named_scope("b_wait"):
                arrived(ret.at[k, part, pl.ds(0, members - 1)], b_recv.at[k, part])
            flat = jnp.concatenate([ret[k, part, e] for e in range(members)], axis=0)
            joined = jnp.dot(chi[k], flat, preferred_element_type=F32) + jnp.dot(clo[k], flat, preferred_element_type=F32)
            if own:
                fin[groups - 1, part] = joined.astype(BF16)
            else:
                slot = place(my_group, k)
                zo[k, part] = joined.astype(BF16)
                remote(zo.at[k, part], fin.at[slot, part], sent.at[6], f_recv.at[slot, part], relay(k)).start()

    weights_now(4 + parts)
    chunks = {"o": my_group, "n": others[0], "m": others[1], "f": others[2]}
    for step in " ".join(SEQUENCE).split():
        k = chunks[step[1]]
        if step[:2] == "Fo":
            for part in [int(step[2])] if step[2:] else range(x_parts):
                forward_own(part)
        elif step[0] == "F":
            for part in [int(step[2])] if step[2:] else range(x_parts):
                forward(k, part)
        elif step[0] == "E":
            for part in [int(step[2])] if step[2:] else range(x_parts):
                absorb(k, step[1], part)
        elif step[0] == "B":
            for part in [int(step[2])] if step[2:] else range(b_parts):
                answer_back(k, part)
        elif step[0] == "S":
            serve(k, step[1])
        else:
            collect(k, [int(step[2])] if step[2:] else range(b_parts), own=step[1] == "o")

    for part in range(b_parts):
        cut = slice(part * b_piece, (part + 1) * b_piece)
        total = stream_f32[:, cut]
        arrivals = [(groups - 1, my_group)] + [(place(g, my_group), g) for g in others]
        with jax.named_scope("f_wait"):
            for slot, _ in arrivals[1:]:
                arrived(fin.at[slot, part], f_recv.at[slot, part])
        flat = jnp.concatenate([fin[slot, part] for slot, _ in arrivals], axis=0)
        out_ref[:, cut] = (total + jnp.dot(spread_b, flat, preferred_element_type=F32)).astype(BF16)

    @pl.when(sp < p.sp - 1)
    def _():
        for copy in halo_copies:
            copy.wait_send()

    arrived(s1, sent.at[0])
    arrived(s2, sent.at[1])
    arrived(meta_out.at[pl.ds(0, groups - 1)], sent.at[2])
    arrived(zb.at[pl.ds(0, groups - 1)], sent.at[3])
    arrived(xout.at[:, :, pl.ds(0, members - 1)], sent.at[4])
    arrived(ans.at[:, :, pl.ds(0, members - 1)], sent.at[5])
    arrived(zo.at[pl.ds(0, groups - 1)], sent.at[6])


def shards(
    sp_size,
    tp_size,
    mix_in,
    resid_in,
    doc_ids,
    group_weight,
    pool_scale,
    out_weight,
    norm_gain,
    expert_ids,
    route_weights,
    w_gate,
    w_up,
    w_down,
):
    local_rows, width = mix_in.shape
    rows, d = resid_in.shape
    ff = w_gate.shape[2]
    p = Plan(sp_size, tp_size, rows)
    g, half, parts = p.groups, p.half, p.parts
    vmem = pl.BlockSpec(memory_space=pltpu.VMEM)
    hbm = pl.BlockSpec(memory_space=pl.ANY)
    dma = pltpu.SemaphoreType.DMA
    common = [
        pltpu.VMEM((local_rows, width), BF16),
        pltpu.VMEM((rows, d), BF16),
        pltpu.VMEM(group_weight.shape[1:], BF16),
        pltpu.VMEM(out_weight.shape, BF16),
        pltpu.VMEM(w_gate.shape[1:], BF16),
        pltpu.VMEM(w_up.shape[1:], BF16),
        pltpu.VMEM(w_down.shape[1:], BF16),
        pltpu.VMEM((HALO, width), BF16),
        pltpu.VMEM((1, local_rows), I32),
        pltpu.VMEM((tp_size, rows, width), BF16),
    ]
    stream_and_meta = [
        pltpu.VMEM((rows, d), F32),
        pltpu.VMEM((g, p.block, 128), F32),
        pltpu.VMEM((g, p.block, 128), F32),
    ]
    if p.chunks == g and sp_size == g == 4:
        body = chunk_kernel
        parts, x_parts, b_parts = PARTS
        exchange = (half, parts, rows, d // parts)
        remote_exchange = (half - 1, parts, rows, d // parts)
        slots = (g, parts, p.block, d // parts)
        scratch = common + [
            pltpu.VMEM(exchange, F32),
            pltpu.VMEM(exchange, BF16),
            pltpu.VMEM(exchange, BF16),
            pltpu.VMEM(remote_exchange, BF16),
            pltpu.VMEM(remote_exchange, BF16),
            pltpu.VMEM((rows, d), F32),
            pltpu.VMEM((g, p.block, 128), F32),
            pltpu.VMEM((g - 1, p.block, 128), F32),
            pltpu.VMEM(slots, BF16),
            pltpu.VMEM((g - 1, *slots[1:]), BF16),
            pltpu.VMEM((g, p.served, p.block), BF16),
            pltpu.VMEM((g, p.block, p.served), BF16),
            pltpu.VMEM((g, p.block, p.served), BF16),
            pltpu.VMEM((g, x_parts, p.members, p.message, d // x_parts), BF16),
            pltpu.VMEM((g, x_parts, p.members, p.message, d // x_parts), BF16),
            pltpu.VMEM((g, p.served, w_gate.shape[2]), F32),
            pltpu.VMEM((g, p.served, w_gate.shape[2]), F32),
            pltpu.VMEM((g, p.served, 128), F32),
            pltpu.VMEM((g, b_parts, p.members, p.message, d // b_parts), BF16),
            pltpu.VMEM((g, b_parts, p.members, p.message, d // b_parts), BF16),
            pltpu.VMEM((g, b_parts, p.block, d // b_parts), BF16),
            pltpu.VMEM((g, b_parts, p.block, d // b_parts), BF16),
            dma((7,)), dma((7,)),
            dma((2,)), dma((2,)),
            dma((g - 1,)),
            dma((half, parts)),
            dma((half - 1, parts)),
            dma((g - 1, parts)),
            dma((g, x_parts)),
            dma((g, b_parts)),
            dma((g - 1, b_parts)),
            pltpu.SemaphoreType.REGULAR((sp_size - 2,)),
        ]
    else:
        body = kernel
        span_rows = p.per_chunk * p.block
        messages = (p.chunks, p.members, p.message, d)
        exchange = (half, parts, rows, d // parts)
        scratch = common + [
            pltpu.VMEM(exchange, F32),
            pltpu.VMEM(exchange, BF16),
            pltpu.VMEM(exchange, BF16),
            pltpu.VMEM(exchange, BF16),
            pltpu.VMEM(exchange, BF16),
        ] + stream_and_meta + [
            pltpu.VMEM((g, p.block, d), BF16),
            pltpu.VMEM((g, p.block, d), BF16),
            pltpu.VMEM((p.chunks, p.served, span_rows), BF16),
            pltpu.VMEM((p.chunks, span_rows, p.served), BF16),
            pltpu.VMEM((p.chunks, span_rows, p.served), BF16),
            pltpu.VMEM(messages, BF16),
            pltpu.VMEM(messages, BF16),
            pltpu.VMEM(messages, BF16),
            pltpu.VMEM(messages, BF16),
            pltpu.VMEM((g, p.block, d), BF16),
            pltpu.VMEM((g, p.block, d), BF16),
            dma((7,)),
            dma((2,)), dma((2,)),
            dma((g,)), dma((g,)),
            dma((half, parts)), dma((half, parts)),
            dma((half, parts)), dma((half, parts)),
            dma((g,)), dma((g,)),
            dma((p.chunks, p.members)), dma((p.chunks, p.members)),
            dma((p.chunks, p.members)), dma((p.chunks, p.members)),
            dma((g,)), dma((g,)),
        ]
    return pl.pallas_call(
        functools.partial(body, p),
        out_shape=pltpu.VMEM((rows, d), BF16),
        in_specs=[hbm, hbm, vmem, hbm, vmem, hbm, vmem, vmem, vmem, hbm, hbm, hbm],
        out_specs=vmem,
        scratch_shapes=scratch,
        compiler_params=pltpu.CompilerParams(
            collective_id=0, has_side_effects=True, vmem_limit_bytes=56 * 1024 * 1024
        ),
    )(
        mix_in, resid_in, doc_ids.reshape(1, -1), group_weight, pool_scale, out_weight,
        norm_gain.reshape(1, -1), expert_ids.T, route_weights.T, w_gate, w_up, w_down,
    )


def solution(mesh):
    return jax.shard_map(
        functools.partial(shards, mesh.shape["sp"], mesh.shape["tp"]),
        mesh=mesh,
        in_specs=(
            P(("grp", "sp"), "tp"),
            P(("grp", "sp", "tp"), None),
            P(("grp", "sp")),
            P("tp", None, None),
            P("tp"),
            P("tp", None),
            P(),
            P(("grp", "sp", "tp"), None),
            P(("grp", "sp", "tp"), None),
            P(("sp", "tp"), None, None),
            P(("sp", "tp"), None, None),
            P(("sp", "tp"), None, None),
        ),
        out_specs=P(("grp", "sp", "tp"), None),
        check_vma=False,
    )
```
